32 devices in a mesh: sp: 4 (over y, x), tp: 8 (over z, core).
Axes of the slice: x: 2, y: 2, z: 4, core: 2. Of those that a mesh axis runs over, the one named last changes fastest.
Arguments:
- query_heads: bfloat16 [4096, 2048], P('sp', 'tp'), may hold values from -256 to 256
- key_heads: bfloat16 [4096, 1024], P('sp', 'tp'), may hold values from -7 to 7
- value_heads: bfloat16 [4096, 1024], P('sp', 'tp'), may hold values from -6 to 6
- sink_logit: float32 [32], P('tp'), may hold values from 3 to 7
- residual: bfloat16 [4096, 2048], P(('sp', 'tp')), may hold values from -6 to 6
- out_weight: bfloat16 [2048, 2048], replicated, may hold values from -0.5 to 0.5
- norm_gain: float32 [2048], replicated, may hold values from 0.1 to 1.9
- routes: int32 [4096, 2], P('sp'), may hold values from 0 to 3, all different within a row; in each aligned block of 128 rows (0 to 127, 128 to 255, ...) at most 80 rows name the same one
- route_weight: float32 [4096, 2], P(('sp', 'tp')), may hold values from 0.2 to 1
- gate_weight: bfloat16 [4, 2048, 2048], P('sp', None, 'tp'), may hold values from -0.3125 to 0.3125
- up_weight: bfloat16 [4, 2048, 2048], P('sp', None, 'tp'), may hold values from -0.3125 to 0.3125
- down_weight: bfloat16 [4, 2048, 2048], P('sp', 'tp'), may hold values from -0.0625 to 0.0625
Outputs:
- updated: bfloat16 [4096, 2048], P(('sp', 'tp'))
The draws below stay inside these ranges and needn't reach their ends.
Inputs may be any that keep to these rules, and one draw needn't show every extreme that they name: `routes`: each row names 2 different experts. In each aligned block of 128 rows no expert is named more than 80 times, and in every draw some block names some expert exactly 80 times.
All inputs are finite; a program needn't handle non-finite values.
Results may differ from the reference program's by a relative error of at most 0.023.
Values may be sent and summed in bfloat16 or wider, within the bound.
A program may use at most 128 MiB of HBM per device.

```python
import math
import jax
import jax.numpy as jnp
import numpy as np
from jax import lax

D = 2048
HEAD = 64
HQ = 32
KVH = 16
FF = 2048
WINDOW = 128
TOP = 2
SEQ = 4096
TOKENS = 4096
TOK_DEV = 128
EXPERTS = 4
CAP = 80
N_SP = 4
N_TP = 8


def drawn_keys(key):
    base = jnp.clip(jax.random.normal(jax.random.fold_in(key, 101), (SEQ, KVH * HEAD), jnp.float32), -6.0, 6.0)
    return base


def draw_key_heads(key, part):
    base = drawn_keys(key)
    return base.astype(jnp.bfloat16)


def draw_query_heads(key, part):
    queries = jnp.clip(jax.random.normal(jax.random.fold_in(key, 104), (SEQ, HQ * HEAD), jnp.float32), -6.0, 6.0)
    return queries.astype(jnp.bfloat16)


def steps_of(key, extent, shards, least, top_value):
    factor_of, own = 1.0, jax.random.fold_in(key, 6)
    for axis_at, blocks in shards:
        draws = jnp.exp(jax.random.uniform(jax.random.fold_in(own, axis_at), (blocks,), jnp.float32, least / len(shards), top_value / len(shards)))
        factor_of = factor_of * jnp.repeat(draws, extent[axis_at] // blocks).reshape([-1 if axis == axis_at else 1 for axis in range(len(extent))])
    return factor_of


def routed_block(stream_key, own, number, rows, amount, top, limit, slope):
    order = jax.random.permutation(stream_key, amount)
    packed, common = shares(amount, rows * top, limit, slope, True), shares(amount, rows * top, limit, slope, False)
    places = jnp.arange(amount)

    def named(lengths, offset_by):
        used = int((lengths > 0).sum())
        fixed = max(1, used // 4)
        shifted = fixed + (places - fixed + offset_by * (used - fixed)) % max(1, amount - fixed)
        return jnp.zeros((amount,), jnp.int32).at[order[jnp.where(places < fixed, places, shifted)]].set(jnp.asarray(lengths, jnp.int32))

    lengths = jnp.where(number % 4 == 0, named(packed, number // 4), named(common, number - number // 4 - 1))
    mixed = jax.random.permutation(jax.random.fold_in(own, 3), amount)
    donor, sink = mixed[0:amount // 2 * 2:2], mixed[1:amount // 2 * 2:2]
    room = jnp.minimum(lengths[donor] - 1, limit - lengths[sink]) // 2
    room = jnp.where((donor == order[0]) | (sink == order[0]) | (lengths[sink] == 0), 0, jnp.maximum(room, 0))
    shifted = jax.random.randint(jax.random.fold_in(own, 4), (amount // 2,), 0, 1 << 20) % (room + 1)
    lengths = lengths.at[donor].add(-shifted).at[sink].add(shifted)
    members = jnp.searchsorted(jnp.cumsum(lengths), jnp.arange(rows * top), side="right").astype(jnp.int32)
    grid = members.reshape(top, rows).T
    grid = grid[jax.random.permutation(jax.random.fold_in(own, 1), rows)]
    offset_by = jax.random.randint(jax.random.fold_in(own, 2), (rows, 1), 0, top)
    return jnp.take_along_axis(grid, (jnp.arange(top)[None, :] + offset_by) % top, axis=1)


def shares(amount, total, bound, slope, full):
    weights = [(1 << 20) // math.isqrt(standing ** slope) + 1 for standing in range(1, amount + 1)]
    largest = bound if full else min(bound, max(-(-total // amount), total * weights[0] // sum(weights)))
    least = 1 if total - largest >= amount - 1 else 0
    given, rest = [largest] + [least] * (amount - 1), total - largest - least * (amount - 1)
    while rest > 0:
        free = [i for i in range(1, amount) if given[i] < largest] or [i for i in range(1, amount) if given[i] < bound]
        pool, remaining = sum([weights[i] for i in free]), rest
        for i in free:
            extra = min(bound - given[i], max(1, remaining * weights[i] // pool), rest)
            given[i] = given[i] + extra
            rest = rest - extra
    return np.array(given)


def centred(own_key, dims, spread, limit, shards=(), held_as=jnp.bfloat16):
    array = spread * jax.random.normal(own_key, dims, jnp.float32)
    if shards:
        array = array * steps_of(own_key, dims, shards, -0.22, 0.18)
    return jnp.clip(array, -limit, limit).astype(held_as)


def setup_inputs(seed: int = 0) -> dict:
    arg_keys = jax.random.split(jax.random.key(seed), 13)
    query_heads = draw_query_heads(jax.random.fold_in(arg_keys[12], 71), 0)
    key_heads = draw_key_heads(jax.random.fold_in(arg_keys[12], 71), 0)
    value_heads = centred(arg_keys[2], (SEQ, KVH * HEAD), 1.0, 6.0, ((0, 4), (1, 8)))
    sink_logit = jnp.clip(3.0 + 4.0 * jax.random.uniform(arg_keys[3], (HQ,), jnp.float32) ** steps_of(arg_keys[3], (HQ,), ((0, 8),), -0.2, 0.2), 3.0, 7.0)
    residual = centred(arg_keys[4], (TOKENS, D), 1.0, 6.0, ((0, 32),))
    out_weight = centred(arg_keys[5], (HQ * HEAD, D), (HQ * HEAD // 16) ** -0.5, 0.5)
    norm_gain = jnp.clip(1.0 + 0.18 * jax.random.normal(arg_keys[6], (D,), jnp.float32), 0.1, 1.9)
    routes_keys = jax.random.split(jax.random.fold_in(arg_keys[7], 1), TOKENS // TOK_DEV)
    routes_turns = jax.random.permutation(jax.random.fold_in(arg_keys[7], 3), TOKENS // TOK_DEV)
    routes = jax.vmap(lambda own, number: routed_block(jax.random.fold_in(arg_keys[7], 2), own, number, TOK_DEV, EXPERTS, TOP, CAP, 1))(routes_keys, routes_turns).reshape((TOKENS, TOP))
    route_weight = jnp.clip(0.2 + 0.8 * jax.random.uniform(arg_keys[8], (TOKENS, TOP), jnp.float32) ** steps_of(arg_keys[8], (TOKENS, TOP), ((0, 32),), -0.2, 0.2), 0.2, 1.0)
    gate_weight = centred(arg_keys[9], (EXPERTS, D, FF), (D // 6) ** -0.5, 0.3125, ((0, 4), (2, 8)))
    up_weight = centred(arg_keys[10], (EXPERTS, D, FF), (D // 6) ** -0.5, 0.3125, ((0, 4), (2, 8)))
    down_weight = centred(arg_keys[11], (EXPERTS, FF, D), (FF * 4) ** -0.5, 0.0625, ((0, 4), (1, 8)))
    return {"query_heads": query_heads, "key_heads": key_heads, "value_heads": value_heads, "sink_logit": sink_logit, "residual": residual, "out_weight": out_weight, "norm_gain": norm_gain, "routes": routes, "route_weight": route_weight, "gate_weight": gate_weight, "up_weight": up_weight, "down_weight": down_weight}


eps = 1e-06
clamp_limit = 7.0
sigmoid_alpha = 1.702

def attention(query_heads, key_heads, value_heads, sink_logit):
    block_count = TOKENS // WINDOW
    group_size = HQ // KVH
    queries = query_heads.reshape(block_count, WINDOW, KVH, group_size, HEAD).transpose(2, 0, 1, 3, 4)
    key_blocks = key_heads.reshape(block_count, WINDOW, KVH, HEAD).transpose(2, 0, 1, 3)
    value_blocks = value_heads.reshape(block_count, WINDOW, KVH, HEAD).transpose(2, 0, 1, 3)
    sinks = sink_logit.reshape(KVH, group_size)
    query_pos = jnp.arange(WINDOW)[:, None]
    key_col = jnp.arange(2 * WINDOW)[None, :]
    distance = query_pos + WINDOW - key_col
    block_ids = jnp.arange(block_count)[:, None, None]
    key_global = (block_ids - 1) * WINDOW + key_col[None]
    allowed = (distance[None] >= 0) & (distance[None] < WINDOW) & (key_global >= 0)

    def banded(current):
        earlier = jnp.concatenate([jnp.zeros_like(current[:1]), current[:-1]], axis=0)
        return jnp.concatenate([earlier, current], axis=1)

    def one_head(items):
        query_part, key_part, value_part, sink_part = items
        key_band = banded(key_part).astype(jnp.float32)
        value_band = banded(value_part).astype(jnp.float32)
        scores = jnp.einsum('nqgd,nkd->ngqk', query_part.astype(jnp.float32), key_band) * HEAD ** (-0.5)
        logits = jnp.where(allowed[:, None], scores, -jnp.inf)
        sink_term = sink_part[None, :, None, None]
        row_max = jnp.maximum(lax.optimization_barrier(jnp.max(logits, axis=-1, keepdims=True)), sink_term)
        raised = jnp.exp(logits - row_max)
        weights_bf = (raised / (lax.optimization_barrier(jnp.sum(raised, axis=-1, keepdims=True)) + jnp.exp(sink_term - row_max))).astype(jnp.bfloat16)
        result = jnp.einsum('ngqk,nkd->nqgd', weights_bf.astype(jnp.float32), value_band)
        return result.astype(jnp.bfloat16)
    heads_out = lax.map(one_head, (queries, key_blocks, value_blocks, sinks))
    return heads_out.transpose(1, 2, 0, 3, 4).reshape(TOKENS, HQ * HEAD)

def reference(query_heads, key_heads, value_heads, sink_logit, residual, out_weight, norm_gain, routes, route_weight, gate_weight, up_weight, down_weight):
    attended = attention(query_heads, key_heads, value_heads, sink_logit)
    mixed = jnp.dot(attended, out_weight, preferred_element_type=jnp.float32)
    stream = (residual.astype(jnp.float32) + mixed).astype(jnp.bfloat16)
    stream32 = stream.astype(jnp.float32)
    normed = (stream32 * lax.rsqrt(lax.optimization_barrier(jnp.mean(stream32 * stream32, axis=-1, keepdims=True)) + eps) * norm_gain).astype(jnp.bfloat16)
    device_count = N_SP * N_TP
    choice_rows = routes.reshape(device_count, TOK_DEV * TOP)
    one_hot = (choice_rows[:, :, None] == jnp.arange(EXPERTS, dtype=jnp.int32)[None, None, :]).astype(jnp.int32)
    ranked = lax.optimization_barrier(jnp.sum((jnp.cumsum(one_hot, axis=1) - one_hot) * one_hot, axis=-1)).astype(jnp.int32)
    device_ids = jnp.arange(device_count, dtype=jnp.int32)[:, None]
    token_ids = device_ids * TOK_DEV + jnp.arange(TOK_DEV * TOP, dtype=jnp.int32)[None, :] // TOP
    table = jnp.full((device_count, EXPERTS, CAP), TOKENS, dtype=jnp.int32)
    table = table.at[device_ids, choice_rows, ranked].set(token_ids.astype(jnp.int32))
    padded = jnp.concatenate([normed, jnp.zeros((1, D), jnp.bfloat16)], axis=0)

    def run_expert(index):
        row_block = padded[table[:, index, :].reshape(-1)]
        gate_pre = jnp.dot(row_block, gate_weight[index], preferred_element_type=jnp.float32)
        upward = jnp.dot(row_block, up_weight[index], preferred_element_type=jnp.float32)
        capped = jnp.minimum(gate_pre, clamp_limit)
        linear = jnp.clip(upward, -clamp_limit, clamp_limit)
        hidden = (capped * jax.nn.sigmoid(sigmoid_alpha * capped) * (linear + 1.0)).astype(jnp.bfloat16)
        pieces = hidden.astype(jnp.float32).reshape(device_count * CAP, N_TP, FF // N_TP)
        down_pieces = down_weight[index].astype(jnp.float32).reshape(N_TP, FF // N_TP, D)
        partial_value = jnp.einsum('rjf,jfd->jrd', pieces, down_pieces).astype(jnp.bfloat16)
        return lax.optimization_barrier(jnp.sum(partial_value.astype(jnp.float32), axis=0)).astype(jnp.bfloat16)
    outputs = lax.map(run_expert, jnp.arange(EXPERTS, dtype=jnp.int32))
    shaped = outputs.reshape(EXPERTS, device_count, CAP, D)
    picked = shaped[choice_rows, device_ids, ranked]
    combined = lax.optimization_barrier(jnp.sum(picked.astype(jnp.float32).reshape(TOKENS, TOP, D) * route_weight[:, :, None], axis=1))
    return (stream32 + combined).astype(jnp.bfloat16)
```

```python
import functools
import math

import jax
import jax.numpy as jnp
from jax import lax
from jax.experimental import pallas as pl
from jax.experimental.pallas import tpu as pltpu
from jax.sharding import PartitionSpec as P

HEAD = 64
WINDOW = 128


eps = 1e-06
clamp_limit = 7.0
sigmoid_alpha = 1.702


MESH = pl.DeviceIdType.MESH
CORES = 2
LANES = 128
MIB = 1024 * 1024


def round_up(value, unit):
    return (value + unit - 1) // unit * unit


def place():
    tp = lax.axis_index("tp")
    return lax.axis_index("sp"), tp // CORES, lax.rem(tp, CORES)


def partner_of(sp, d, n_sp):
    if n_sp & (n_sp - 1):
        return lax.rem(sp + d, n_sp)
    total, bit = 0, 1
    while bit < n_sp:
        total = total + lax.rem(sp // bit + d // bit, 2) * bit
        bit *= 2
    return total


def source_of(sp, d, n_sp):
    if n_sp & (n_sp - 1):
        return lax.rem(sp + n_sp - d, n_sp)
    return partner_of(sp, d, n_sp)


def greet(n_sp, nz, sp, z, c):
    barrier = pltpu.get_barrier_semaphore()
    tp = z * CORES + c
    for d in range(1, n_sp):
        pl.semaphore_signal(
            barrier, inc=1, device_id=(partner_of(sp, d, n_sp), tp), device_id_type=MESH
        )
    pl.semaphore_signal(
        barrier, inc=1, device_id=(sp, z * CORES + 1 - c), device_id_type=MESH
    )

    @pl.when(z > 0)
    def _():
        pl.semaphore_signal(barrier, inc=1, device_id=(sp, tp - CORES), device_id_type=MESH)

    @pl.when(z < nz - 1)
    def _():
        pl.semaphore_signal(barrier, inc=1, device_id=(sp, tp + CORES), device_id_type=MESH)

    beside = jnp.where(z > 0, 1, 0) + jnp.where(z < nz - 1, 1, 0)
    pl.semaphore_wait(barrier, n_sp + beside)


def send(src, dst, send_sem, recv_sem, device):
    return pltpu.make_async_remote_copy(
        src_ref=src,
        dst_ref=dst,
        send_sem=send_sem,
        recv_sem=recv_sem,
        device_id=device,
        device_id_type=MESH,
    )


def dot(a, b):
    return jnp.dot(a, b, preferred_element_type=jnp.float32)


def tiled(extent, tile, visit):
    def one(t, carry):
        visit(pl.ds(pl.multiple_of(t * tile, tile), tile))
        return carry

    lax.fori_loop(0, extent // tile, one, 0)


def both_sides(z, nz, away, visit):
    def one(behind, carry):
        block = z + away * (1 - 2 * behind)

        @pl.when((block >= 0) & (block < nz))
        def _():
            visit(block, behind)

        return carry

    lax.fori_loop(0, 2, one, 0)


def expert_kernel(
    n_sp, nz, normed, stream, onehot, share, gate, up, down, out,
    gate_v, up_v, down_v, toks, comp_a, comp_b, rows_a, rows_b, hid,
    sums_a, sums_b, back_a, back_b, a_out, a_up, a_dn, b_up, b_dn,
    w_l, w_s, w_r, ru_s, ru_r, rd_s, rd_r, xa_s, xa_r, xb_s, xb_r,
    bu_s, bu_r, bd_s, bd_r, ya_s, ya_r, yb_s, yb_r,
    au_s, au_r, ad_s, ad_r, cu_s, cu_r, cd_s, cd_r,
):
    sp, z, c = place()
    tp = z * CORES + c
    peer_core = (sp, z * CORES + 1 - c)
    above = (sp, lax.rem(z + 1, nz) * CORES + c)
    below = (sp, lax.rem(z + nz - 1, nz) * CORES + c)
    capp, ka, kb = rows_a.shape[2], rows_a.shape[3], rows_b.shape[3]
    na, nb = sums_a.shape[3], sums_b.shape[3]
    slots = n_sp * capp
    units = gate.shape[1]
    tile = math.gcd(math.gcd(ka, kb), 256)
    wide = math.gcd(math.gcd(na, nb), 512)
    greet(n_sp, nz, sp, z, c)

    def raw_above(block, src):
        return send(src, toks.at[block], ru_s.at[block], ru_r.at[block], above)

    def raw_below(block, src):
        return send(src, toks.at[block], rd_s.at[block], rd_r.at[block], below)

    own_raw = normed.at[:, pl.ds(0, ka)]

    @pl.when(z < nz - 1)
    def _():
        raw_above(z, own_raw).start()

    @pl.when(z > 0)
    def _():
        raw_below(z, own_raw).start()

    mine = pl.ds(pl.multiple_of(c * units, units), units)
    held = (gate_v.at[:, mine], up_v.at[:, mine], down_v.at[mine, :])
    locals_ = [
        pltpu.make_async_copy(src, dst, w_l.at[i])
        for i, (src, dst) in enumerate(zip((gate, up, down), held))
    ]
    lent = [
        send(src, dst, w_s.at[i], w_r.at[i], peer_core)
        for i, (src, dst) in enumerate(zip((gate, up, down), held))
    ]

    def xa_to(block, d):
        e = partner_of(sp, d, n_sp)
        return send(
            comp_a.at[block, e], rows_a.at[block, sp], xa_s.at[block, d], xa_r.at[block, d], (e, tp)
        )

    def xa_from(block, d):
        e = source_of(sp, d, n_sp)
        return send(
            comp_a.at[block, e], rows_a.at[block, e], xa_s.at[block, d], xa_r.at[block, d], (e, tp)
        )

    def xb_to(d):
        e = partner_of(sp, d, n_sp)
        return send(comp_b.at[e], rows_b.at[z, sp], xb_s.at[d], xb_r.at[d], (e, tp))

    def xb_from(d):
        e = source_of(sp, d, n_sp)
        return send(comp_b.at[e], rows_b.at[z, e], xb_s.at[d], xb_r.at[d], (e, tp))

    def b_above(block):
        return send(rows_b.at[block], rows_b.at[block], bu_s.at[block], bu_r.at[block], above)

    def b_below(block):
        return send(rows_b.at[block], rows_b.at[block], bd_s.at[block], bd_r.at[block], below)

    def deal_b(cols):
        picked = dot(onehot[z], normed[:, pl.ds(pl.multiple_of(ka + cols.start, tile), tile)])
        comp_b[:, :, cols] = picked.astype(jnp.bfloat16).reshape(n_sp, capp, tile)

    tiled(kb, tile, deal_b)
    for d in range(1, n_sp):
        xb_to(d).start()
    rows_b[z, sp] = comp_b[sp]

    def deal(block, src):
        def one(cols):
            picked = dot(onehot[block], src[:, cols])
            comp_a[block, :, :, cols] = picked.astype(jnp.bfloat16).reshape(n_sp, capp, tile)

        tiled(ka, tile, one)
        for d in range(1, n_sp):
            xa_to(block, d).start()
        rows_a[block, sp] = comp_a[block, sp]

    deal(z, normed)
    for copy in locals_ + lent:
        copy.start()

    def spread_own():
        for d in range(1, n_sp):
            xb_from(d).wait_recv()

        @pl.when(z < nz - 1)
        def _():
            b_above(z).start()

        @pl.when(z > 0)
        def _():
            b_below(z).start()

    def gather_raw(block, behind):
        @pl.when(behind == 1)
        def _():
            raw_above(block, toks.at[block]).wait_recv()

            @pl.when(z < nz - 1)
            def _():
                raw_above(block, toks.at[block]).start()

        @pl.when(behind == 0)
        def _():
            raw_below(block, toks.at[block]).wait_recv()

            @pl.when(z > 0)
            def _():
                raw_below(block, toks.at[block]).start()

        deal(block, toks.at[block])

    def gather_b(block, behind):
        @pl.when(behind == 1)
        def _():
            b_above(block).wait_recv()

            @pl.when(z < nz - 1)
            def _():
                b_above(block).start()

        @pl.when(behind == 0)
        def _():
            b_below(block).wait_recv()

            @pl.when(z > 0)
            def _():
                b_below(block).start()

    unit = min(256, CORES * units)

    def serve(block, behind):
        for d in range(1, n_sp):
            xa_from(block, d).wait_recv()

        def one(cols):
            tile_a = rows_a[block].reshape(slots, ka)
            tile_b = rows_b[block].reshape(slots, kb)
            gate_pre = dot(tile_a, gate_v[:ka, cols]) + dot(tile_b, gate_v[ka:, cols])
            upward = dot(tile_a, up_v[:ka, cols]) + dot(tile_b, up_v[ka:, cols])
            capped = jnp.minimum(gate_pre, clamp_limit)
            linear = jnp.clip(upward, -clamp_limit, clamp_limit)
            gated = capped * jax.nn.sigmoid(sigmoid_alpha * capped)
            hid[:, cols] = (gated * (linear + 1.0)).astype(jnp.bfloat16)

        tiled(CORES * units, unit, one)

        def part_a(cols):
            part = dot(hid[...], down_v[:, cols]).astype(jnp.bfloat16)
            sums_a[block, :, :, cols] = part.reshape(n_sp, capp, wide)

        def part_b(cols):
            at = pl.ds(pl.multiple_of(na + cols.start, wide), wide)
            part = dot(hid[...], down_v[:, at]).astype(jnp.bfloat16)
            sums_b[block, :, :, cols] = part.reshape(n_sp, capp, wide)

        tiled(na, wide, part_a)
        tiled(nb, wide, part_b)

    def arrive(i, carry):
        both_sides(z, nz, i, gather_raw)

        @pl.when(i == 1)
        def _():
            spread_own()

        @pl.when(i > 1)
        def _():
            both_sides(z, nz, i - 1, gather_b)

        @pl.when(i == min(2, nz - 1))
        def _():
            for copy in locals_:
                copy.wait()
            for copy in lent:
                copy.wait()

        @pl.when(i > 1)
        def _():
            both_sides(z, nz, i - 2, lambda block, behind: serve_once(block, behind, i - 2))

        return carry

    def serve_once(block, behind, away):
        @pl.when((away > 0) | (behind == 0))
        def _():
            serve(block, behind)

    lax.fori_loop(1, nz, arrive, 0)
    both_sides(z, nz, nz - 2, lambda block, behind: serve_once(block, behind, nz - 2))
    both_sides(z, nz, nz - 1, gather_b)
    both_sides(z, nz, nz - 1, serve)

    def ya_to(block, d):
        e = partner_of(sp, d, n_sp)
        return send(
            sums_a.at[block, e], back_a.at[block, sp], ya_s.at[block, d], ya_r.at[block, d], (e, tp)
        )

    def ya_from(block, d):
        e = source_of(sp, d, n_sp)
        return send(
            sums_a.at[block, e], back_a.at[block, e], ya_s.at[block, d], ya_r.at[block, d], (e, tp)
        )

    def yb_to(d):
        e = partner_of(sp, d, n_sp)
        return send(sums_b.at[z, e], back_b.at[sp], yb_s.at[d], yb_r.at[d], (e, tp))

    def yb_from(d):
        e = source_of(sp, d, n_sp)
        return send(sums_b.at[z, e], back_b.at[e], yb_s.at[d], yb_r.at[d], (e, tp))

    def a_above(block):
        return send(a_out.at[block], a_up.at[block], au_s.at[block], au_r.at[block], above)

    def a_below(block):
        return send(a_out.at[block], a_dn.at[block], ad_s.at[block], ad_r.at[block], below)

    def c_above(block):
        return send(sums_b.at[block], b_up.at[block], cu_s.at[block], cu_r.at[block], above)

    def c_below(block):
        return send(sums_b.at[block], b_dn.at[block], cd_s.at[block], cd_r.at[block], below)

    def push(block, behind):
        for d in range(1, n_sp):
            ya_to(block, d).start()
        back_a[block, sp] = sums_a[block, sp]

    def far_push(i, carry):
        both_sides(z, nz, nz - 1 - i, push)
        return carry

    lax.fori_loop(0, nz - 1, far_push, 0)
    push(z, 0)

    def add_b(block, arrived):
        total = sums_b[block].astype(jnp.float32) + arrived[block].astype(jnp.float32)
        sums_b[block] = total.astype(jnp.bfloat16)

    def relay_b(block, behind):
        @pl.when(behind == 0)
        def _():
            @pl.when(z > 0)
            def _():
                c_above(block).wait_recv()
                add_b(block, b_up)

            c_above(block).start()

        @pl.when(behind == 1)
        def _():
            @pl.when(z < nz - 1)
            def _():
                c_below(block).wait_recv()
                add_b(block, b_dn)

            c_below(block).start()

    def settle_b():
        @pl.when(z > 0)
        def _():
            c_above(z).wait_recv()
            add_b(z, b_up)

        @pl.when(z < nz - 1)
        def _():
            c_below(z).wait_recv()
            add_b(z, b_dn)

        for d in range(1, n_sp):
            yb_to(d).start()
        back_b[sp] = sums_b[z, sp]

    def combined(block, cols):
        return dot(share[block], back_a[block, :, :, cols].reshape(slots, wide))

    def relay_a(block, behind):
        for d in range(1, n_sp):
            ya_from(block, d).wait_recv()

        @pl.when(behind == 0)
        def _():
            @pl.when(z > 0)
            def _():
                a_above(block).wait_recv()

            def one(cols):
                total = combined(block, cols)
                total = jnp.where(z > 0, total + a_up[block, :, cols].astype(jnp.float32), total)
                a_out[block, :, cols] = total.astype(jnp.bfloat16)

            tiled(na, wide, one)
            a_above(block).start()

        @pl.when(behind == 1)
        def _():
            @pl.when(z < nz - 1)
            def _():
                a_below(block).wait_recv()

            def one(cols):
                total = combined(block, cols)
                total = jnp.where(
                    z < nz - 1, total + a_dn[block, :, cols].astype(jnp.float32), total
                )
                a_out[block, :, cols] = total.astype(jnp.bfloat16)

            tiled(na, wide, one)
            a_below(block).start()

    both_sides(z, nz, nz - 1, relay_b)

    def relay(i, carry):
        away = nz - 1 - i

        @pl.when(away > 1)
        def _():
            both_sides(z, nz, away - 1, relay_b)

        @pl.when(away == 1)
        def _():
            settle_b()

        both_sides(z, nz, away, relay_a)
        return carry

    lax.fori_loop(0, nz - 1, relay, 0)

    for d in range(1, n_sp):
        yb_from(d).wait_recv()

    def final_b(cols):
        at = pl.ds(pl.multiple_of(na + cols.start, wide), wide)
        total = dot(share[z], back_b[:, :, cols].reshape(slots, wide))
        out[:, at] = (stream[:, at].astype(jnp.float32) + total).astype(jnp.bfloat16)

    tiled(nb, wide, final_b)
    for d in range(1, n_sp):
        ya_from(z, d).wait_recv()

    @pl.when(z > 0)
    def _():
        a_above(z).wait_recv()

    @pl.when(z < nz - 1)
    def _():
        a_below(z).wait_recv()

    def final_a(cols):
        total = combined(z, cols)
        total = jnp.where(z > 0, total + a_up[z, :, cols].astype(jnp.float32), total)
        total = jnp.where(z < nz - 1, total + a_dn[z, :, cols].astype(jnp.float32), total)
        out[:, cols] = (stream[:, cols].astype(jnp.float32) + total).astype(jnp.bfloat16)

    tiled(na, wide, final_a)

    for d in range(1, n_sp):
        xb_to(d).wait_send()
        yb_to(d).wait_send()

    def drain_exchange(block):
        for d in range(1, n_sp):
            xa_to(block, d).wait_send()
            ya_to(block, d).wait_send()

    drain_exchange(z)

    @pl.when(z < nz - 1)
    def _():
        raw_above(z, own_raw).wait_send()
        b_above(z).wait_send()

    @pl.when(z > 0)
    def _():
        raw_below(z, own_raw).wait_send()
        b_below(z).wait_send()

    def drain(block, behind):
        drain_exchange(block)

        @pl.when(behind == 0)
        def _():
            a_above(block).wait_send()
            c_above(block).wait_send()

        @pl.when(behind == 1)
        def _():
            a_below(block).wait_send()
            c_below(block).wait_send()

        @pl.when((behind == 1) & (z < nz - 1))
        def _():
            raw_above(block, toks.at[block]).wait_send()
            b_above(block).wait_send()

        @pl.when((behind == 0) & (z > 0))
        def _():
            raw_below(block, toks.at[block]).wait_send()
            b_below(block).wait_send()

    def drain_all(i, carry):
        both_sides(z, nz, i, drain)
        return carry

    lax.fori_loop(1, nz, drain_all, 0)


def split_columns(width, share):
    return max(256, min(width - 256, int(width * share) // 256 * 256))


def experts(normed, stream, onehot, share, gate_local, up_local, down_local):
    n_sp = lax.axis_size("sp")
    nz = lax.axis_size("tp") // CORES
    tok, width = normed.shape
    units = gate_local.shape[1]
    slots = onehot.shape[1]
    capp = slots // n_sp
    ka = split_columns(width, 0.75)
    na = split_columns(width, 0.75)
    kb, nb = width - ka, width - na
    vmem = pl.BlockSpec(memory_space=pltpu.VMEM)
    anywhere = pl.BlockSpec(memory_space=pl.ANY)
    dma = pltpu.SemaphoreType.DMA
    bf = jnp.bfloat16
    line = [dma((nz,))] * 4
    return pl.pallas_call(
        functools.partial(expert_kernel, n_sp, nz),
        out_shape=jax.ShapeDtypeStruct((tok, width), bf),
        in_specs=[vmem] * 4 + [anywhere] * 3,
        out_specs=vmem,
        scratch_shapes=[
            pltpu.VMEM((width, CORES * units), bf),
            pltpu.VMEM((width, CORES * units), bf),
            pltpu.VMEM((CORES * units, width), bf),
            pltpu.VMEM((nz, tok, ka), bf),
            pltpu.VMEM((nz, n_sp, capp, ka), bf),
            pltpu.VMEM((n_sp, capp, kb), bf),
            pltpu.VMEM((nz, n_sp, capp, ka), bf),
            pltpu.VMEM((nz, n_sp, capp, kb), bf),
            pltpu.VMEM((slots, CORES * units), bf),
            pltpu.VMEM((nz, n_sp, capp, na), bf),
            pltpu.VMEM((nz, n_sp, capp, nb), bf),
            pltpu.VMEM((nz, n_sp, capp, na), bf),
            pltpu.VMEM((n_sp, capp, nb), bf),
            pltpu.VMEM((nz, tok, na), bf),
            pltpu.VMEM((nz, tok, na), bf),
            pltpu.VMEM((nz, tok, na), bf),
            pltpu.VMEM((nz, n_sp, capp, nb), bf),
            pltpu.VMEM((nz, n_sp, capp, nb), bf),
        ]
        + [dma((3,))] * 3
        + line
        + [dma((nz, n_sp))] * 2
        + [dma((n_sp,))] * 2
        + line
        + [dma((nz, n_sp))] * 2
        + [dma((n_sp,))] * 2
        + line
        + line,
        compiler_params=pltpu.CompilerParams(
            collective_id=0, has_side_effects=True, vmem_limit_bytes=54 * MIB
        ),
        name="experts",
    )(normed, stream, onehot, share, gate_local, up_local, down_local)


def tables(n_sp, nz, tok, capp, c, routes, rw_all, onehot, share):
    choose = routes.shape[0]
    epad = round_up(n_sp, 16)
    earlier = lax.broadcasted_iota(jnp.int32, (tok, tok), 0) < lax.broadcasted_iota(
        jnp.int32, (tok, tok), 1
    )
    earlier = jnp.where(earlier, 1.0, 0.0).astype(jnp.bfloat16)
    same = lax.broadcasted_iota(jnp.int32, (tok, tok), 0) == lax.broadcasted_iota(
        jnp.int32, (tok, tok), 1
    )
    same = jnp.where(same, 1.0, 0.0).astype(jnp.bfloat16)
    which = lax.broadcasted_iota(jnp.int32, (epad, tok), 0)
    place_in = lax.broadcasted_iota(jnp.int32, (capp, tok), 0).astype(jnp.float32)
    for b in range(nz):
        first = routes[:, (CORES * b) * tok : (CORES * b + 1) * tok]
        second = routes[:, (CORES * b + 1) * tok : (CORES * b + 2) * tok]
        ids = jnp.where(c == 0, first, second)
        weight = jnp.zeros((epad, tok), jnp.float32)
        member = jnp.zeros((epad, tok), jnp.float32)
        for m in range(choose):
            named = ids[m : m + 1, :] == which
            member = jnp.where(named, 1.0, member)
            weight = jnp.where(named, rw_all[b, m : m + 1, :tok], weight)
        rank = dot(member.astype(jnp.bfloat16), earlier)
        rank = jnp.where(member > 0.0, rank, -1.0)
        shares = []
        for e in range(n_sp):
            hit = place_in == rank[e : e + 1, :]
            onehot[b, e * capp : (e + 1) * capp, :] = jnp.where(hit, 1.0, 0.0).astype(jnp.bfloat16)
            shares.append(jnp.where(hit, weight[e : e + 1, :], 0.0).astype(jnp.bfloat16))
        turned = lax.dot_general(
            same,
            jnp.concatenate(shares, axis=0),
            (((1,), (1,)), ((), ())),
            preferred_element_type=jnp.float32,
        )
        share[b] = turned.astype(jnp.bfloat16)


def front_kernel(
    n_sp, n_tp, tok, capp, q, k, v, sink, residual, weight, gain, routes, rweight,
    normed, stream, onehot, share,
    q_all, k_all, v_all, k_tail, v_tail, att, got, w_all, res, acc, rw_src, rw_all,
    in_s, o_s, t_s, t_r, a_s, a_r, g_s, g_r,
):
    sp, z, c = place()
    tp = z * CORES + c
    nz = n_tp // CORES
    span, kv_cols = k.shape
    cols = q.shape[1]
    width = weight.shape[1]
    kv_local = kv_cols // HEAD
    group = cols // kv_cols
    blocks = span // WINDOW
    pieces = WINDOW // tok
    scale = HEAD ** (-0.5)
    body = pl.ds(WINDOW, span)
    copies = [
        pltpu.make_async_copy(k, k_all.at[body], in_s.at[0]),
        pltpu.make_async_copy(v, v_all.at[body], in_s.at[1]),
        pltpu.make_async_copy(q, q_all, in_s.at[2]),
        pltpu.make_async_copy(residual, res, in_s.at[3]),
    ]
    for copy in copies:
        copy.start()

    def out_rows(p):
        rows = pl.ds(pl.multiple_of(p * cols, cols), cols)
        return pltpu.make_async_copy(weight.at[rows], w_all.at[rows], o_s.at[p])

    barrier = pltpu.get_barrier_semaphore()
    for d in range(1, n_tp):
        pl.semaphore_signal(
            barrier, inc=1, device_id=(sp, lax.rem(tp + d, n_tp)), device_id_type=MESH
        )

    @pl.when(sp > 0)
    def _():
        pl.semaphore_signal(barrier, inc=1, device_id=(sp - 1, tp), device_id_type=MESH)

    @pl.when(sp < n_sp - 1)
    def _():
        pl.semaphore_signal(barrier, inc=1, device_id=(sp + 1, tp), device_id_type=MESH)

    rw_src[...] = jnp.zeros_like(rw_src)
    rw_src[: rweight.shape[0], :tok] = rweight[...]
    rw_all[z] = rw_src[...]
    beside = jnp.where(sp > 0, 1, 0) + jnp.where(sp < n_sp - 1, 1, 0)
    pl.semaphore_wait(barrier, n_tp - 1 + beside)
    ahead = (lax.rem(sp + 1, n_sp), tp)
    last = pl.ds(span, WINDOW)
    tails = (
        send(k_all.at[last], k_tail, t_s.at[0], t_r.at[0], ahead),
        send(v_all.at[last], v_tail, t_s.at[1], t_r.at[1], ahead),
    )
    copies[0].wait()
    copies[1].wait()

    @pl.when(sp < n_sp - 1)
    def _():
        for copy in tails:
            copy.start()

    def tell(d):
        there = lax.rem(z + d, nz)
        return send(rw_src, rw_all.at[z], g_s.at[d], g_r.at[z], (sp, there * CORES + c))

    def told(d):
        there = lax.rem(z + d, nz)
        return send(rw_src, rw_all.at[there], g_s.at[d], g_r.at[there], (sp, there * CORES + c))

    for d in range(1, nz):
        tell(d).start()
    copies[2].wait()
    for p in range(n_tp):
        out_rows(p).start()

    row = lax.broadcasted_iota(jnp.int32, (WINDOW, 2 * WINDOW), 0)
    col = lax.broadcasted_iota(jnp.int32, (WINDOW, 2 * WINDOW), 1)
    distance = row + WINDOW - col
    banded = (distance >= 0) & (distance < WINDOW)
    low = z < nz // 2
    half = max(1, blocks // 2)

    def to_owner(dest):
        at = pl.multiple_of(dest * tok, tok)
        return send(
            att.at[pl.ds(at, tok)], got.at[tp], a_s.at[dest], a_r.at[tp], (sp, dest)
        )

    def attend(i, carry):
        turned = jnp.where(i < half, lax.rem(i + 1, half), i)
        block = jnp.where(low, blocks - 1 - i, turned)

        @pl.when(block == 0)
        def _():
            @pl.when(sp > 0)
            def _():
                for copy in tails:
                    copy.wait_recv()
                k_all[pl.ds(0, WINDOW), :] = k_tail[...]
                v_all[pl.ds(0, WINDOW), :] = v_tail[...]

            @pl.when(sp == 0)
            def _():
                k_all[pl.ds(0, WINDOW), :] = jnp.zeros((WINDOW, kv_cols), jnp.bfloat16)
                v_all[pl.ds(0, WINDOW), :] = jnp.zeros((WINDOW, kv_cols), jnp.bfloat16)

        at = pl.multiple_of(block * WINDOW, WINDOW)
        start = jnp.where((sp == 0) & (block == 0), WINDOW, 0)
        allowed = banded & (col >= start)
        band = pl.ds(at, 2 * WINDOW)
        for g in range(kv_local):
            keys = k_all[band, g * HEAD : (g + 1) * HEAD]
            values = v_all[band, g * HEAD : (g + 1) * HEAD]
            heads = []
            for m in range(group):
                h = g * group + m
                query = q_all[pl.ds(at, WINDOW), h * HEAD : (h + 1) * HEAD] * jnp.bfloat16(scale)
                scores = lax.dot_general(
                    query, keys, (((1,), (1,)), ((), ())), preferred_element_type=jnp.float32
                )
                logits = jnp.where(allowed, scores, -jnp.inf)
                top = jnp.maximum(jnp.max(logits, axis=-1, keepdims=True), sink[h])
                raised = jnp.exp(logits - top)
                total = jnp.sum(raised, axis=-1, keepdims=True) + jnp.exp(sink[h] - top)
                probs = (raised * (1.0 / total)).astype(jnp.bfloat16)
                heads.append(dot(probs, values))
            att[pl.ds(at, WINDOW), g * group * HEAD : (g + 1) * group * HEAD] = jnp.concatenate(
                heads, axis=1
            ).astype(jnp.bfloat16)
        for piece in range(pieces):
            dest = block * pieces + piece

            @pl.when(dest != tp)
            def _():
                to_owner(dest).start()

        return carry

    lax.fori_loop(0, blocks, attend, 0)
    for d in range(1, nz):
        told(d).wait_recv()
    tables(n_sp, nz, tok, capp, c, routes, rw_all, onehot, share)
    got[tp] = att[pl.ds(pl.multiple_of(tp * tok, tok), tok), :]
    copies[3].wait()
    wide = math.gcd(width, 512)

    def begin(at):
        acc[:, at] = res[:, at].astype(jnp.float32)

    tiled(width, wide, begin)
    for p in range(n_tp):
        out_rows(p).wait()

    def mix(i, carry):
        p = jnp.where(low, n_tp - 1 - i, i)

        @pl.when(tp != p)
        def _():
            send(att.at[pl.ds(0, tok)], got.at[p], a_s.at[p], a_r.at[p], (sp, p)).wait_recv()

        rows = pl.ds(pl.multiple_of(p * cols, cols), cols)

        def one(at):
            acc[:, at] = acc[:, at] + dot(got[p], w_all[rows, at])

        tiled(width, wide, one)
        return carry

    lax.fori_loop(0, n_tp, mix, 0)
    squares = jnp.zeros((tok, 1), jnp.float32)
    for t in range(width // wide):
        at = slice(t * wide, (t + 1) * wide)
        held = acc[:, at].astype(jnp.bfloat16)
        stream[:, at] = held
        held32 = held.astype(jnp.float32)
        squares = squares + jnp.sum(held32 * held32, axis=-1, keepdims=True)
    root = lax.rsqrt(squares * (1.0 / width) + eps)
    for t in range(width // wide):
        at = slice(t * wide, (t + 1) * wide)
        normed[:, at] = (stream[:, at].astype(jnp.float32) * root * gain[:, at]).astype(
            jnp.bfloat16
        )
    for p in range(n_tp):
        @pl.when(tp != p)
        def _():
            to_owner(p).wait_send()

    for d in range(1, nz):
        tell(d).wait_send()

    @pl.when(sp < n_sp - 1)
    def _():
        for copy in tails:
            copy.wait_send()


def front(query_heads, key_heads, value_heads, sink_logit, residual, out_weight, norm_gain, routes,
          route_weight):
    n_sp, n_tp = lax.axis_size("sp"), lax.axis_size("tp")
    nz = n_tp // CORES
    span, cols = query_heads.shape
    kv_cols = key_heads.shape[1]
    tok, width = residual.shape
    choose = routes.shape[1]
    capp = round_up(max(2, 5 * tok * choose // (4 * n_sp)), 16)
    slots = n_sp * capp
    vmem = pl.BlockSpec(memory_space=pltpu.VMEM)
    anywhere = pl.BlockSpec(memory_space=pl.ANY)
    smem = pl.BlockSpec(memory_space=pltpu.SMEM)
    dma = pltpu.SemaphoreType.DMA
    bf = jnp.bfloat16
    return pl.pallas_call(
        functools.partial(front_kernel, n_sp, n_tp, tok, capp),
        out_shape=(
            jax.ShapeDtypeStruct((tok, width), bf),
            jax.ShapeDtypeStruct((tok, width), bf),
            jax.ShapeDtypeStruct((nz, slots, tok), bf),
            jax.ShapeDtypeStruct((nz, tok, slots), bf),
        ),
        in_specs=[anywhere] * 3 + [smem] + [anywhere] * 2 + [vmem] * 3,
        out_specs=(vmem,) * 4,
        scratch_shapes=[
            pltpu.VMEM((span, cols), bf),
            pltpu.VMEM((span + WINDOW, kv_cols), bf),
            pltpu.VMEM((span + WINDOW, kv_cols), bf),
            pltpu.VMEM((WINDOW, kv_cols), bf),
            pltpu.VMEM((WINDOW, kv_cols), bf),
            pltpu.VMEM((span, cols), bf),
            pltpu.VMEM((n_tp, tok, cols), bf),
            pltpu.VMEM((n_tp * cols, width), bf),
            pltpu.VMEM((tok, width), bf),
            pltpu.VMEM((tok, width), jnp.float32),
            pltpu.VMEM((8, LANES), jnp.float32),
            pltpu.VMEM((nz, 8, LANES), jnp.float32),
            dma((4,)),
            dma((n_tp,)),
            dma((2,)),
            dma((2,)),
            dma((n_tp,)),
            dma((n_tp,)),
            dma((nz,)),
            dma((nz,)),
        ],
        compiler_params=pltpu.CompilerParams(
            collective_id=2, has_side_effects=True, vmem_limit_bytes=32 * MIB
        ),
        name="front",
    )(
        query_heads, key_heads, value_heads, sink_logit, residual, out_weight,
        norm_gain.reshape(1, -1), routes.T, route_weight.T,
    )


def local(
    query_heads,
    key_heads,
    value_heads,
    sink_logit,
    residual,
    out_weight,
    norm_gain,
    routes,
    route_weight,
    gate_weight,
    up_weight,
    down_weight,
):
    normed, stream, onehot, share = front(
        query_heads, key_heads, value_heads, sink_logit, residual, out_weight, norm_gain, routes,
        route_weight,
    )
    return experts(normed, stream, onehot, share, gate_weight[0], up_weight[0], down_weight[0])


def solution(mesh):
    placed = (
        P("sp", "tp"),
        P("sp", "tp"),
        P("sp", "tp"),
        P("tp"),
        P(("sp", "tp"), None),
        P(),
        P(),
        P("sp", None),
        P(("sp", "tp"), None),
        P("sp", None, "tp"),
        P("sp", None, "tp"),
        P("sp", "tp", None),
    )
    return jax.shard_map(
        local, mesh=mesh, in_specs=placed, out_specs=P(("sp", "tp"), None), check_vma=False
    )
```

```python
import functools
import math

import jax
import jax.numpy as jnp
from jax import lax
from jax.experimental import pallas as pl
from jax.experimental.pallas import tpu as pltpu
from jax.sharding import PartitionSpec as P

HEAD = 64
WINDOW = 128


eps = 1e-06
clamp_limit = 7.0
sigmoid_alpha = 1.702


MESH = pl.DeviceIdType.MESH
CORES = 2
LANES = 128
MIB = 1024 * 1024


def round_up(value, unit):
    return (value + unit - 1) // unit * unit


def place():
    tp = lax.axis_index("tp")
    return lax.axis_index("sp"), tp // CORES, lax.rem(tp, CORES)


def partner_of(sp, d, n_sp):
    if n_sp & (n_sp - 1):
        return lax.rem(sp + d, n_sp)
    total, bit = 0, 1
    while bit < n_sp:
        total = total + lax.rem(sp // bit + d // bit, 2) * bit
        bit *= 2
    return total


def source_of(sp, d, n_sp):
    if n_sp & (n_sp - 1):
        return lax.rem(sp + n_sp - d, n_sp)
    return partner_of(sp, d, n_sp)


def greet(n_sp, nz, sp, z, c):
    barrier = pltpu.get_barrier_semaphore()
    tp = z * CORES + c
    for d in range(1, n_sp):
        pl.semaphore_signal(
            barrier, inc=1, device_id=(partner_of(sp, d, n_sp), tp), device_id_type=MESH
        )
    pl.semaphore_signal(
        barrier, inc=1, device_id=(sp, z * CORES + 1 - c), device_id_type=MESH
    )

    @pl.when(z > 0)
    def _():
        pl.semaphore_signal(barrier, inc=1, device_id=(sp, tp - CORES), device_id_type=MESH)

    @pl.when(z < nz - 1)
    def _():
        pl.semaphore_signal(barrier, inc=1, device_id=(sp, tp + CORES), device_id_type=MESH)

    beside = jnp.where(z > 0, 1, 0) + jnp.where(z < nz - 1, 1, 0)
    pl.semaphore_wait(barrier, n_sp + beside)


def send(src, dst, send_sem, recv_sem, device):
    return pltpu.make_async_remote_copy(
        src_ref=src,
        dst_ref=dst,
        send_sem=send_sem,
        recv_sem=recv_sem,
        device_id=device,
        device_id_type=MESH,
    )


def dot(a, b):
    return jnp.dot(a, b, preferred_element_type=jnp.float32)


def tiled(extent, tile, visit):
    def one(t, carry):
        visit(pl.ds(pl.multiple_of(t * tile, tile), tile))
        return carry

    lax.fori_loop(0, extent // tile, one, 0)


def both_sides(z, nz, away, visit):
    def one(behind, carry):
        block = z + away * (1 - 2 * behind)

        @pl.when((block >= 0) & (block < nz))
        def _():
            visit(block, behind)

        return carry

    lax.fori_loop(0, 2, one, 0)


def expert_kernel(
    n_sp, nz, normed, stream, onehot, share, gate, up, down, out,
    gate_v, up_v, down_v, toks, comp_a, comp_b, rows_a, rows_b, hid,
    sums_a, sums_b, back_a, back_b, a_out, a_up, a_dn, b_up, b_dn,
    w_l, w_s, w_r, ru_s, ru_r, rd_s, rd_r, xa_s, xa_r, xb_s, xb_r,
    bu_s, bu_r, bd_s, bd_r, ya_s, ya_r, yb_s, yb_r,
    au_s, au_r, ad_s, ad_r, cu_s, cu_r, cd_s, cd_r,
):
    sp, z, c = place()
    tp = z * CORES + c
    peer_core = (sp, z * CORES + 1 - c)
    above = (sp, lax.rem(z + 1, nz) * CORES + c)
    below = (sp, lax.rem(z + nz - 1, nz) * CORES + c)
    capp, ka, kb = rows_a.shape[2], rows_a.shape[3], rows_b.shape[3]
    na, nb = sums_a.shape[3], sums_b.shape[3]
    slots = n_sp * capp
    units = gate.shape[1]
    tile = math.gcd(math.gcd(ka, kb), 256)
    wide = math.gcd(math.gcd(na, nb), 512)
    greet(n_sp, nz, sp, z, c)

    def raw_above(block, src):
        return send(src, toks.at[block], ru_s.at[block], ru_r.at[block], above)

    def raw_below(block, src):
        return send(src, toks.at[block], rd_s.at[block], rd_r.at[block], below)

    own_raw = normed.at[:, pl.ds(0, ka)]

    @pl.when(z < nz - 1)
    def _():
        raw_above(z, own_raw).start()

    @pl.when(z > 0)
    def _():
        raw_below(z, own_raw).start()

    mine = pl.ds(pl.multiple_of(c * units, units), units)
    held = (gate_v.at[:, mine], up_v.at[:, mine], down_v.at[mine, :])
    locals_ = [
        pltpu.make_async_copy(src, dst, w_l.at[i])
        for i, (src, dst) in enumerate(zip((gate, up, down), held))
    ]
    lent = [
        send(src, dst, w_s.at[i], w_r.at[i], peer_core)
        for i, (src, dst) in enumerate(zip((gate, up, down), held))
    ]

    def xa_to(block, d):
        e = partner_of(sp, d, n_sp)
        return send(
            comp_a.at[block, e], rows_a.at[block, sp], xa_s.at[block, d], xa_r.at[block, d], (e, tp)
        )

    def xa_from(block, d):
        e = source_of(sp, d, n_sp)
        return send(
            comp_a.at[block, e], rows_a.at[block, e], xa_s.at[block, d], xa_r.at[block, d], (e, tp)
        )

    def xb_to(d):
        e = partner_of(sp, d, n_sp)
        return send(comp_b.at[e], rows_b.at[z, sp], xb_s.at[d], xb_r.at[d], (e, tp))

    def xb_from(d):
        e = source_of(sp, d, n_sp)
        return send(comp_b.at[e], rows_b.at[z, e], xb_s.at[d], xb_r.at[d], (e, tp))

    def b_above(block):
        return send(rows_b.at[block], rows_b.at[block], bu_s.at[block], bu_r.at[block], above)

    def b_below(block):
        return send(rows_b.at[block], rows_b.at[block], bd_s.at[block], bd_r.at[block], below)

    def deal_b(cols):
        picked = dot(onehot[z], normed[:, pl.ds(pl.multiple_of(ka + cols.start, tile), tile)])
        comp_b[:, :, cols] = picked.astype(jnp.bfloat16).reshape(n_sp, capp, tile)

    tiled(kb, tile, deal_b)
    for d in range(1, n_sp):
        xb_to(d).start()
    rows_b[z, sp] = comp_b[sp]

    def deal(block, src):
        def one(cols):
            picked = dot(onehot[block], src[:, cols])
            comp_a[block, :, :, cols] = picked.astype(jnp.bfloat16).reshape(n_sp, capp, tile)

        tiled(ka, tile, one)
        for d in range(1, n_sp):
            xa_to(block, d).start()
        rows_a[block, sp] = comp_a[block, sp]

    deal(z, normed)
    for copy in locals_ + lent:
        copy.start()

    def spread_own():
        for d in range(1, n_sp):
            xb_from(d).wait_recv()

        @pl.when(z < nz - 1)
        def _():
            b_above(z).start()

        @pl.when(z > 0)
        def _():
            b_below(z).start()

    def gather_raw(block, behind):
        @pl.when(behind == 1)
        def _():
            raw_above(block, toks.at[block]).wait_recv()

            @pl.when(z < nz - 1)
            def _():
                raw_above(block, toks.at[block]).start()

        @pl.when(behind == 0)
        def _():
            raw_below(block, toks.at[block]).wait_recv()

            @pl.when(z > 0)
            def _():
                raw_below(block, toks.at[block]).start()

        deal(block, toks.at[block])

    def gather_b(block, behind):
        @pl.when(behind == 1)
        def _():
            b_above(block).wait_recv()

            @pl.when(z < nz - 1)
            def _():
                b_above(block).start()

        @pl.when(behind == 0)
        def _():
            b_below(block).wait_recv()

            @pl.when(z > 0)
            def _():
                b_below(block).start()

    unit = min(256, CORES * units)

    def serve(block, behind):
        for d in range(1, n_sp):
            xa_from(block, d).wait_recv()

        def one(cols):
            tile_a = rows_a[block].reshape(slots, ka)
            tile_b = rows_b[block].reshape(slots, kb)
            gate_pre = dot(tile_a, gate_v[:ka, cols]) + dot(tile_b, gate_v[ka:, cols])
            upward = dot(tile_a, up_v[:ka, cols]) + dot(tile_b, up_v[ka:, cols])
            capped = jnp.minimum(gate_pre, clamp_limit)
            linear = jnp.clip(upward, -clamp_limit, clamp_limit)
            gated = capped * jax.nn.sigmoid(sigmoid_alpha * capped)
            hid[:, cols] = (gated * (linear + 1.0)).astype(jnp.bfloat16)

        tiled(CORES * units, unit, one)

        def part_a(cols):
            part = dot(hid[...], down_v[:, cols]).astype(jnp.bfloat16)
            sums_a[block, :, :, cols] = part.reshape(n_sp, capp, wide)

        def part_b(cols):
            at = pl.ds(pl.multiple_of(na + cols.start, wide), wide)
            part = dot(hid[...], down_v[:, at]).astype(jnp.bfloat16)
            sums_b[block, :, :, cols] = part.reshape(n_sp, capp, wide)

        tiled(na, wide, part_a)
        tiled(nb, wide, part_b)

    def arrive(i, carry):
        both_sides(z, nz, i, gather_raw)

        @pl.when(i == 1)
        def _():
            spread_own()

        @pl.when(i > 1)
        def _():
            both_sides(z, nz, i - 1, gather_b)

        @pl.when(i == min(2, nz - 1))
        def _():
            for copy in locals_:
                copy.wait()
            for copy in lent:
                copy.wait()

        @pl.when(i > 1)
        def _():
            both_sides(z, nz, i - 2, lambda block, behind: serve_once(block, behind, i - 2))

        return carry

    def serve_once(block, behind, away):
        @pl.when((away > 0) | (behind == 0))
        def _():
            serve(block, behind)

    lax.fori_loop(1, nz, arrive, 0)
    both_sides(z, nz, nz - 2, lambda block, behind: serve_once(block, behind, nz - 2))
    both_sides(z, nz, nz - 1, gather_b)
    both_sides(z, nz, nz - 1, serve)

    def ya_to(block, d):
        e = partner_of(sp, d, n_sp)
        return send(
            sums_a.at[block, e], back_a.at[block, sp], ya_s.at[block, d], ya_r.at[block, d], (e, tp)
        )

    def ya_from(block, d):
        e = source_of(sp, d, n_sp)
        return send(
            sums_a.at[block, e], back_a.at[block, e], ya_s.at[block, d], ya_r.at[block, d], (e, tp)
        )

    def yb_to(d):
        e = partner_of(sp, d, n_sp)
        return send(sums_b.at[z, e], back_b.at[sp], yb_s.at[d], yb_r.at[d], (e, tp))

    def yb_from(d):
        e = source_of(sp, d, n_sp)
        return send(sums_b.at[z, e], back_b.at[e], yb_s.at[d], yb_r.at[d], (e, tp))

    def a_above(block):
        return send(a_out.at[block], a_up.at[block], au_s.at[block], au_r.at[block], above)

    def a_below(block):
        return send(a_out.at[block], a_dn.at[block], ad_s.at[block], ad_r.at[block], below)

    def c_above(block):
        return send(sums_b.at[block], b_up.at[block], cu_s.at[block], cu_r.at[block], above)

    def c_below(block):
        return send(sums_b.at[block], b_dn.at[block], cd_s.at[block], cd_r.at[block], below)

    def push(block, behind):
        for d in range(1, n_sp):
            ya_to(block, d).start()
        back_a[block, sp] = sums_a[block, sp]

    def far_push(i, carry):
        both_sides(z, nz, nz - 1 - i, push)
        return carry

    lax.fori_loop(0, nz - 1, far_push, 0)
    push(z, 0)

    def add_b(block, arrived):
        total = sums_b[block].astype(jnp.float32) + arrived[block].astype(jnp.float32)
        sums_b[block] = total.astype(jnp.bfloat16)

    def relay_b(block, behind):
        @pl.when(behind == 0)
        def _():
            @pl.when(z > 0)
            def _():
                c_above(block).wait_recv()
                add_b(block, b_up)

            c_above(block).start()

        @pl.when(behind == 1)
        def _():
            @pl.when(z < nz - 1)
            def _():
                c_below(block).wait_recv()
                add_b(block, b_dn)

            c_below(block).start()

    def settle_b():
        @pl.when(z > 0)
        def _():
            c_above(z).wait_recv()
            add_b(z, b_up)

        @pl.when(z < nz - 1)
        def _():
            c_below(z).wait_recv()
            add_b(z, b_dn)

        for d in range(1, n_sp):
            yb_to(d).start()
        back_b[sp] = sums_b[z, sp]

    def combined(block, cols):
        return dot(share[block], back_a[block, :, :, cols].reshape(slots, wide))

    def relay_a(block, behind):
        for d in range(1, n_sp):
            ya_from(block, d).wait_recv()

        @pl.when(behind == 0)
        def _():
            @pl.when(z > 0)
            def _():
                a_above(block).wait_recv()

            def one(cols):
                total = combined(block, cols)
                total = jnp.where(z > 0, total + a_up[block, :, cols].astype(jnp.float32), total)
                a_out[block, :, cols] = total.astype(jnp.bfloat16)

            tiled(na, wide, one)
            a_above(block).start()

        @pl.when(behind == 1)
        def _():
            @pl.when(z < nz - 1)
            def _():
                a_below(block).wait_recv()

            def one(cols):
                total = combined(block, cols)
                total = jnp.where(
                    z < nz - 1, total + a_dn[block, :, cols].astype(jnp.float32), total
                )
                a_out[block, :, cols] = total.astype(jnp.bfloat16)

            tiled(na, wide, one)
            a_below(block).start()

    both_sides(z, nz, nz - 1, relay_b)

    def relay(i, carry):
        away = nz - 1 - i

        @pl.when(away > 1)
        def _():
            both_sides(z, nz, away - 1, relay_b)

        @pl.when(away == 1)
        def _():
            settle_b()

        both_sides(z, nz, away, relay_a)
        return carry

    lax.fori_loop(0, nz - 1, relay, 0)

    for d in range(1, n_sp):
        yb_from(d).wait_recv()

    def final_b(cols):
        at = pl.ds(pl.multiple_of(na + cols.start, wide), wide)
        total = dot(share[z], back_b[:, :, cols].reshape(slots, wide))
        out[:, at] = (stream[:, at].astype(jnp.float32) + total).astype(jnp.bfloat16)

    tiled(nb, wide, final_b)
    for d in range(1, n_sp):
        ya_from(z, d).wait_recv()

    @pl.when(z > 0)
    def _():
        a_above(z).wait_recv()

    @pl.when(z < nz - 1)
    def _():
        a_below(z).wait_recv()

    def final_a(cols):
        total = combined(z, cols)
        total = jnp.where(z > 0, total + a_up[z, :, cols].astype(jnp.float32), total)
        total = jnp.where(z < nz - 1, total + a_dn[z, :, cols].astype(jnp.float32), total)
        out[:, cols] = (stream[:, cols].astype(jnp.float32) + total).astype(jnp.bfloat16)

    tiled(na, wide, final_a)

    for d in range(1, n_sp):
        xb_to(d).wait_send()
        yb_to(d).wait_send()

    def drain_exchange(block):
        for d in range(1, n_sp):
            xa_to(block, d).wait_send()
            ya_to(block, d).wait_send()

    drain_exchange(z)

    @pl.when(z < nz - 1)
    def _():
        raw_above(z, own_raw).wait_send()
        b_above(z).wait_send()

    @pl.when(z > 0)
    def _():
        raw_below(z, own_raw).wait_send()
        b_below(z).wait_send()

    def drain(block, behind):
        drain_exchange(block)

        @pl.when(behind == 0)
        def _():
            a_above(block).wait_send()
            c_above(block).wait_send()

        @pl.when(behind == 1)
        def _():
            a_below(block).wait_send()
            c_below(block).wait_send()

        @pl.when((behind == 1) & (z < nz - 1))
        def _():
            raw_above(block, toks.at[block]).wait_send()
            b_above(block).wait_send()

        @pl.when((behind == 0) & (z > 0))
        def _():
            raw_below(block, toks.at[block]).wait_send()
            b_below(block).wait_send()

    def drain_all(i, carry):
        both_sides(z, nz, i, drain)
        return carry

    lax.fori_loop(1, nz, drain_all, 0)


def split_columns(width, share):
    return max(256, min(width - 256, int(width * share) // 256 * 256))


def experts(normed, stream, onehot, share, gate_local, up_local, down_local):
    n_sp = lax.axis_size("sp")
    nz = lax.axis_size("tp") // CORES
    tok, width = normed.shape
    units = gate_local.shape[1]
    slots = onehot.shape[1]
    capp = slots // n_sp
    ka = split_columns(width, 0.75)
    na = split_columns(width, 0.75)
    kb, nb = width - ka, width - na
    vmem = pl.BlockSpec(memory_space=pltpu.VMEM)
    anywhere = pl.BlockSpec(memory_space=pltpu.HBM)
    dma = pltpu.SemaphoreType.DMA
    bf = jnp.bfloat16
    line = [dma((nz,))] * 4
    return pl.pallas_call(
        functools.partial(expert_kernel, n_sp, nz),
        out_shape=jax.ShapeDtypeStruct((tok, width), bf),
        in_specs=[vmem] * 4 + [anywhere] * 3,
        out_specs=vmem,
        scratch_shapes=[
            pltpu.VMEM((width, CORES * units), bf),
            pltpu.VMEM((width, CORES * units), bf),
            pltpu.VMEM((CORES * units, width), bf),
            pltpu.VMEM((nz, tok, ka), bf),
            pltpu.VMEM((nz, n_sp, capp, ka), bf),
            pltpu.VMEM((n_sp, capp, kb), bf),
            pltpu.VMEM((nz, n_sp, capp, ka), bf),
            pltpu.VMEM((nz, n_sp, capp, kb), bf),
            pltpu.VMEM((slots, CORES * units), bf),
            pltpu.VMEM((nz, n_sp, capp, na), bf),
            pltpu.VMEM((nz, n_sp, capp, nb), bf),
            pltpu.VMEM((nz, n_sp, capp, na), bf),
            pltpu.VMEM((n_sp, capp, nb), bf),
            pltpu.VMEM((nz, tok, na), bf),
            pltpu.VMEM((nz, tok, na), bf),
            pltpu.VMEM((nz, tok, na), bf),
            pltpu.VMEM((nz, n_sp, capp, nb), bf),
            pltpu.VMEM((nz, n_sp, capp, nb), bf),
        ]
        + [dma((3,))] * 3
        + line
        + [dma((nz, n_sp))] * 2
        + [dma((n_sp,))] * 2
        + line
        + [dma((nz, n_sp))] * 2
        + [dma((n_sp,))] * 2
        + line
        + line,
        compiler_params=pltpu.CompilerParams(
            collective_id=0, has_side_effects=True, vmem_limit_bytes=48 * MIB
        ),
        name="experts",
    )(normed, stream, onehot, share, gate_local, up_local, down_local)


def tables(n_sp, nz, tok, capp, c, routes, rw_all, onehot, share):
    choose = routes.shape[0]
    epad = round_up(n_sp, 16)
    earlier = lax.broadcasted_iota(jnp.int32, (tok, tok), 0) < lax.broadcasted_iota(
        jnp.int32, (tok, tok), 1
    )
    earlier = jnp.where(earlier, 1.0, 0.0).astype(jnp.bfloat16)
    same = lax.broadcasted_iota(jnp.int32, (tok, tok), 0) == lax.broadcasted_iota(
        jnp.int32, (tok, tok), 1
    )
    same = jnp.where(same, 1.0, 0.0).astype(jnp.bfloat16)
    which = lax.broadcasted_iota(jnp.int32, (epad, tok), 0)
    place_in = lax.broadcasted_iota(jnp.int32, (capp, tok), 0).astype(jnp.float32)
    for b in range(nz):
        first = routes[:, (CORES * b) * tok : (CORES * b + 1) * tok]
        second = routes[:, (CORES * b + 1) * tok : (CORES * b + 2) * tok]
        ids = jnp.where(c == 0, first, second)
        weight = jnp.zeros((epad, tok), jnp.float32)
        member = jnp.zeros((epad, tok), jnp.float32)
        for m in range(choose):
            named = ids[m : m + 1, :] == which
            member = jnp.where(named, 1.0, member)
            weight = jnp.where(named, rw_all[b, m : m + 1, :tok], weight)
        rank = dot(member.astype(jnp.bfloat16), earlier)
        rank = jnp.where(member > 0.0, rank, -1.0)
        shares = []
        for e in range(n_sp):
            hit = place_in == rank[e : e + 1, :]
            onehot[b, e * capp : (e + 1) * capp, :] = jnp.where(hit, 1.0, 0.0).astype(jnp.bfloat16)
            shares.append(jnp.where(hit, weight[e : e + 1, :], 0.0).astype(jnp.bfloat16))
        turned = lax.dot_general(
            same,
            jnp.concatenate(shares, axis=0),
            (((1,), (1,)), ((), ())),
            preferred_element_type=jnp.float32,
        )
        share[b] = turned.astype(jnp.bfloat16)


def front_kernel(
    n_sp, n_tp, tok, capp, q, k, v, sink_in, residual, weight, gain_in, routes_in, rweight,
    normed, stream, onehot, share,
    q_all, k_all, v_all, k_tail, v_tail, att, got, w_all, res, acc, rw_src, rw_all,
    sink, gain, routes, rw_in,
    in_s, o_s, t_s, t_r, a_s, a_r, g_s, g_r,
):
    sp, z, c = place()
    tp = z * CORES + c
    nz = n_tp // CORES
    span, kv_cols = k.shape
    cols = q.shape[1]
    width = weight.shape[1]
    kv_local = kv_cols // HEAD
    group = cols // kv_cols
    blocks = span // WINDOW
    pieces = WINDOW // tok
    scale = HEAD ** (-0.5)
    body = pl.ds(WINDOW, span)
    copies = [
        pltpu.make_async_copy(k, k_all.at[body], in_s.at[0]),
        pltpu.make_async_copy(v, v_all.at[body], in_s.at[1]),
        pltpu.make_async_copy(q, q_all, in_s.at[2]),
        pltpu.make_async_copy(rweight, rw_in, in_s.at[3]),
        pltpu.make_async_copy(sink_in, sink, in_s.at[4]),
        pltpu.make_async_copy(routes_in, routes, in_s.at[5]),
        pltpu.make_async_copy(residual, res, in_s.at[6]),
        pltpu.make_async_copy(gain_in, gain, in_s.at[7]),
    ]
    for copy in copies:
        copy.start()

    def out_rows(p):
        rows = pl.ds(pl.multiple_of(p * cols, cols), cols)
        return pltpu.make_async_copy(weight.at[rows], w_all.at[rows], o_s.at[p])

    barrier = pltpu.get_barrier_semaphore()
    for d in range(1, n_tp):
        pl.semaphore_signal(
            barrier, inc=1, device_id=(sp, lax.rem(tp + d, n_tp)), device_id_type=MESH
        )

    @pl.when(sp > 0)
    def _():
        pl.semaphore_signal(barrier, inc=1, device_id=(sp - 1, tp), device_id_type=MESH)

    @pl.when(sp < n_sp - 1)
    def _():
        pl.semaphore_signal(barrier, inc=1, device_id=(sp + 1, tp), device_id_type=MESH)

    rw_src[...] = jnp.zeros_like(rw_src)
    copies[3].wait()
    rw_src[: rweight.shape[0], :tok] = rw_in[...]
    rw_all[z] = rw_src[...]
    beside = jnp.where(sp > 0, 1, 0) + jnp.where(sp < n_sp - 1, 1, 0)
    pl.semaphore_wait(barrier, n_tp - 1 + beside)
    ahead = (lax.rem(sp + 1, n_sp), tp)
    last = pl.ds(span, WINDOW)
    tails = (
        send(k_all.at[last], k_tail, t_s.at[0], t_r.at[0], ahead),
        send(v_all.at[last], v_tail, t_s.at[1], t_r.at[1], ahead),
    )
    copies[0].wait()
    copies[1].wait()

    @pl.when(sp < n_sp - 1)
    def _():
        for copy in tails:
            copy.start()

    def tell(d):
        there = lax.rem(z + d, nz)
        return send(rw_src, rw_all.at[z], g_s.at[d], g_r.at[z], (sp, there * CORES + c))

    def told(d):
        there = lax.rem(z + d, nz)
        return send(rw_src, rw_all.at[there], g_s.at[d], g_r.at[there], (sp, there * CORES + c))

    for d in range(1, nz):
        tell(d).start()
    copies[2].wait()
    copies[4].wait()
    for p in range(n_tp):
        out_rows(p).start()

    row = lax.broadcasted_iota(jnp.int32, (WINDOW, 2 * WINDOW), 0)
    col = lax.broadcasted_iota(jnp.int32, (WINDOW, 2 * WINDOW), 1)
    distance = row + WINDOW - col
    banded = (distance >= 0) & (distance < WINDOW)
    low = z < nz // 2
    half = max(1, blocks // 2)

    def to_owner(dest):
        at = pl.multiple_of(dest * tok, tok)
        return send(
            att.at[pl.ds(at, tok)], got.at[tp], a_s.at[dest], a_r.at[tp], (sp, dest)
        )

    def attend(i, carry):
        turned = jnp.where(i < half, lax.rem(i + 1, half), i)
        block = jnp.where(low, blocks - 1 - i, turned)

        @pl.when(block == 0)
        def _():
            @pl.when(sp > 0)
            def _():
                for copy in tails:
                    copy.wait_recv()
                k_all[pl.ds(0, WINDOW), :] = k_tail[...]
                v_all[pl.ds(0, WINDOW), :] = v_tail[...]

            @pl.when(sp == 0)
            def _():
                k_all[pl.ds(0, WINDOW), :] = jnp.zeros((WINDOW, kv_cols), jnp.bfloat16)
                v_all[pl.ds(0, WINDOW), :] = jnp.zeros((WINDOW, kv_cols), jnp.bfloat16)

        at = pl.multiple_of(block * WINDOW, WINDOW)
        start = jnp.where((sp == 0) & (block == 0), WINDOW, 0)
        allowed = banded & (col >= start)
        band = pl.ds(at, 2 * WINDOW)
        for g in range(kv_local):
            keys = k_all[band, g * HEAD : (g + 1) * HEAD]
            values = v_all[band, g * HEAD : (g + 1) * HEAD]
            heads = []
            for m in range(group):
                h = g * group + m
                query = q_all[pl.ds(at, WINDOW), h * HEAD : (h + 1) * HEAD] * jnp.bfloat16(scale)
                scores = lax.dot_general(
                    query, keys, (((1,), (1,)), ((), ())), preferred_element_type=jnp.float32
                )
                logits = jnp.where(allowed, scores, -jnp.inf)
                top = jnp.maximum(jnp.max(logits, axis=-1, keepdims=True), sink[h])
                raised = jnp.exp(logits - top)
                total = jnp.sum(raised, axis=-1, keepdims=True) + jnp.exp(sink[h] - top)
                probs = (raised * (1.0 / total)).astype(jnp.bfloat16)
                heads.append(dot(probs, values))
            att[pl.ds(at, WINDOW), g * group * HEAD : (g + 1) * group * HEAD] = jnp.concatenate(
                heads, axis=1
            ).astype(jnp.bfloat16)
        for piece in range(pieces):
            dest = block * pieces + piece

            @pl.when(dest != tp)
            def _():
                to_owner(dest).start()

        return carry

    lax.fori_loop(0, blocks, attend, 0)
    for d in range(1, nz):
        told(d).wait_recv()
    copies[5].wait()
    tables(n_sp, nz, tok, capp, c, routes, rw_all, onehot, share)
    got[tp] = att[pl.ds(pl.multiple_of(tp * tok, tok), tok), :]
    copies[6].wait()
    copies[7].wait()
    wide = math.gcd(width, 512)

    def begin(at):
        acc[:, at] = res[:, at].astype(jnp.float32)

    tiled(width, wide, begin)
    for p in range(n_tp):
        out_rows(p).wait()

    def mix(i, carry):
        p = jnp.where(low, n_tp - 1 - i, i)

        @pl.when(tp != p)
        def _():
            send(att.at[pl.ds(0, tok)], got.at[p], a_s.at[p], a_r.at[p], (sp, p)).wait_recv()

        rows = pl.ds(pl.multiple_of(p * cols, cols), cols)

        def one(at):
            acc[:, at] = acc[:, at] + dot(got[p], w_all[rows, at])

        tiled(width, wide, one)
        return carry

    lax.fori_loop(0, n_tp, mix, 0)
    squares = jnp.zeros((tok, 1), jnp.float32)
    for t in range(width // wide):
        at = slice(t * wide, (t + 1) * wide)
        held = acc[:, at].astype(jnp.bfloat16)
        stream[:, at] = held
        held32 = held.astype(jnp.float32)
        squares = squares + jnp.sum(held32 * held32, axis=-1, keepdims=True)
    root = lax.rsqrt(squares * (1.0 / width) + eps)
    for t in range(width // wide):
        at = slice(t * wide, (t + 1) * wide)
        normed[:, at] = (stream[:, at].astype(jnp.float32) * root * gain[:, at]).astype(
            jnp.bfloat16
        )
    for p in range(n_tp):
        @pl.when(tp != p)
        def _():
            to_owner(p).wait_send()

    for d in range(1, nz):
        tell(d).wait_send()

    @pl.when(sp < n_sp - 1)
    def _():
        for copy in tails:
            copy.wait_send()


def front(query_heads, key_heads, value_heads, sink_logit, residual, out_weight, norm_gain, routes,
          route_weight):
    n_sp, n_tp = lax.axis_size("sp"), lax.axis_size("tp")
    nz = n_tp // CORES
    span, cols = query_heads.shape
    kv_cols = key_heads.shape[1]
    tok, width = residual.shape
    choose = routes.shape[1]
    capp = round_up(max(2, 5 * tok * choose // (4 * n_sp)), 16)
    slots = n_sp * capp
    vmem = pl.BlockSpec(memory_space=pltpu.VMEM)
    anywhere = pl.BlockSpec(memory_space=pltpu.HBM)
    dma = pltpu.SemaphoreType.DMA
    bf = jnp.bfloat16
    return pl.pallas_call(
        functools.partial(front_kernel, n_sp, n_tp, tok, capp),
        out_shape=(
            jax.ShapeDtypeStruct((tok, width), bf),
            jax.ShapeDtypeStruct((tok, width), bf),
            jax.ShapeDtypeStruct((nz, slots, tok), bf),
            jax.ShapeDtypeStruct((nz, tok, slots), bf),
        ),
        in_specs=[anywhere] * 9,
        out_specs=(vmem,) * 4,
        scratch_shapes=[
            pltpu.VMEM((span, cols), bf),
            pltpu.VMEM((span + WINDOW, kv_cols), bf),
            pltpu.VMEM((span + WINDOW, kv_cols), bf),
            pltpu.VMEM((WINDOW, kv_cols), bf),
            pltpu.VMEM((WINDOW, kv_cols), bf),
            pltpu.VMEM((span, cols), bf),
            pltpu.VMEM((n_tp, tok, cols), bf),
            pltpu.VMEM((n_tp * cols, width), bf),
            pltpu.VMEM((tok, width), bf),
            pltpu.VMEM((tok, width), jnp.float32),
            pltpu.VMEM((8, LANES), jnp.float32),
            pltpu.VMEM((nz, 8, LANES), jnp.float32),
            pltpu.SMEM(sink_logit.shape, jnp.float32),
            pltpu.VMEM((1, width), jnp.float32),
            pltpu.VMEM(routes.shape[::-1], routes.dtype),
            pltpu.VMEM(route_weight.shape[::-1], jnp.float32),
            dma((8,)),
            dma((n_tp,)),
            dma((2,)),
            dma((2,)),
            dma((n_tp,)),
            dma((n_tp,)),
            dma((nz,)),
            dma((nz,)),
        ],
        compiler_params=pltpu.CompilerParams(
            collective_id=2, has_side_effects=True, vmem_limit_bytes=32 * MIB
        ),
        name="front",
    )(*[
        pltpu.with_memory_space_constraint(x, pltpu.HBM)
        for x in (
            query_heads, key_heads, value_heads, sink_logit, residual, out_weight,
            norm_gain.reshape(1, -1), routes.T, route_weight.T,
        )
    ])


def local(
    query_heads,
    key_heads,
    value_heads,
    sink_logit,
    residual,
    out_weight,
    norm_gain,
    routes,
    route_weight,
    gate_weight,
    up_weight,
    down_weight,
):
    normed, stream, onehot, share = front(
        query_heads, key_heads, value_heads, sink_logit, residual, out_weight, norm_gain, routes,
        route_weight,
    )
    return experts(normed, stream, onehot, share, gate_weight[0], up_weight[0], down_weight[0])


def solution(mesh):
    placed = (
        P("sp", "tp"),
        P("sp", "tp"),
        P("sp", "tp"),
        P("tp"),
        P(("sp", "tp"), None),
        P(),
        P(),
        P("sp", None),
        P(("sp", "tp"), None),
        P("sp", None, "tp"),
        P("sp", None, "tp"),
        P("sp", "tp", None),
    )
    return jax.shard_map(
        local, mesh=mesh, in_specs=placed, out_specs=P(("sp", "tp"), None), check_vma=False
    )
```

```python
import functools
import math

import jax
import jax.numpy as jnp
from jax import lax
from jax.experimental import pallas as pl
from jax.experimental.pallas import tpu as pltpu
from jax.sharding import PartitionSpec as P

HEAD = 64
WINDOW = 128


eps = 1e-06
clamp_limit = 7.0
sigmoid_alpha = 1.702


MESH = pl.DeviceIdType.MESH
CORES = 2
LANES = 128
MIB = 1024 * 1024


def round_up(value, unit):
    return (value + unit - 1) // unit * unit


def place():
    tp = lax.axis_index("tp")
    return lax.axis_index("sp"), tp // CORES, lax.rem(tp, CORES)


def partner_of(sp, d, n_sp):
    if n_sp & (n_sp - 1):
        return lax.rem(sp + d, n_sp)
    total, bit = 0, 1
    while bit < n_sp:
        total = total + lax.rem(sp // bit + d // bit, 2) * bit
        bit *= 2
    return total


def source_of(sp, d, n_sp):
    if n_sp & (n_sp - 1):
        return lax.rem(sp + n_sp - d, n_sp)
    return partner_of(sp, d, n_sp)


def greet(n_sp, nz, sp, z, c):
    barrier = pltpu.get_barrier_semaphore()
    tp = z * CORES + c
    for d in range(1, n_sp):
        pl.semaphore_signal(
            barrier, inc=1, device_id=(partner_of(sp, d, n_sp), tp), device_id_type=MESH
        )
    pl.semaphore_signal(
        barrier, inc=1, device_id=(sp, z * CORES + 1 - c), device_id_type=MESH
    )

    @pl.when(z > 0)
    def _():
        pl.semaphore_signal(barrier, inc=1, device_id=(sp, tp - CORES), device_id_type=MESH)

    @pl.when(z < nz - 1)
    def _():
        pl.semaphore_signal(barrier, inc=1, device_id=(sp, tp + CORES), device_id_type=MESH)

    beside = jnp.where(z > 0, 1, 0) + jnp.where(z < nz - 1, 1, 0)
    pl.semaphore_wait(barrier, n_sp + beside)


def send(src, dst, send_sem, recv_sem, device):
    return pltpu.make_async_remote_copy(
        src_ref=src,
        dst_ref=dst,
        send_sem=send_sem,
        recv_sem=recv_sem,
        device_id=device,
        device_id_type=MESH,
    )


def dot(a, b):
    return jnp.dot(a, b, preferred_element_type=jnp.float32)


def tiled(extent, tile, visit):
    def one(t, carry):
        visit(pl.ds(pl.multiple_of(t * tile, tile), tile))
        return carry

    lax.fori_loop(0, extent // tile, one, 0)
    if extent % tile:
        visit(pl.ds(extent // tile * tile, extent % tile))


def shifted(cols, offset):
    start = cols.start + offset
    if not isinstance(start, int):
        start = pl.multiple_of(start, LANES)
    return pl.ds(start, cols.size)


RAW, NEAR, SERVE, PUSH, CHAIN, RELAY = range(1, 7)
KINDS = 8
PER_WORD = 5


def sides(nz, z, away):
    return [b for b in ((z + away, z - away) if away else (z,)) if 0 <= b < nz]


def plain_order(nz, z):
    order = []
    for i in range(1, nz):
        order += [(RAW, b) for b in sides(nz, z, i)]
        order += [(NEAR, b) for b in sides(nz, z, i - 1)]
        if i > 1:
            order += [(SERVE, b) for b in sides(nz, z, i - 2)]
    order += [(SERVE, b) for b in sides(nz, z, nz - 2)]
    order += [(NEAR, b) for b in sides(nz, z, nz - 1)]
    order += [(SERVE, b) for b in sides(nz, z, nz - 1)]
    for i in range(nz - 1):
        order += [(PUSH, b) for b in sides(nz, z, nz - 1 - i)]
    order.append((PUSH, z))
    order += [(CHAIN, b) for b in sides(nz, z, nz - 1)]
    for away in range(nz - 1, 0, -1):
        order += [(CHAIN, b) for b in sides(nz, z, away - 1)]
        order += [(RELAY, b) for b in sides(nz, z, away)]
    return order


ORDERS = {
    4: [
        [
            (NEAR, 0), (RAW, 1), (RAW, 2), (RAW, 3), (NEAR, 1),
            (SERVE, 1), (CHAIN, 1), (SERVE, 0), (NEAR, 3), (SERVE, 3),
            (PUSH, 3), (CHAIN, 3), (NEAR, 2), (SERVE, 2), (PUSH, 2),
            (PUSH, 1), (CHAIN, 2), (RELAY, 3), (PUSH, 0), (RELAY, 2),
            (RELAY, 1), (CHAIN, 0),
        ],
        [
            (RAW, 0), (RAW, 2), (NEAR, 0), (RAW, 3), (NEAR, 1),
            (NEAR, 3), (NEAR, 2), (SERVE, 2), (SERVE, 1), (PUSH, 2),
            (SERVE, 0), (SERVE, 3), (CHAIN, 3), (PUSH, 3), (CHAIN, 2),
            (PUSH, 0), (RELAY, 3), (PUSH, 1), (CHAIN, 1), (CHAIN, 0),
            (RELAY, 2), (RELAY, 0),
        ],
    ],
}
DISPATCH_SHARE = 0.6875
RETURN_SHARE = 0.75


def order_of(nz, z):
    if nz not in ORDERS:
        return plain_order(nz, z)
    if z < nz // 2:
        return ORDERS[nz][z]
    return [(kind, nz - 1 - b) for kind, b in ORDERS[nz][nz - 1 - z]]


def order_words(nz):
    orders = [order_of(nz, z) for z in range(nz)]
    words = round_up(max(len(order) for order in orders), PER_WORD) // PER_WORD
    table = []
    for order in orders:
        codes = [b * KINDS + kind for kind, b in order]
        codes += [0] * (words * PER_WORD - len(codes))
        base = KINDS * 8
        table.append([
            sum(code * base**i for i, code in enumerate(codes[w * PER_WORD : (w + 1) * PER_WORD]))
            for w in range(words)
        ])
    return table, words


def both_sides(z, nz, away, visit):
    def one(behind, carry):
        block = z + away * (1 - 2 * behind)

        @pl.when((block >= 0) & (block < nz))
        def _():
            visit(block, behind)

        return carry

    lax.fori_loop(0, 2, one, 0)


def expert_kernel(
    n_sp, nz, normed, stream, onehot, share, gate, up, down, out,
    gate_v, up_v, down_v, toks, comp_a, comp_b, rows_a, rows_b, hid,
    sums_a, sums_b, back_a, back_b, a_out, a_up, a_dn, b_up, b_dn,
    w_l, w_s, w_r, ru_s, ru_r, rd_s, rd_r, xa_s, xa_r, xb_s, xb_r,
    bu_s, bu_r, bd_s, bd_r, ya_s, ya_r, yb_s, yb_r,
    au_s, au_r, ad_s, ad_r, cu_s, cu_r, cd_s, cd_r,
):
    sp, z, c = place()
    tp = z * CORES + c
    peer_core = (sp, z * CORES + 1 - c)
    above = (sp, lax.rem(z + 1, nz) * CORES + c)
    below = (sp, lax.rem(z + nz - 1, nz) * CORES + c)
    capp, ka, kb = rows_a.shape[2], rows_a.shape[3], rows_b.shape[3]
    na, nb = sums_a.shape[3], sums_b.shape[3]
    slots = n_sp * capp
    units = gate.shape[1]
    tile, wide = 256, 512
    greet(n_sp, nz, sp, z, c)

    def raw_above(block, src):
        return send(src, toks.at[block], ru_s.at[block], ru_r.at[block], above)

    def raw_below(block, src):
        return send(src, toks.at[block], rd_s.at[block], rd_r.at[block], below)

    own_raw = normed.at[:, pl.ds(0, ka)]

    @pl.when(z < nz - 1)
    def _():
        raw_above(z, own_raw).start()

    @pl.when(z > 0)
    def _():
        raw_below(z, own_raw).start()

    mine = pl.ds(pl.multiple_of(c * units, units), units)
    held = (gate_v.at[:, mine], up_v.at[:, mine], down_v.at[mine, :])
    locals_ = [
        pltpu.make_async_copy(src, dst, w_l.at[i])
        for i, (src, dst) in enumerate(zip((gate, up, down), held))
    ]
    lent = [
        send(src, dst, w_s.at[i], w_r.at[i], peer_core)
        for i, (src, dst) in enumerate(zip((gate, up, down), held))
    ]

    def xa_to(block, d):
        e = partner_of(sp, d, n_sp)
        return send(
            comp_a.at[block, e], rows_a.at[block, sp], xa_s.at[block, d], xa_r.at[block, d], (e, tp)
        )

    def xa_from(block, d):
        e = source_of(sp, d, n_sp)
        return send(
            comp_a.at[block, e], rows_a.at[block, e], xa_s.at[block, d], xa_r.at[block, d], (e, tp)
        )

    def xb_to(d):
        e = partner_of(sp, d, n_sp)
        return send(comp_b.at[e], rows_b.at[z, sp], xb_s.at[d], xb_r.at[d], (e, tp))

    def xb_from(d):
        e = source_of(sp, d, n_sp)
        return send(comp_b.at[e], rows_b.at[z, e], xb_s.at[d], xb_r.at[d], (e, tp))

    def b_above(block):
        return send(rows_b.at[block], rows_b.at[block], bu_s.at[block], bu_r.at[block], above)

    def b_below(block):
        return send(rows_b.at[block], rows_b.at[block], bd_s.at[block], bd_r.at[block], below)

    def deal_b(cols):
        picked = dot(onehot[z], normed[:, shifted(cols, ka)])
        comp_b[:, :, cols] = picked.astype(jnp.bfloat16).reshape(n_sp, capp, cols.size)

    tiled(kb, tile, deal_b)
    for d in range(1, n_sp):
        xb_to(d).start()
    rows_b[z, sp] = comp_b[sp]

    def deal(block, src):
        def one(cols):
            picked = dot(onehot[block], src[:, cols])
            comp_a[block, :, :, cols] = picked.astype(jnp.bfloat16).reshape(n_sp, capp, cols.size)

        tiled(ka, tile, one)
        for d in range(1, n_sp):
            xa_to(block, d).start()
        rows_a[block, sp] = comp_a[block, sp]

    deal(z, normed)
    for copy in locals_ + lent:
        copy.start()

    def spread_own():
        for d in range(1, n_sp):
            xb_from(d).wait_recv()

        @pl.when(z < nz - 1)
        def _():
            b_above(z).start()

        @pl.when(z > 0)
        def _():
            b_below(z).start()

    def gather_raw(block, behind):
        @pl.when(behind == 1)
        def _():
            raw_above(block, toks.at[block]).wait_recv()

            @pl.when(z < nz - 1)
            def _():
                raw_above(block, toks.at[block]).start()

        @pl.when(behind == 0)
        def _():
            raw_below(block, toks.at[block]).wait_recv()

            @pl.when(z > 0)
            def _():
                raw_below(block, toks.at[block]).start()

        deal(block, toks.at[block])

    def gather_b(block, behind):
        @pl.when(behind == 1)
        def _():
            b_above(block).wait_recv()

            @pl.when(z < nz - 1)
            def _():
                b_above(block).start()

        @pl.when(behind == 0)
        def _():
            b_below(block).wait_recv()

            @pl.when(z > 0)
            def _():
                b_below(block).start()

    unit = min(256, CORES * units)

    def serve(block):
        for d in range(1, n_sp):
            xa_from(block, d).wait_recv()

        def one(cols):
            tile_a = rows_a[block].reshape(slots, ka)
            tile_b = rows_b[block].reshape(slots, kb)
            gate_pre = dot(tile_a, gate_v[:ka, cols]) + dot(tile_b, gate_v[ka:, cols])
            upward = dot(tile_a, up_v[:ka, cols]) + dot(tile_b, up_v[ka:, cols])
            capped = jnp.minimum(gate_pre, clamp_limit)
            linear = jnp.clip(upward, -clamp_limit, clamp_limit)
            gated = capped * jax.nn.sigmoid(sigmoid_alpha * capped)
            hid[:, cols] = (gated * (linear + 1.0)).astype(jnp.bfloat16)

        tiled(CORES * units, unit, one)

        def part_a(cols):
            part = dot(hid[...], down_v[:, cols]).astype(jnp.bfloat16)
            sums_a[block, :, :, cols] = part.reshape(n_sp, capp, cols.size)

        def part_b(cols):
            part = dot(hid[...], down_v[:, shifted(cols, na)]).astype(jnp.bfloat16)
            sums_b[block, :, :, cols] = part.reshape(n_sp, capp, cols.size)

        tiled(na, wide, part_a)
        tiled(nb, wide, part_b)

    def ya_to(block, d):
        e = partner_of(sp, d, n_sp)
        return send(
            sums_a.at[block, e], back_a.at[block, sp], ya_s.at[block, d], ya_r.at[block, d], (e, tp)
        )

    def ya_from(block, d):
        e = source_of(sp, d, n_sp)
        return send(
            sums_a.at[block, e], back_a.at[block, e], ya_s.at[block, d], ya_r.at[block, d], (e, tp)
        )

    def yb_to(d):
        e = partner_of(sp, d, n_sp)
        return send(sums_b.at[z, e], back_b.at[sp], yb_s.at[d], yb_r.at[d], (e, tp))

    def yb_from(d):
        e = source_of(sp, d, n_sp)
        return send(sums_b.at[z, e], back_b.at[e], yb_s.at[d], yb_r.at[d], (e, tp))

    def a_above(block):
        return send(a_out.at[block], a_up.at[block], au_s.at[block], au_r.at[block], above)

    def a_below(block):
        return send(a_out.at[block], a_dn.at[block], ad_s.at[block], ad_r.at[block], below)

    def c_above(block):
        return send(sums_b.at[block], b_up.at[block], cu_s.at[block], cu_r.at[block], above)

    def c_below(block):
        return send(sums_b.at[block], b_dn.at[block], cd_s.at[block], cd_r.at[block], below)

    def push(block):
        for d in range(1, n_sp):
            ya_to(block, d).start()
        back_a[block, sp] = sums_a[block, sp]

    def add_b(block, arrived):
        total = sums_b[block].astype(jnp.float32) + arrived[block].astype(jnp.float32)
        sums_b[block] = total.astype(jnp.bfloat16)

    def relay_b(block, behind):
        @pl.when(behind == 0)
        def _():
            @pl.when(z > 0)
            def _():
                c_above(block).wait_recv()
                add_b(block, b_up)

            c_above(block).start()

        @pl.when(behind == 1)
        def _():
            @pl.when(z < nz - 1)
            def _():
                c_below(block).wait_recv()
                add_b(block, b_dn)

            c_below(block).start()

    def settle_b():
        @pl.when(z > 0)
        def _():
            c_above(z).wait_recv()
            add_b(z, b_up)

        @pl.when(z < nz - 1)
        def _():
            c_below(z).wait_recv()
            add_b(z, b_dn)

        for d in range(1, n_sp):
            yb_to(d).start()
        back_b[sp] = sums_b[z, sp]

    def combined(block, cols):
        return dot(share[block], back_a[block, :, :, cols].reshape(slots, cols.size))

    def relay_a(block, behind):
        for d in range(1, n_sp):
            ya_from(block, d).wait_recv()

        @pl.when(behind == 0)
        def _():
            @pl.when(z > 0)
            def _():
                a_above(block).wait_recv()

            def one(cols):
                total = combined(block, cols)
                total = jnp.where(z > 0, total + a_up[block, :, cols].astype(jnp.float32), total)
                a_out[block, :, cols] = total.astype(jnp.bfloat16)

            tiled(na, wide, one)
            a_above(block).start()

        @pl.when(behind == 1)
        def _():
            @pl.when(z < nz - 1)
            def _():
                a_below(block).wait_recv()

            def one(cols):
                total = combined(block, cols)
                total = jnp.where(
                    z < nz - 1, total + a_dn[block, :, cols].astype(jnp.float32), total
                )
                a_out[block, :, cols] = total.astype(jnp.bfloat16)

            tiled(na, wide, one)
            a_below(block).start()

    for copy in locals_:
        copy.wait()
    for copy in lent:
        copy.wait()
    table, words = order_words(nz)

    def word_of(w):
        word = jnp.int32(0)
        for level in range(nz):
            for at in range(words):
                word = jnp.where((z == level) & (w == at), jnp.int32(table[level][at]), word)
        return word

    def task(i, word):
        kind = lax.rem(word, KINDS)
        block = lax.rem(word // KINDS, 8)
        behind = jnp.where(block < z, 1, 0)
        elsewhere = block != z

        @pl.when(kind == RAW)
        def _():
            gather_raw(block, behind)

        @pl.when((kind == NEAR) & elsewhere)
        def _():
            gather_b(block, behind)

        @pl.when((kind == NEAR) & (block == z))
        def _():
            spread_own()

        @pl.when(kind == SERVE)
        def _():
            serve(block)

        @pl.when(kind == PUSH)
        def _():
            push(block)

        @pl.when((kind == CHAIN) & elsewhere)
        def _():
            relay_b(block, behind)

        @pl.when((kind == CHAIN) & (block == z))
        def _():
            settle_b()

        @pl.when(kind == RELAY)
        def _():
            relay_a(block, behind)

        return word // (KINDS * 8)

    def tasks(w, carry):
        lax.fori_loop(0, PER_WORD, task, word_of(w))
        return carry

    lax.fori_loop(0, words, tasks, 0)

    for d in range(1, n_sp):
        yb_from(d).wait_recv()

    def final_b(cols):
        at = shifted(cols, na)
        total = dot(share[z], back_b[:, :, cols].reshape(slots, cols.size))
        out[:, at] = (stream[:, at].astype(jnp.float32) + total).astype(jnp.bfloat16)

    tiled(nb, wide, final_b)
    for d in range(1, n_sp):
        ya_from(z, d).wait_recv()

    @pl.when(z > 0)
    def _():
        a_above(z).wait_recv()

    @pl.when(z < nz - 1)
    def _():
        a_below(z).wait_recv()

    def final_a(cols):
        total = combined(z, cols)
        total = jnp.where(z > 0, total + a_up[z, :, cols].astype(jnp.float32), total)
        total = jnp.where(z < nz - 1, total + a_dn[z, :, cols].astype(jnp.float32), total)
        out[:, cols] = (stream[:, cols].astype(jnp.float32) + total).astype(jnp.bfloat16)

    tiled(na, wide, final_a)

    for d in range(1, n_sp):
        xb_to(d).wait_send()
        yb_to(d).wait_send()

    def drain_exchange(block):
        for d in range(1, n_sp):
            xa_to(block, d).wait_send()
            ya_to(block, d).wait_send()

    drain_exchange(z)

    @pl.when(z < nz - 1)
    def _():
        raw_above(z, own_raw).wait_send()
        b_above(z).wait_send()

    @pl.when(z > 0)
    def _():
        raw_below(z, own_raw).wait_send()
        b_below(z).wait_send()

    def drain(block, behind):
        drain_exchange(block)

        @pl.when(behind == 0)
        def _():
            a_above(block).wait_send()
            c_above(block).wait_send()

        @pl.when(behind == 1)
        def _():
            a_below(block).wait_send()
            c_below(block).wait_send()

        @pl.when((behind == 1) & (z < nz - 1))
        def _():
            raw_above(block, toks.at[block]).wait_send()
            b_above(block).wait_send()

        @pl.when((behind == 0) & (z > 0))
        def _():
            raw_below(block, toks.at[block]).wait_send()
            b_below(block).wait_send()

    def drain_all(i, carry):
        both_sides(z, nz, i, drain)
        return carry

    lax.fori_loop(1, nz, drain_all, 0)


def split_columns(width, share):
    return max(LANES, min(width - LANES, int(width * share) // LANES * LANES))


def experts(normed, stream, onehot, share, gate_local, up_local, down_local):
    n_sp = lax.axis_size("sp")
    nz = lax.axis_size("tp") // CORES
    tok, width = normed.shape
    units = gate_local.shape[1]
    slots = onehot.shape[1]
    capp = slots // n_sp
    ka = split_columns(width, DISPATCH_SHARE)
    na = split_columns(width, RETURN_SHARE)
    kb, nb = width - ka, width - na
    vmem = pl.BlockSpec(memory_space=pltpu.VMEM)
    anywhere = pl.BlockSpec(memory_space=pltpu.HBM)
    dma = pltpu.SemaphoreType.DMA
    bf = jnp.bfloat16
    line = [dma((nz,))] * 4
    return pl.pallas_call(
        functools.partial(expert_kernel, n_sp, nz),
        out_shape=jax.ShapeDtypeStruct((tok, width), bf),
        in_specs=[vmem] * 4 + [anywhere] * 3,
        out_specs=vmem,
        scratch_shapes=[
            pltpu.VMEM((width, CORES * units), bf),
            pltpu.VMEM((width, CORES * units), bf),
            pltpu.VMEM((CORES * units, width), bf),
            pltpu.VMEM((nz, tok, ka), bf),
            pltpu.VMEM((nz, n_sp, capp, ka), bf),
            pltpu.VMEM((n_sp, capp, kb), bf),
            pltpu.VMEM((nz, n_sp, capp, ka), bf),
            pltpu.VMEM((nz, n_sp, capp, kb), bf),
            pltpu.VMEM((slots, CORES * units), bf),
            pltpu.VMEM((nz, n_sp, capp, na), bf),
            pltpu.VMEM((nz, n_sp, capp, nb), bf),
            pltpu.VMEM((nz, n_sp, capp, na), bf),
            pltpu.VMEM((n_sp, capp, nb), bf),
            pltpu.VMEM((nz, tok, na), bf),
            pltpu.VMEM((nz, tok, na), bf),
            pltpu.VMEM((nz, tok, na), bf),
            pltpu.VMEM((nz, n_sp, capp, nb), bf),
            pltpu.VMEM((nz, n_sp, capp, nb), bf),
        ]
        + [dma((3,))] * 3
        + line
        + [dma((nz, n_sp))] * 2
        + [dma((n_sp,))] * 2
        + line
        + [dma((nz, n_sp))] * 2
        + [dma((n_sp,))] * 2
        + line
        + line,
        compiler_params=pltpu.CompilerParams(
            collective_id=0, has_side_effects=True, vmem_limit_bytes=48 * MIB
        ),
        name="experts",
    )(normed, stream, onehot, share, gate_local, up_local, down_local)


def tables(n_sp, nz, tok, capp, c, routes, rw_all, onehot, share):
    choose = routes.shape[0]
    epad = round_up(n_sp, 16)
    earlier = lax.broadcasted_iota(jnp.int32, (tok, tok), 0) < lax.broadcasted_iota(
        jnp.int32, (tok, tok), 1
    )
    earlier = jnp.where(earlier, 1.0, 0.0).astype(jnp.bfloat16)
    same = lax.broadcasted_iota(jnp.int32, (tok, tok), 0) == lax.broadcasted_iota(
        jnp.int32, (tok, tok), 1
    )
    same = jnp.where(same, 1.0, 0.0).astype(jnp.bfloat16)
    which = lax.broadcasted_iota(jnp.int32, (epad, tok), 0)
    place_in = lax.broadcasted_iota(jnp.int32, (capp, tok), 0).astype(jnp.float32)
    for b in range(nz):
        first = routes[:, (CORES * b) * tok : (CORES * b + 1) * tok]
        second = routes[:, (CORES * b + 1) * tok : (CORES * b + 2) * tok]
        ids = jnp.where(c == 0, first, second)
        weight = jnp.zeros((epad, tok), jnp.float32)
        member = jnp.zeros((epad, tok), jnp.float32)
        for m in range(choose):
            named = ids[m : m + 1, :] == which
            member = jnp.where(named, 1.0, member)
            weight = jnp.where(named, rw_all[b, m : m + 1, :tok], weight)
        rank = dot(member.astype(jnp.bfloat16), earlier)
        rank = jnp.where(member > 0.0, rank, -1.0)
        shares = []
        for e in range(n_sp):
            hit = place_in == rank[e : e + 1, :]
            onehot[b, e * capp : (e + 1) * capp, :] = jnp.where(hit, 1.0, 0.0).astype(jnp.bfloat16)
            shares.append(jnp.where(hit, weight[e : e + 1, :], 0.0).astype(jnp.bfloat16))
        turned = lax.dot_general(
            same,
            jnp.concatenate(shares, axis=0),
            (((1,), (1,)), ((), ())),
            preferred_element_type=jnp.float32,
        )
        share[b] = turned.astype(jnp.bfloat16)


def front_kernel(
    n_sp, n_tp, tok, capp, q, k, v, sink_in, residual, weight, gain_in, routes_in, rweight,
    normed, stream, onehot, share,
    q_all, k_all, v_all, k_tail, v_tail, att, got, w_all, res, acc, rw_src, rw_all,
    sink, gain, routes, rw_in,
    in_s, o_s, t_s, t_r, a_s, a_r, g_s, g_r,
):
    sp, z, c = place()
    tp = z * CORES + c
    nz = n_tp // CORES
    span, kv_cols = k.shape
    cols = q.shape[1]
    width = weight.shape[1]
    kv_local = kv_cols // HEAD
    group = cols // kv_cols
    blocks = span // WINDOW
    pieces = WINDOW // tok
    scale = HEAD ** (-0.5)
    body = pl.ds(WINDOW, span)
    copies = [
        pltpu.make_async_copy(k, k_all.at[body], in_s.at[0]),
        pltpu.make_async_copy(v, v_all.at[body], in_s.at[1]),
        pltpu.make_async_copy(q, q_all, in_s.at[2]),
        pltpu.make_async_copy(rweight, rw_in, in_s.at[3]),
        pltpu.make_async_copy(sink_in, sink, in_s.at[4]),
        pltpu.make_async_copy(routes_in, routes, in_s.at[5]),
        pltpu.make_async_copy(residual, res, in_s.at[6]),
        pltpu.make_async_copy(gain_in, gain, in_s.at[7]),
    ]
    for copy in copies:
        copy.start()

    def out_rows(p):
        rows = pl.ds(pl.multiple_of(p * cols, cols), cols)
        return pltpu.make_async_copy(weight.at[rows], w_all.at[rows], o_s.at[p])

    barrier = pltpu.get_barrier_semaphore()
    for d in range(1, n_tp):
        pl.semaphore_signal(
            barrier, inc=1, device_id=(sp, lax.rem(tp + d, n_tp)), device_id_type=MESH
        )

    @pl.when(sp > 0)
    def _():
        pl.semaphore_signal(barrier, inc=1, device_id=(sp - 1, tp), device_id_type=MESH)

    @pl.when(sp < n_sp - 1)
    def _():
        pl.semaphore_signal(barrier, inc=1, device_id=(sp + 1, tp), device_id_type=MESH)

    rw_src[...] = jnp.zeros_like(rw_src)
    copies[3].wait()
    rw_src[: rweight.shape[0], :tok] = rw_in[...]
    rw_all[z] = rw_src[...]
    beside = jnp.where(sp > 0, 1, 0) + jnp.where(sp < n_sp - 1, 1, 0)
    pl.semaphore_wait(barrier, n_tp - 1 + beside)
    ahead = (lax.rem(sp + 1, n_sp), tp)
    last = pl.ds(span, WINDOW)
    tails = (
        send(k_all.at[last], k_tail, t_s.at[0], t_r.at[0], ahead),
        send(v_all.at[last], v_tail, t_s.at[1], t_r.at[1], ahead),
    )
    copies[0].wait()
    copies[1].wait()

    @pl.when(sp < n_sp - 1)
    def _():
        for copy in tails:
            copy.start()

    def tell(d):
        there = lax.rem(z + d, nz)
        return send(rw_src, rw_all.at[z], g_s.at[d], g_r.at[z], (sp, there * CORES + c))

    def told(d):
        there = lax.rem(z + d, nz)
        return send(rw_src, rw_all.at[there], g_s.at[d], g_r.at[there], (sp, there * CORES + c))

    for d in range(1, nz):
        tell(d).start()
    copies[2].wait()
    copies[4].wait()
    for p in range(n_tp):
        out_rows(p).start()

    row = lax.broadcasted_iota(jnp.int32, (WINDOW, 2 * WINDOW), 0)
    col = lax.broadcasted_iota(jnp.int32, (WINDOW, 2 * WINDOW), 1)
    distance = row + WINDOW - col
    banded = (distance >= 0) & (distance < WINDOW)
    low = z < nz // 2
    half = max(1, blocks // 2)

    def to_owner(dest):
        at = pl.multiple_of(dest * tok, tok)
        return send(
            att.at[pl.ds(at, tok)], got.at[tp], a_s.at[dest], a_r.at[tp], (sp, dest)
        )

    def attend(i, carry):
        turned = jnp.where(i < half, lax.rem(i + 1, half), i)
        block = jnp.where(low, blocks - 1 - i, turned)

        @pl.when(block == 0)
        def _():
            @pl.when(sp > 0)
            def _():
                for copy in tails:
                    copy.wait_recv()
                k_all[pl.ds(0, WINDOW), :] = k_tail[...]
                v_all[pl.ds(0, WINDOW), :] = v_tail[...]

            @pl.when(sp == 0)
            def _():
                k_all[pl.ds(0, WINDOW), :] = jnp.zeros((WINDOW, kv_cols), jnp.bfloat16)
                v_all[pl.ds(0, WINDOW), :] = jnp.zeros((WINDOW, kv_cols), jnp.bfloat16)

        at = pl.multiple_of(block * WINDOW, WINDOW)
        start = jnp.where((sp == 0) & (block == 0), WINDOW, 0)
        allowed = banded & (col >= start)
        band = pl.ds(at, 2 * WINDOW)
        for g in range(kv_local):
            keys = k_all[band, g * HEAD : (g + 1) * HEAD]
            values = v_all[band, g * HEAD : (g + 1) * HEAD]
            heads = []
            for m in range(group):
                h = g * group + m
                query = q_all[pl.ds(at, WINDOW), h * HEAD : (h + 1) * HEAD] * jnp.bfloat16(scale)
                scores = lax.dot_general(
                    query, keys, (((1,), (1,)), ((), ())), preferred_element_type=jnp.float32
                )
                logits = jnp.where(allowed, scores, -jnp.inf)
                top = jnp.maximum(jnp.max(logits, axis=-1, keepdims=True), sink[h])
                raised = jnp.exp(logits - top)
                total = jnp.sum(raised, axis=-1, keepdims=True) + jnp.exp(sink[h] - top)
                probs = (raised * (1.0 / total)).astype(jnp.bfloat16)
                heads.append(dot(probs, values))
            att[pl.ds(at, WINDOW), g * group * HEAD : (g + 1) * group * HEAD] = jnp.concatenate(
                heads, axis=1
            ).astype(jnp.bfloat16)
        for piece in range(pieces):
            dest = block * pieces + piece

            @pl.when(dest != tp)
            def _():
                to_owner(dest).start()

        return carry

    lax.fori_loop(0, blocks, attend, 0)
    for d in range(1, nz):
        told(d).wait_recv()
    copies[5].wait()
    tables(n_sp, nz, tok, capp, c, routes, rw_all, onehot, share)
    got[tp] = att[pl.ds(pl.multiple_of(tp * tok, tok), tok), :]
    copies[6].wait()
    copies[7].wait()
    wide = math.gcd(width, 512)

    def begin(at):
        acc[:, at] = res[:, at].astype(jnp.float32)

    tiled(width, wide, begin)
    for p in range(n_tp):
        out_rows(p).wait()

    def mix(i, carry):
        p = jnp.where(low, n_tp - 1 - i, i)

        @pl.when(tp != p)
        def _():
            send(att.at[pl.ds(0, tok)], got.at[p], a_s.at[p], a_r.at[p], (sp, p)).wait_recv()

        rows = pl.ds(pl.multiple_of(p * cols, cols), cols)

        def one(at):
            acc[:, at] = acc[:, at] + dot(got[p], w_all[rows, at])

        tiled(width, wide, one)
        return carry

    lax.fori_loop(0, n_tp, mix, 0)
    squares = jnp.zeros((tok, 1), jnp.float32)
    for t in range(width // wide):
        at = slice(t * wide, (t + 1) * wide)
        held = acc[:, at].astype(jnp.bfloat16)
        stream[:, at] = held
        held32 = held.astype(jnp.float32)
        squares = squares + jnp.sum(held32 * held32, axis=-1, keepdims=True)
    root = lax.rsqrt(squares * (1.0 / width) + eps)
    for t in range(width // wide):
        at = slice(t * wide, (t + 1) * wide)
        normed[:, at] = (stream[:, at].astype(jnp.float32) * root * gain[:, at]).astype(
            jnp.bfloat16
        )
    for p in range(n_tp):
        @pl.when(tp != p)
        def _():
            to_owner(p).wait_send()

    for d in range(1, nz):
        tell(d).wait_send()

    @pl.when(sp < n_sp - 1)
    def _():
        for copy in tails:
            copy.wait_send()


def front(query_heads, key_heads, value_heads, sink_logit, residual, out_weight, norm_gain, routes,
          route_weight):
    n_sp, n_tp = lax.axis_size("sp"), lax.axis_size("tp")
    nz = n_tp // CORES
    span, cols = query_heads.shape
    kv_cols = key_heads.shape[1]
    tok, width = residual.shape
    choose = routes.shape[1]
    capp = round_up(max(2, 5 * tok * choose // (4 * n_sp)), 16)
    slots = n_sp * capp
    vmem = pl.BlockSpec(memory_space=pltpu.VMEM)
    anywhere = pl.BlockSpec(memory_space=pltpu.HBM)
    dma = pltpu.SemaphoreType.DMA
    bf = jnp.bfloat16
    return pl.pallas_call(
        functools.partial(front_kernel, n_sp, n_tp, tok, capp),
        out_shape=(
            jax.ShapeDtypeStruct((tok, width), bf),
            jax.ShapeDtypeStruct((tok, width), bf),
            jax.ShapeDtypeStruct((nz, slots, tok), bf),
            jax.ShapeDtypeStruct((nz, tok, slots), bf),
        ),
        in_specs=[anywhere] * 9,
        out_specs=(vmem,) * 4,
        scratch_shapes=[
            pltpu.VMEM((span, cols), bf),
            pltpu.VMEM((span + WINDOW, kv_cols), bf),
            pltpu.VMEM((span + WINDOW, kv_cols), bf),
            pltpu.VMEM((WINDOW, kv_cols), bf),
            pltpu.VMEM((WINDOW, kv_cols), bf),
            pltpu.VMEM((span, cols), bf),
            pltpu.VMEM((n_tp, tok, cols), bf),
            pltpu.VMEM((n_tp * cols, width), bf),
            pltpu.VMEM((tok, width), bf),
            pltpu.VMEM((tok, width), jnp.float32),
            pltpu.VMEM((8, LANES), jnp.float32),
            pltpu.VMEM((nz, 8, LANES), jnp.float32),
            pltpu.SMEM(sink_logit.shape, jnp.float32),
            pltpu.VMEM((1, width), jnp.float32),
            pltpu.VMEM(routes.shape[::-1], routes.dtype),
            pltpu.VMEM(route_weight.shape[::-1], jnp.float32),
            dma((8,)),
            dma((n_tp,)),
            dma((2,)),
            dma((2,)),
            dma((n_tp,)),
            dma((n_tp,)),
            dma((nz,)),
            dma((nz,)),
        ],
        compiler_params=pltpu.CompilerParams(
            collective_id=2, has_side_effects=True, vmem_limit_bytes=32 * MIB
        ),
        name="front",
    )(*[
        pltpu.with_memory_space_constraint(x, pltpu.HBM)
        for x in (
            query_heads, key_heads, value_heads, sink_logit, residual, out_weight,
            norm_gain.reshape(1, -1), routes.T, route_weight.T,
        )
    ])


def local(
    query_heads,
    key_heads,
    value_heads,
    sink_logit,
    residual,
    out_weight,
    norm_gain,
    routes,
    route_weight,
    gate_weight,
    up_weight,
    down_weight,
):
    normed, stream, onehot, share = front(
        query_heads, key_heads, value_heads, sink_logit, residual, out_weight, norm_gain, routes,
        route_weight,
    )
    return experts(normed, stream, onehot, share, gate_weight[0], up_weight[0], down_weight[0])


def solution(mesh):
    placed = (
        P("sp", "tp"),
        P("sp", "tp"),
        P("sp", "tp"),
        P("tp"),
        P(("sp", "tp"), None),
        P(),
        P(),
        P("sp", None),
        P(("sp", "tp"), None),
        P("sp", None, "tp"),
        P("sp", None, "tp"),
        P("sp", "tp", None),
    )
    return jax.shard_map(
        local, mesh=mesh, in_specs=placed, out_specs=P(("sp", "tp"), None), check_vma=False
    )
```

```python
import functools
import math

import jax
import jax.numpy as jnp
from jax import lax
from jax.experimental import pallas as pl
from jax.experimental.pallas import tpu as pltpu
from jax.sharding import PartitionSpec as P

HEAD = 64
WINDOW = 128


eps = 1e-06
clamp_limit = 7.0
sigmoid_alpha = 1.702


MESH = pl.DeviceIdType.MESH
CORES = 2
LANES = 128
SPARE = 2 * 1024 * 1024


def round_up(value, unit):
    return (value + unit - 1) // unit * unit


def place():
    tp = lax.axis_index("tp")
    return lax.axis_index("sp"), tp // CORES, lax.rem(tp, CORES)


def partner_of(sp, d, n_sp):
    if n_sp & (n_sp - 1):
        return lax.rem(sp + d, n_sp)
    total, bit = 0, 1
    while bit < n_sp:
        total = total + lax.rem(sp // bit + d // bit, 2) * bit
        bit *= 2
    return total


def source_of(sp, d, n_sp):
    if n_sp & (n_sp - 1):
        return lax.rem(sp + n_sp - d, n_sp)
    return partner_of(sp, d, n_sp)


def send(src, dst, send_sem, recv_sem, device):
    return pltpu.make_async_remote_copy(
        src_ref=src,
        dst_ref=dst,
        send_sem=send_sem,
        recv_sem=recv_sem,
        device_id=device,
        device_id_type=MESH,
    )


def dot(a, b):
    return jnp.dot(a, b, preferred_element_type=jnp.float32)


def tiled(extent, tile, visit):
    for start in range(0, extent, tile):
        visit(pl.ds(start, min(tile, extent - start)))


def shifted(cols, offset):
    return pl.ds(cols.start + offset, cols.size)


RAW, NEAR, SERVE, PUSH, CHAIN, RELAY = range(1, 7)
KINDS = 8
PER_WORD = 5


def sides(nz, z, away):
    return [b for b in ((z + away, z - away) if away else (z,)) if 0 <= b < nz]


def plain_order(nz, z):
    order = []
    for i in range(1, nz):
        order += [(RAW, b) for b in sides(nz, z, i)]
        order += [(NEAR, b) for b in sides(nz, z, i - 1)]
        if i > 1:
            order += [(SERVE, b) for b in sides(nz, z, i - 2)]
    order += [(SERVE, b) for b in sides(nz, z, nz - 2)]
    order += [(NEAR, b) for b in sides(nz, z, nz - 1)]
    order += [(SERVE, b) for b in sides(nz, z, nz - 1)]
    for i in range(nz - 1):
        order += [(PUSH, b) for b in sides(nz, z, nz - 1 - i)]
    order.append((PUSH, z))
    order += [(CHAIN, b) for b in sides(nz, z, nz - 1)]
    for away in range(nz - 1, 0, -1):
        order += [(CHAIN, b) for b in sides(nz, z, away - 1)]
        order += [(RELAY, b) for b in sides(nz, z, away)]
    return order


ORDERS = {
    4: [
        [
            (NEAR, 0), (RAW, 1), (RAW, 2), (RAW, 3), (NEAR, 1),
            (SERVE, 1), (CHAIN, 1), (SERVE, 0), (NEAR, 3), (SERVE, 3),
            (PUSH, 3), (CHAIN, 3), (NEAR, 2), (SERVE, 2), (PUSH, 2),
            (PUSH, 1), (CHAIN, 2), (RELAY, 3), (PUSH, 0), (RELAY, 2),
            (RELAY, 1), (CHAIN, 0),
        ],
        [
            (RAW, 0), (RAW, 2), (NEAR, 0), (RAW, 3), (NEAR, 1),
            (NEAR, 3), (NEAR, 2), (SERVE, 2), (SERVE, 1), (PUSH, 2),
            (SERVE, 0), (SERVE, 3), (CHAIN, 3), (PUSH, 3), (CHAIN, 2),
            (PUSH, 0), (RELAY, 3), (PUSH, 1), (CHAIN, 1), (CHAIN, 0),
            (RELAY, 2), (RELAY, 0),
        ],
    ],
}
DISPATCH_SHARE = 0.6875
RETURN_SHARE = 0.75


def order_of(nz, z):
    if nz not in ORDERS:
        return plain_order(nz, z)
    if z < nz // 2:
        return ORDERS[nz][z]
    return [(kind, nz - 1 - b) for kind, b in ORDERS[nz][nz - 1 - z]]


def order_words(nz):
    orders = [order_of(nz, z) for z in range(nz)]
    words = round_up(max(len(order) for order in orders), PER_WORD) // PER_WORD
    table = []
    for order in orders:
        codes = [b * KINDS + kind for kind, b in order]
        codes += [0] * (words * PER_WORD - len(codes))
        base = KINDS * 8
        table.append([
            sum(code * base**i for i, code in enumerate(codes[w * PER_WORD : (w + 1) * PER_WORD]))
            for w in range(words)
        ])
    return table, words


def both_sides(z, nz, away, visit):
    def one(behind, carry):
        block = z + away * (1 - 2 * behind)

        @pl.when((block >= 0) & (block < nz))
        def _():
            visit(block, behind)

        return carry

    lax.fori_loop(0, 2, one, 0)


def expert_kernel(
    n_sp, nz, swap, normed, stream, onehot, share, out,
    gate_v, up_v, down_v, toks, comp_a, comp_b, rows_a, rows_b, hid,
    sums_a, sums_b, back_a, back_b, a_out, a_up, a_dn, b_up, b_dn,
    ru_s, ru_r, rd_s, rd_r, xa_s, xa_r, xb_s, xb_r,
    bu_s, bu_r, bd_s, bd_r, ya_s, ya_r, yb_s, yb_r,
    au_s, au_r, ad_s, ad_r, cu_s, cu_r, cd_s, cd_r,
):
    sp, z, c = place()
    tp = z * CORES + c
    above = (sp, lax.rem(z + 1, nz) * CORES + c)
    below = (sp, lax.rem(z + nz - 1, nz) * CORES + c)
    capp, ka, kb = rows_a.shape[2], rows_a.shape[3], rows_b.shape[3]
    na, nb = sums_a.shape[3], sums_b.shape[3]
    slots = n_sp * capp
    units = gate_v.shape[1] // CORES
    tile, wide = 512, 512

    def raw_above(block, src):
        return send(src, toks.at[block], ru_s.at[block], ru_r.at[block], above)

    def raw_below(block, src):
        return send(src, toks.at[block], rd_s.at[block], rd_r.at[block], below)

    own_raw = normed.at[:, pl.ds(0, ka)]

    @pl.when(z < nz - 1)
    def _():
        raw_above(z, own_raw).start()

    @pl.when(z > 0)
    def _():
        raw_below(z, own_raw).start()

    def xa_to(block, d):
        e = partner_of(sp, d, n_sp)
        return send(
            comp_a.at[block, e], rows_a.at[block, sp], xa_s.at[block, d], xa_r.at[block, d], (e, tp)
        )

    def xa_from(block, d):
        e = source_of(sp, d, n_sp)
        return send(
            comp_a.at[block, e], rows_a.at[block, e], xa_s.at[block, d], xa_r.at[block, d], (e, tp)
        )

    def xb_to(d):
        e = partner_of(sp, d, n_sp)
        return send(comp_b.at[e], rows_b.at[z, sp], xb_s.at[d], xb_r.at[d], (e, tp))

    def xb_from(d):
        e = source_of(sp, d, n_sp)
        return send(comp_b.at[e], rows_b.at[z, e], xb_s.at[d], xb_r.at[d], (e, tp))

    def b_above(block):
        return send(rows_b.at[block], rows_b.at[block], bu_s.at[block], bu_r.at[block], above)

    def b_below(block):
        return send(rows_b.at[block], rows_b.at[block], bd_s.at[block], bd_r.at[block], below)

    def deal_b(cols):
        picked = dot(onehot[z], normed[:, shifted(cols, ka)])
        comp_b[:, :, cols] = picked.astype(jnp.bfloat16).reshape(n_sp, capp, cols.size)

    tiled(kb, tile, deal_b)
    for d in range(1, n_sp):
        xb_to(d).start()
    rows_b[z, sp] = comp_b[sp]

    def deal(block, src):
        def one(cols):
            picked = dot(onehot[block], src[:, cols])
            comp_a[block, :, :, cols] = picked.astype(jnp.bfloat16).reshape(n_sp, capp, cols.size)

        tiled(ka, tile, one)
        for d in range(1, n_sp):
            xa_to(block, d).start()
        rows_a[block, sp] = comp_a[block, sp]

    deal(z, normed)

    def spread_own():
        for d in range(1, n_sp):
            xb_from(d).wait_recv()

        @pl.when(z < nz - 1)
        def _():
            b_above(z).start()

        @pl.when(z > 0)
        def _():
            b_below(z).start()

    def gather_raw(block, behind):
        @pl.when(behind == 1)
        def _():
            raw_above(block, toks.at[block]).wait_recv()

            @pl.when(z < nz - 1)
            def _():
                raw_above(block, toks.at[block]).start()

        @pl.when(behind == 0)
        def _():
            raw_below(block, toks.at[block]).wait_recv()

            @pl.when(z > 0)
            def _():
                raw_below(block, toks.at[block]).start()

        deal(block, toks.at[block])

    def gather_b(block, behind):
        @pl.when(behind == 1)
        def _():
            b_above(block).wait_recv()

            @pl.when(z < nz - 1)
            def _():
                b_above(block).start()

        @pl.when(behind == 0)
        def _():
            b_below(block).wait_recv()

            @pl.when(z > 0)
            def _():
                b_below(block).start()

    unit = min(256, CORES * units)

    def serve(block):
        for d in range(1, n_sp):
            xa_from(block, d).wait_recv()

        def one(cols):
            tile_a = rows_a[block].reshape(slots, ka)
            tile_b = rows_b[block].reshape(slots, kb)
            gate_pre = dot(tile_a, gate_v[:ka, cols]) + dot(tile_b, gate_v[ka:, cols])
            upward = dot(tile_a, up_v[:ka, cols]) + dot(tile_b, up_v[ka:, cols])
            capped = jnp.minimum(gate_pre, clamp_limit)
            linear = jnp.clip(upward, -clamp_limit, clamp_limit)
            gated = capped * jax.nn.sigmoid(sigmoid_alpha * capped)
            hid[:, cols] = (gated * (linear + 1.0)).astype(jnp.bfloat16)

        tiled(CORES * units, unit, one)

        def part_a(cols):
            part = dot(hid[...], down_v[:, cols]).astype(jnp.bfloat16)
            sums_a[block, :, :, cols] = part.reshape(n_sp, capp, cols.size)

        def part_b(cols):
            part = dot(hid[...], down_v[:, shifted(cols, na)]).astype(jnp.bfloat16)
            sums_b[block, :, :, cols] = part.reshape(n_sp, capp, cols.size)

        tiled(na, wide, part_a)
        tiled(nb, wide, part_b)

    def ya_to(block, d):
        e = partner_of(sp, d, n_sp)
        return send(
            sums_a.at[block, e], back_a.at[block, sp], ya_s.at[block, d], ya_r.at[block, d], (e, tp)
        )

    def ya_from(block, d):
        e = source_of(sp, d, n_sp)
        return send(
            sums_a.at[block, e], back_a.at[block, e], ya_s.at[block, d], ya_r.at[block, d], (e, tp)
        )

    def yb_to(d):
        e = partner_of(sp, d, n_sp)
        return send(sums_b.at[z, e], back_b.at[sp], yb_s.at[d], yb_r.at[d], (e, tp))

    def yb_from(d):
        e = source_of(sp, d, n_sp)
        return send(sums_b.at[z, e], back_b.at[e], yb_s.at[d], yb_r.at[d], (e, tp))

    def a_above(block):
        return send(a_out.at[block], a_up.at[block], au_s.at[block], au_r.at[block], above)

    def a_below(block):
        return send(a_out.at[block], a_dn.at[block], ad_s.at[block], ad_r.at[block], below)

    def c_above(block):
        return send(sums_b.at[block], b_up.at[block], cu_s.at[block], cu_r.at[block], above)

    def c_below(block):
        return send(sums_b.at[block], b_dn.at[block], cd_s.at[block], cd_r.at[block], below)

    def push(block):
        for d in range(1, n_sp):
            ya_to(block, d).start()
        back_a[block, sp] = sums_a[block, sp]

    def add_b(block, arrived):
        total = sums_b[block].astype(jnp.float32) + arrived[block].astype(jnp.float32)
        sums_b[block] = total.astype(jnp.bfloat16)

    def relay_b(block, behind):
        @pl.when(behind == 0)
        def _():
            @pl.when(z > 0)
            def _():
                c_above(block).wait_recv()
                add_b(block, b_up)

            c_above(block).start()

        @pl.when(behind == 1)
        def _():
            @pl.when(z < nz - 1)
            def _():
                c_below(block).wait_recv()
                add_b(block, b_dn)

            c_below(block).start()

    def settle_b():
        @pl.when(z > 0)
        def _():
            c_above(z).wait_recv()
            add_b(z, b_up)

        @pl.when(z < nz - 1)
        def _():
            c_below(z).wait_recv()
            add_b(z, b_dn)

        for d in range(1, n_sp):
            yb_to(d).start()
        back_b[sp] = sums_b[z, sp]

    def combined(block, cols):
        return dot(share[block], back_a[block, :, :, cols].reshape(slots, cols.size))

    def relay_a(block, behind):
        for d in range(1, n_sp):
            ya_from(block, d).wait_recv()

        @pl.when(behind == 0)
        def _():
            @pl.when(z > 0)
            def _():
                a_above(block).wait_recv()

            def one(cols):
                total = combined(block, cols)
                total = jnp.where(z > 0, total + a_up[block, :, cols].astype(jnp.float32), total)
                a_out[block, :, cols] = total.astype(jnp.bfloat16)

            tiled(na, wide, one)
            a_above(block).start()

        @pl.when(behind == 1)
        def _():
            @pl.when(z < nz - 1)
            def _():
                a_below(block).wait_recv()

            def one(cols):
                total = combined(block, cols)
                total = jnp.where(
                    z < nz - 1, total + a_dn[block, :, cols].astype(jnp.float32), total
                )
                a_out[block, :, cols] = total.astype(jnp.bfloat16)

            tiled(na, wide, one)
            a_below(block).start()

    swap.wait()
    table, words = order_words(nz)

    def word_of(w):
        word = jnp.int32(0)
        for level in range(nz):
            for at in range(words):
                word = jnp.where((z == level) & (w == at), jnp.int32(table[level][at]), word)
        return word

    def task(i, word):
        kind = lax.rem(word, KINDS)
        block = lax.rem(word // KINDS, 8)
        behind = jnp.where(block < z, 1, 0)
        elsewhere = block != z

        @pl.when(kind == RAW)
        def _():
            gather_raw(block, behind)

        @pl.when((kind == NEAR) & elsewhere)
        def _():
            gather_b(block, behind)

        @pl.when((kind == NEAR) & (block == z))
        def _():
            spread_own()

        @pl.when(kind == SERVE)
        def _():
            serve(block)

        @pl.when(kind == PUSH)
        def _():
            push(block)

        @pl.when((kind == CHAIN) & elsewhere)
        def _():
            relay_b(block, behind)

        @pl.when((kind == CHAIN) & (block == z))
        def _():
            settle_b()

        @pl.when(kind == RELAY)
        def _():
            relay_a(block, behind)

        return word // (KINDS * 8)

    def tasks(w, carry):
        lax.fori_loop(0, PER_WORD, task, word_of(w))
        return carry

    lax.fori_loop(0, words, tasks, 0)

    for d in range(1, n_sp):
        yb_from(d).wait_recv()

    def final_b(cols):
        at = shifted(cols, na)
        total = dot(share[z], back_b[:, :, cols].reshape(slots, cols.size))
        out[:, at] = (stream[:, at].astype(jnp.float32) + total).astype(jnp.bfloat16)

    tiled(nb, wide, final_b)
    for d in range(1, n_sp):
        ya_from(z, d).wait_recv()

    @pl.when(z > 0)
    def _():
        a_above(z).wait_recv()

    @pl.when(z < nz - 1)
    def _():
        a_below(z).wait_recv()

    def final_a(cols):
        total = combined(z, cols)
        total = jnp.where(z > 0, total + a_up[z, :, cols].astype(jnp.float32), total)
        total = jnp.where(z < nz - 1, total + a_dn[z, :, cols].astype(jnp.float32), total)
        out[:, cols] = (stream[:, cols].astype(jnp.float32) + total).astype(jnp.bfloat16)

    tiled(na, wide, final_a)

    for d in range(1, n_sp):
        xb_to(d).wait_send()
        yb_to(d).wait_send()

    def drain_exchange(block):
        for d in range(1, n_sp):
            xa_to(block, d).wait_send()
            ya_to(block, d).wait_send()

    drain_exchange(z)

    @pl.when(z < nz - 1)
    def _():
        raw_above(z, own_raw).wait_send()
        b_above(z).wait_send()

    @pl.when(z > 0)
    def _():
        raw_below(z, own_raw).wait_send()
        b_below(z).wait_send()

    def drain(block, behind):
        drain_exchange(block)

        @pl.when(behind == 0)
        def _():
            a_above(block).wait_send()
            c_above(block).wait_send()

        @pl.when(behind == 1)
        def _():
            a_below(block).wait_send()
            c_below(block).wait_send()

        @pl.when((behind == 1) & (z < nz - 1))
        def _():
            raw_above(block, toks.at[block]).wait_send()
            b_above(block).wait_send()

        @pl.when((behind == 0) & (z > 0))
        def _():
            raw_below(block, toks.at[block]).wait_send()
            b_below(block).wait_send()

    def drain_all(i, carry):
        both_sides(z, nz, i, drain)
        return carry

    lax.fori_loop(1, nz, drain_all, 0)


def held_bytes(scratch):
    total = 0
    for ref in scratch:
        if getattr(ref, "memory_space", None) == pltpu.VMEM:
            item = jnp.dtype(ref.dtype).itemsize
            lead = math.prod(ref.shape[:-2])
            rows = round_up(ref.shape[-2], 32 // item)
            total += lead * rows * round_up(ref.shape[-1], LANES) * item
    return total


def split_columns(width, share):
    return max(LANES, min(width - LANES, int(width * share) // LANES * LANES))


class Swap:
    def __init__(self, place_at, weights, held, sems):
        sp, z, c = place_at
        peer_core = (sp, z * CORES + 1 - c)
        units = weights[0].shape[1]
        mine = pl.ds(pl.multiple_of(c * units, units), units)
        gate_v, up_v, down_v = held
        into = (gate_v.at[:, mine], up_v.at[:, mine], down_v.at[mine, :])
        w_l, w_s, w_r = sems
        self.copies = [
            pltpu.make_async_copy(src, dst, w_l.at[i]) for i, (src, dst) in enumerate(zip(weights, into))
        ] + [
            send(src, dst, w_s.at[i], w_r.at[i], peer_core)
            for i, (src, dst) in enumerate(zip(weights, into))
        ]

    def start(self):
        for copy in self.copies:
            copy.start()

    def wait(self):
        for copy in self.copies:
            copy.wait()


def tables(n_sp, nz, tok, capp, c, routes, rw_all, onehot, share):
    choose = routes.shape[0]
    epad = round_up(n_sp, 16)
    earlier = lax.broadcasted_iota(jnp.int32, (tok, tok), 0) < lax.broadcasted_iota(
        jnp.int32, (tok, tok), 1
    )
    earlier = jnp.where(earlier, 1.0, 0.0).astype(jnp.bfloat16)
    same = lax.broadcasted_iota(jnp.int32, (tok, tok), 0) == lax.broadcasted_iota(
        jnp.int32, (tok, tok), 1
    )
    same = jnp.where(same, 1.0, 0.0).astype(jnp.bfloat16)
    which = lax.broadcasted_iota(jnp.int32, (epad, tok), 0)
    place_in = lax.broadcasted_iota(jnp.int32, (capp, tok), 0).astype(jnp.float32)
    for b in range(nz):
        first = routes[:, (CORES * b) * tok : (CORES * b + 1) * tok]
        second = routes[:, (CORES * b + 1) * tok : (CORES * b + 2) * tok]
        ids = jnp.where(c == 0, first, second)
        weight = jnp.zeros((epad, tok), jnp.float32)
        member = jnp.zeros((epad, tok), jnp.float32)
        for m in range(choose):
            named = ids[m : m + 1, :] == which
            member = jnp.where(named, 1.0, member)
            weight = jnp.where(named, rw_all[b, m : m + 1, :tok], weight)
        rank = dot(member.astype(jnp.bfloat16), earlier)
        rank = jnp.where(member > 0.0, rank, -1.0)
        shares = []
        for e in range(n_sp):
            hit = place_in == rank[e : e + 1, :]
            onehot[b, e * capp : (e + 1) * capp, :] = jnp.where(hit, 1.0, 0.0).astype(jnp.bfloat16)
            shares.append(jnp.where(hit, weight[e : e + 1, :], 0.0).astype(jnp.bfloat16))
        turned = lax.dot_general(
            same,
            jnp.concatenate(shares, axis=0),
            (((1,), (1,)), ((), ())),
            preferred_element_type=jnp.float32,
        )
        share[b] = turned.astype(jnp.bfloat16)


def layer_kernel(
    n_sp, n_tp, tok, capp, q, k, v, sink_in, residual, weight, gain_in, routes_in, rweight,
    gate, up, down, out, normed, stream, onehot, share, gate_v, up_v, down_v,
    q_all, k_all, v_all, k_tail, v_tail, att, got, w_all, res, acc, rw_src, rw_all,
    sink, gain, routes, rw_in,
    in_s, o_s, t_s, t_r, a_s, a_r, g_s, g_r, w_l, w_s, w_r, *rest,
):
    sp, z, c = place()
    tp = z * CORES + c
    nz = n_tp // CORES
    span, kv_cols = k.shape
    cols = q.shape[1]
    width = weight.shape[1]
    kv_local = kv_cols // HEAD
    group = cols // kv_cols
    blocks = span // WINDOW
    pieces = WINDOW // tok
    scale = HEAD ** (-0.5)
    body = pl.ds(WINDOW, span)
    copies = [
        pltpu.make_async_copy(k, k_all.at[body], in_s.at[0]),
        pltpu.make_async_copy(v, v_all.at[body], in_s.at[1]),
        pltpu.make_async_copy(q, q_all, in_s.at[2]),
        pltpu.make_async_copy(rweight, rw_in, in_s.at[3]),
        pltpu.make_async_copy(sink_in, sink, in_s.at[4]),
        pltpu.make_async_copy(routes_in, routes, in_s.at[5]),
        pltpu.make_async_copy(residual, res, in_s.at[6]),
        pltpu.make_async_copy(gain_in, gain, in_s.at[7]),
    ]
    for copy in copies:
        copy.start()

    def out_rows(p):
        rows = pl.ds(pl.multiple_of(p * cols, cols), cols)
        return pltpu.make_async_copy(weight.at[rows], w_all.at[rows], o_s.at[p])

    barrier = pltpu.get_barrier_semaphore()
    for d in range(1, n_tp):
        pl.semaphore_signal(
            barrier, inc=1, device_id=(sp, lax.rem(tp + d, n_tp)), device_id_type=MESH
        )

    for d in range(1, n_sp):
        pl.semaphore_signal(
            barrier, inc=1, device_id=(lax.rem(sp + d, n_sp), tp), device_id_type=MESH
        )
    swap = Swap((sp, z, c), (gate, up, down), (gate_v, up_v, down_v), (w_l, w_s, w_r))
    rw_src[...] = jnp.zeros_like(rw_src)
    copies[3].wait()
    rw_src[: rweight.shape[0], :tok] = rw_in[...]
    rw_all[z] = rw_src[...]
    pl.semaphore_wait(barrier, n_tp - 1 + n_sp - 1)
    ahead = (lax.rem(sp + 1, n_sp), tp)
    last = pl.ds(span, WINDOW)
    tails = (
        send(k_all.at[last], k_tail, t_s.at[0], t_r.at[0], ahead),
        send(v_all.at[last], v_tail, t_s.at[1], t_r.at[1], ahead),
    )
    copies[0].wait()
    copies[1].wait()

    @pl.when(sp < n_sp - 1)
    def _():
        for copy in tails:
            copy.start()

    def tell(d):
        there = lax.rem(z + d, nz)
        return send(rw_src, rw_all.at[z], g_s.at[d], g_r.at[z], (sp, there * CORES + c))

    def told(d):
        there = lax.rem(z + d, nz)
        return send(rw_src, rw_all.at[there], g_s.at[d], g_r.at[there], (sp, there * CORES + c))

    for d in range(1, nz):
        tell(d).start()
    copies[2].wait()
    copies[4].wait()
    for p in range(n_tp):
        out_rows(p).start()

    row = lax.broadcasted_iota(jnp.int32, (WINDOW, 2 * WINDOW), 0)
    col = lax.broadcasted_iota(jnp.int32, (WINDOW, 2 * WINDOW), 1)
    distance = row + WINDOW - col
    banded = (distance >= 0) & (distance < WINDOW)
    low = z < nz // 2
    half = max(1, blocks // 2)

    own_cols = pl.ds(pl.multiple_of(tp * cols, cols), cols)

    def to_owner(dest):
        at = pl.multiple_of(dest * tok, tok)
        return send(
            att.at[pl.ds(at, tok)], got.at[:, own_cols], a_s.at[dest], a_r.at[tp], (sp, dest)
        )

    def attend(i, carry):
        turned = jnp.where(i < half, lax.rem(i + 1, half), i)
        block = jnp.where(low, blocks - 1 - i, turned)

        @pl.when(block == 0)
        def _():
            @pl.when(sp > 0)
            def _():
                for copy in tails:
                    copy.wait_recv()
                k_all[pl.ds(0, WINDOW), :] = k_tail[...]
                v_all[pl.ds(0, WINDOW), :] = v_tail[...]

            @pl.when(sp == 0)
            def _():
                k_all[pl.ds(0, WINDOW), :] = jnp.zeros((WINDOW, kv_cols), jnp.bfloat16)
                v_all[pl.ds(0, WINDOW), :] = jnp.zeros((WINDOW, kv_cols), jnp.bfloat16)

        at = pl.multiple_of(block * WINDOW, WINDOW)
        start = jnp.where((sp == 0) & (block == 0), WINDOW, 0)
        allowed = banded & (col >= start)
        band = pl.ds(at, 2 * WINDOW)
        for g in range(kv_local):
            keys = k_all[band, g * HEAD : (g + 1) * HEAD]
            values = v_all[band, g * HEAD : (g + 1) * HEAD]
            heads = []
            for m in range(group):
                h = g * group + m
                query = q_all[pl.ds(at, WINDOW), h * HEAD : (h + 1) * HEAD] * jnp.bfloat16(scale)
                scores = lax.dot_general(
                    query, keys, (((1,), (1,)), ((), ())), preferred_element_type=jnp.float32
                )
                logits = jnp.where(allowed, scores, -jnp.inf)
                top = jnp.maximum(jnp.max(logits, axis=-1, keepdims=True), sink[h])
                raised = jnp.exp(logits - top)
                total = jnp.sum(raised, axis=-1, keepdims=True) + jnp.exp(sink[h] - top)
                probs = (raised * (1.0 / total)).astype(jnp.bfloat16)
                heads.append(dot(probs, values))
            att[pl.ds(at, WINDOW), g * group * HEAD : (g + 1) * group * HEAD] = jnp.concatenate(
                heads, axis=1
            ).astype(jnp.bfloat16)
        for piece in range(pieces):
            dest = block * pieces + piece

            @pl.when(dest != tp)
            def _():
                to_owner(dest).start()

        return carry

    lax.fori_loop(0, blocks, attend, 0)
    for d in range(1, nz):
        told(d).wait_recv()
    copies[5].wait()
    tables(n_sp, nz, tok, capp, c, routes, rw_all, onehot, share)
    swap.start()
    got[:, own_cols] = att[pl.ds(pl.multiple_of(tp * tok, tok), tok), :]
    copies[6].wait()
    copies[7].wait()
    wide = math.gcd(width, 512)

    def begin(at):
        acc[:, at] = res[:, at].astype(jnp.float32)

    tiled(width, wide, begin)
    for p in range(n_tp):
        out_rows(p).wait()

    part = n_tp // 2

    def arrived(i, carry):
        p = jnp.where(low, n_tp - 1 - i, i)

        @pl.when(tp != p)
        def _():
            into = got.at[:, pl.ds(pl.multiple_of(p * cols, cols), cols)]
            send(att.at[pl.ds(0, tok)], into, a_s.at[p], a_r.at[p], (sp, p)).wait_recv()

        return carry

    for far in range(2):
        lax.fori_loop(far * part, (far + 1) * part, arrived, 0)
        first = jnp.where(low, (1 - far) * part, far * part) * cols
        rows = pl.ds(pl.multiple_of(first, part * cols), part * cols)

        def one(at):
            acc[:, at] = acc[:, at] + dot(got[:, rows], w_all[rows, at])

        tiled(width, wide, one)

    squares = jnp.zeros((tok, 1), jnp.float32)
    for t in range(width // wide):
        at = slice(t * wide, (t + 1) * wide)
        held = acc[:, at].astype(jnp.bfloat16)
        stream[:, at] = held
        held32 = held.astype(jnp.float32)
        squares = squares + jnp.sum(held32 * held32, axis=-1, keepdims=True)
    root = lax.rsqrt(squares * (1.0 / width) + eps)
    for t in range(width // wide):
        at = slice(t * wide, (t + 1) * wide)
        normed[:, at] = (stream[:, at].astype(jnp.float32) * root * gain[:, at]).astype(
            jnp.bfloat16
        )
    expert_kernel(
        n_sp, nz, swap, normed, stream, onehot, share, out, gate_v, up_v, down_v, *rest
    )
    for p in range(n_tp):
        @pl.when(tp != p)
        def _():
            to_owner(p).wait_send()

    for d in range(1, nz):
        tell(d).wait_send()

    @pl.when(sp < n_sp - 1)
    def _():
        for copy in tails:
            copy.wait_send()


def local(
    query_heads,
    key_heads,
    value_heads,
    sink_logit,
    residual,
    out_weight,
    norm_gain,
    routes,
    route_weight,
    gate_weight,
    up_weight,
    down_weight,
):
    n_sp, n_tp = lax.axis_size("sp"), lax.axis_size("tp")
    nz = n_tp // CORES
    span, cols = query_heads.shape
    kv_cols = key_heads.shape[1]
    tok, width = residual.shape
    choose = routes.shape[1]
    capp = round_up(max(2, 5 * tok * choose // (4 * n_sp)), 16)
    slots = n_sp * capp
    hidden = CORES * gate_weight.shape[2]
    ka = split_columns(width, DISPATCH_SHARE)
    na = split_columns(width, RETURN_SHARE)
    kb, nb = width - ka, width - na
    vmem = pl.BlockSpec(memory_space=pltpu.VMEM)
    inputs = (
        query_heads, key_heads, value_heads, sink_logit, residual, out_weight,
        norm_gain.reshape(1, -1), routes.T, route_weight.T,
        gate_weight[0], up_weight[0], down_weight[0],
    )
    dma = pltpu.SemaphoreType.DMA
    bf = jnp.bfloat16
    line = [dma((nz,))] * 4
    scratch = (
        [
            pltpu.VMEM((tok, width), bf),
            pltpu.VMEM((tok, width), bf),
            pltpu.VMEM((nz, slots, tok), bf),
            pltpu.VMEM((nz, tok, slots), bf),
            pltpu.VMEM((width, hidden), bf),
            pltpu.VMEM((width, hidden), bf),
            pltpu.VMEM((hidden, width), bf),
            pltpu.VMEM((span, cols), bf),
            pltpu.VMEM((span + WINDOW, kv_cols), bf),
            pltpu.VMEM((span + WINDOW, kv_cols), bf),
            pltpu.VMEM((WINDOW, kv_cols), bf),
            pltpu.VMEM((WINDOW, kv_cols), bf),
            pltpu.VMEM((span, cols), bf),
            pltpu.VMEM((tok, n_tp * cols), bf),
            pltpu.VMEM((n_tp * cols, width), bf),
            pltpu.VMEM((tok, width), bf),
            pltpu.VMEM((tok, width), jnp.float32),
            pltpu.VMEM((8, LANES), jnp.float32),
            pltpu.VMEM((nz, 8, LANES), jnp.float32),
            pltpu.SMEM(sink_logit.shape, jnp.float32),
            pltpu.VMEM((1, width), jnp.float32),
            pltpu.VMEM(routes.shape[::-1], routes.dtype),
            pltpu.VMEM(route_weight.shape[::-1], jnp.float32),
            dma((8,)),
            dma((n_tp,)),
            dma((2,)),
            dma((2,)),
            dma((n_tp,)),
            dma((n_tp,)),
            dma((nz,)),
            dma((nz,)),
        ]
        + [dma((3,))] * 3
        + [
            pltpu.VMEM((nz, tok, ka), bf),
            pltpu.VMEM((nz, n_sp, capp, ka), bf),
            pltpu.VMEM((n_sp, capp, kb), bf),
            pltpu.VMEM((nz, n_sp, capp, ka), bf),
            pltpu.VMEM((nz, n_sp, capp, kb), bf),
            pltpu.VMEM((slots, hidden), bf),
            pltpu.VMEM((nz, n_sp, capp, na), bf),
            pltpu.VMEM((nz, n_sp, capp, nb), bf),
            pltpu.VMEM((nz, n_sp, capp, na), bf),
            pltpu.VMEM((n_sp, capp, nb), bf),
            pltpu.VMEM((nz, tok, na), bf),
            pltpu.VMEM((nz, tok, na), bf),
            pltpu.VMEM((nz, tok, na), bf),
            pltpu.VMEM((nz, n_sp, capp, nb), bf),
            pltpu.VMEM((nz, n_sp, capp, nb), bf),
        ]
        + line
        + [dma((nz, n_sp))] * 2
        + [dma((n_sp,))] * 2
        + line
        + [dma((nz, n_sp))] * 2
        + [dma((n_sp,))] * 2
        + line
        + line
    )
    return pl.pallas_call(
        functools.partial(layer_kernel, n_sp, n_tp, tok, capp),
        out_shape=jax.ShapeDtypeStruct((tok, width), bf),
        in_specs=[pl.BlockSpec(memory_space=pltpu.HBM)] * len(inputs),
        out_specs=vmem,
        scratch_shapes=scratch,
        compiler_params=pltpu.CompilerParams(
            collective_id=0, has_side_effects=True, vmem_limit_bytes=held_bytes(scratch) + SPARE
        ),
        name="layer",
    )(*[pltpu.with_memory_space_constraint(x, pltpu.HBM) for x in inputs])


def solution(mesh):
    placed = (
        P("sp", "tp"),
        P("sp", "tp"),
        P("sp", "tp"),
        P("tp"),
        P(("sp", "tp"), None),
        P(),
        P(),
        P("sp", None),
        P(("sp", "tp"), None),
        P("sp", None, "tp"),
        P("sp", None, "tp"),
        P("sp", "tp", None),
    )
    return jax.shard_map(
        local, mesh=mesh, in_specs=placed, out_specs=P(("sp", "tp"), None), check_vma=False
    )
```

```python
import functools
import math

import jax
import jax.numpy as jnp
from jax import lax
from jax.experimental import pallas as pl
from jax.experimental.pallas import tpu as pltpu
from jax.sharding import PartitionSpec as P

HEAD = 64
WINDOW = 128


eps = 1e-06
clamp_limit = 7.0
sigmoid_alpha = 1.702


MESH = pl.DeviceIdType.MESH
CORES = 2
LANES = 128
SPARE = 2 * 1024 * 1024


def round_up(value, unit):
    return (value + unit - 1) // unit * unit


def place():
    tp = lax.axis_index("tp")
    return lax.axis_index("sp"), tp // CORES, lax.rem(tp, CORES)


def partner_of(sp, d, n_sp):
    if n_sp & (n_sp - 1):
        return lax.rem(sp + d, n_sp)
    total, bit = 0, 1
    while bit < n_sp:
        total = total + lax.rem(sp // bit + d // bit, 2) * bit
        bit *= 2
    return total


def source_of(sp, d, n_sp):
    if n_sp & (n_sp - 1):
        return lax.rem(sp + n_sp - d, n_sp)
    return partner_of(sp, d, n_sp)


def send(src, dst, send_sem, recv_sem, device):
    return pltpu.make_async_remote_copy(
        src_ref=src,
        dst_ref=dst,
        send_sem=send_sem,
        recv_sem=recv_sem,
        device_id=device,
        device_id_type=MESH,
    )


def dot(a, b):
    return jnp.dot(a, b, preferred_element_type=jnp.float32)


def tiled(extent, tile, visit):
    for start in range(0, extent, tile):
        visit(pl.ds(start, min(tile, extent - start)))


def shifted(cols, offset):
    return pl.ds(cols.start + offset, cols.size)


CHUNKS = 2
NEAR, SERVE = 1, 2
RAW = (3, 4)
CHAIN = 5
PUSH = (6, 7)
RELAY = (8, 9)
LAST_IN = 4
KINDS = 16
BLOCKS = 64
PER_WORD = 3


def sides(nz, z, away):
    return [b for b in ((z + away, z - away) if away else (z,)) if 0 <= b < nz]


def plain_order(nz, z):
    order = []
    for i in range(1, nz):
        order += [(RAW[j], b) for b in sides(nz, z, i) for j in range(CHUNKS)]
        order += [(NEAR, b) for b in sides(nz, z, i - 1)]
        if i > 1:
            order += [(SERVE, b) for b in sides(nz, z, i - 2)]
    order += [(SERVE, b) for b in sides(nz, z, nz - 2)]
    order += [(NEAR, b) for b in sides(nz, z, nz - 1)]
    order += [(SERVE, b) for b in sides(nz, z, nz - 1)]
    for away in range(nz - 1, -1, -1):
        order += [(PUSH[j], b) for b in sides(nz, z, away) for j in range(CHUNKS)]
    order += [(CHAIN, b) for b in sides(nz, z, nz - 1)]
    for away in range(nz - 1, 0, -1):
        order += [(CHAIN, b) for b in sides(nz, z, away - 1)]
        order += [(RELAY[j], b) for b in sides(nz, z, away) for j in range(CHUNKS)]
    return order


ORDERS = {
    4: [
        [
            (RAW[1], 1), (RAW[0], 1), (RAW[0], 2), (NEAR, 0), (RAW[1], 2),
            (NEAR, 1), (SERVE, 1), (RAW[1], 3), (CHAIN, 1), (NEAR, 2),
            (SERVE, 2), (RAW[0], 3), (CHAIN, 2), (PUSH[0], 1), (NEAR, 3),
            (SERVE, 3), (PUSH[1], 3), (PUSH[0], 3), (PUSH[1], 2), (CHAIN, 3),
            (SERVE, 0), (PUSH[0], 2), (RELAY[1], 3), (PUSH[1], 1), (PUSH[0], 0),
            (RELAY[0], 3), (RELAY[1], 2), (RELAY[0], 2), (RELAY[1], 1), (PUSH[1], 0),
            (CHAIN, 0), (RELAY[0], 1),
        ],
        [
            (RAW[0], 2), (RAW[1], 0), (RAW[1], 2), (NEAR, 1), (RAW[1], 3),
            (NEAR, 2), (RAW[0], 0), (RAW[0], 3), (NEAR, 0), (SERVE, 2),
            (NEAR, 3), (SERVE, 1), (PUSH[1], 2), (PUSH[0], 2), (SERVE, 0),
            (SERVE, 3), (PUSH[1], 1), (PUSH[1], 3), (CHAIN, 2), (PUSH[0], 3),
            (PUSH[0], 0), (CHAIN, 3), (RELAY[0], 3), (RELAY[1], 3), (PUSH[1], 0),
            (CHAIN, 0), (RELAY[0], 0), (RELAY[1], 2), (PUSH[0], 1), (RELAY[0], 2),
            (CHAIN, 1), (RELAY[1], 0),
        ],
    ],
}
DISPATCH_SHARE = 0.75
RETURN_SHARE = 0.6875


def order_of(nz, z):
    if nz not in ORDERS:
        return plain_order(nz, z)
    if z < nz // 2:
        return ORDERS[nz][z]
    return [(kind, nz - 1 - b) for kind, b in ORDERS[nz][nz - 1 - z]]


def order_words(nz):
    orders = [order_of(nz, z) for z in range(nz)]
    words = round_up(max(len(order) for order in orders), PER_WORD) // PER_WORD
    table = []
    for order in orders:
        codes = [b * KINDS + kind for kind, b in order]
        codes += [0] * (words * PER_WORD - len(codes))
        base = KINDS * BLOCKS
        table.append([
            sum(code * base**i for i, code in enumerate(codes[w * PER_WORD : (w + 1) * PER_WORD]))
            for w in range(words)
        ])
    return table, words


def both_sides(z, nz, away, visit):
    def one(behind, carry):
        block = z + away * (1 - 2 * behind)

        @pl.when((block >= 0) & (block < nz))
        def _():
            visit(block, behind)

        return carry

    lax.fori_loop(0, 2, one, 0)


def expert_kernel(
    n_sp, nz, swap, normed, stream, onehot, share, out,
    gate_v, up_v, down_v, toks_0, toks_1, comp_a0, comp_a1, comp_b, rows_a0, rows_a1, rows_b, hid,
    sums_a0, sums_a1, sums_b, back_a0, back_a1, back_b, a_out0, a_out1, a_up0, a_up1, a_dn0, a_dn1,
    b_up, b_dn, ru_s, ru_r, rd_s, rd_r, xa_s, xa_r, xb_s, xb_r,
    bu_s, bu_r, bd_s, bd_r, ya_s, ya_r, yb_s, yb_r,
    au_s, au_r, ad_s, ad_r, cu_s, cu_r, cd_s, cd_r,
):
    sp, z, c = place()
    tp = z * CORES + c
    toks, comp_a, rows_a = (toks_0, toks_1), (comp_a0, comp_a1), (rows_a0, rows_a1)
    sums_a, back_a = (sums_a0, sums_a1), (back_a0, back_a1)
    a_out, a_up, a_dn = (a_out0, a_out1), (a_up0, a_up1), (a_dn0, a_dn1)
    above = (sp, lax.rem(z + 1, nz) * CORES + c)
    below = (sp, lax.rem(z + nz - 1, nz) * CORES + c)
    capp, kb, nb = rows_b.shape[2], rows_b.shape[3], sums_b.shape[3]
    ins = spans([ref.shape[-1] for ref in rows_a])
    outs = spans([ref.shape[-1] for ref in sums_a])
    ka, na = normed.shape[1] - kb, normed.shape[1] - nb
    slots = n_sp * capp
    units = gate_v.shape[1] // CORES
    tile, wide = 512, 512

    def raw_above(block, j, src):
        at = j * nz + block
        return send(src, toks[j].at[block], ru_s.at[at], ru_r.at[at], above)

    def raw_below(block, j, src):
        at = j * nz + block
        return send(src, toks[j].at[block], rd_s.at[at], rd_r.at[at], below)

    def own_raw(j):
        return normed.at[:, pl.ds(ins[j].start, ins[j].size)]

    for j in range(CHUNKS):
        @pl.when(z < nz - 1)
        def _():
            raw_above(z, j, own_raw(j)).start()

        @pl.when(z > 0)
        def _():
            raw_below(z, j, own_raw(j)).start()

    def xa_to(block, j, d):
        e = partner_of(sp, d, n_sp)
        at = j * nz + block
        return send(
            comp_a[j].at[block, e], rows_a[j].at[block, sp], xa_s.at[at, d], xa_r.at[at, d], (e, tp)
        )

    def xa_from(block, j, d):
        e = source_of(sp, d, n_sp)
        at = j * nz + block
        return send(
            comp_a[j].at[block, e], rows_a[j].at[block, e], xa_s.at[at, d], xa_r.at[at, d], (e, tp)
        )

    def xb_to(d):
        e = partner_of(sp, d, n_sp)
        return send(comp_b.at[e], rows_b.at[z, sp], xb_s.at[d], xb_r.at[d], (e, tp))

    def xb_from(d):
        e = source_of(sp, d, n_sp)
        return send(comp_b.at[e], rows_b.at[z, e], xb_s.at[d], xb_r.at[d], (e, tp))

    def b_above(block):
        return send(rows_b.at[block], rows_b.at[block], bu_s.at[block], bu_r.at[block], above)

    def b_below(block):
        return send(rows_b.at[block], rows_b.at[block], bd_s.at[block], bd_r.at[block], below)

    def deal_b(cols):
        picked = dot(onehot[z], normed[:, shifted(cols, ka)])
        comp_b[:, :, cols] = picked.astype(jnp.bfloat16).reshape(n_sp, capp, cols.size)

    tiled(kb, tile, deal_b)
    for d in range(1, n_sp):
        xb_to(d).start()
    rows_b[z, sp] = comp_b[sp]

    def deal(block, j, src):
        def one(cols):
            picked = dot(onehot[block], src(cols))
            comp_a[j][block, :, :, cols] = picked.astype(jnp.bfloat16).reshape(
                n_sp, capp, cols.size
            )

        tiled(ins[j].size, tile, one)
        for d in range(1, n_sp):
            xa_to(block, j, d).start()
        rows_a[j][block, sp] = comp_a[j][block, sp]

    for j in range(CHUNKS):
        deal(z, j, lambda cols: normed[:, shifted(cols, ins[j].start)])

    def spread_own():
        for d in range(1, n_sp):
            xb_from(d).wait_recv()

        @pl.when(z < nz - 1)
        def _():
            b_above(z).start()

        @pl.when(z > 0)
        def _():
            b_below(z).start()

    def gather_raw(block, behind, j):
        @pl.when(behind == 1)
        def _():
            raw_above(block, j, toks[j].at[block]).wait_recv()

            @pl.when(z < nz - 1)
            def _():
                raw_above(block, j, toks[j].at[block]).start()

        @pl.when(behind == 0)
        def _():
            raw_below(block, j, toks[j].at[block]).wait_recv()

            @pl.when(z > 0)
            def _():
                raw_below(block, j, toks[j].at[block]).start()

        deal(block, j, lambda cols: toks[j][block, :, cols])

    def gather_b(block, behind):
        @pl.when(behind == 1)
        def _():
            b_above(block).wait_recv()

            @pl.when(z < nz - 1)
            def _():
                b_above(block).start()

        @pl.when(behind == 0)
        def _():
            b_below(block).wait_recv()

            @pl.when(z > 0)
            def _():
                b_below(block).start()

    unit = min(256, CORES * units)

    def serve(block):
        for j in range(CHUNKS):
            for d in range(1, n_sp):
                xa_from(block, j, d).wait_recv()

        def through(weight, cols):
            total = dot(rows_b[block].reshape(slots, kb), weight[ka:, cols])
            for j in range(CHUNKS):
                part = rows_a[j][block].reshape(slots, ins[j].size)
                total = total + dot(part, weight[ins[j].start : ins[j].start + ins[j].size, cols])
            return total

        def one(cols):
            gate_pre, upward = through(gate_v, cols), through(up_v, cols)
            capped = jnp.minimum(gate_pre, clamp_limit)
            linear = jnp.clip(upward, -clamp_limit, clamp_limit)
            gated = capped * jax.nn.sigmoid(sigmoid_alpha * capped)
            hid[:, cols] = (gated * (linear + 1.0)).astype(jnp.bfloat16)

        tiled(CORES * units, unit, one)

        def part_a(j, cols):
            part = dot(hid[...], down_v[:, shifted(cols, outs[j].start)]).astype(jnp.bfloat16)
            sums_a[j][block, :, :, cols] = part.reshape(n_sp, capp, cols.size)

        def part_b(cols):
            part = dot(hid[...], down_v[:, shifted(cols, na)]).astype(jnp.bfloat16)
            sums_b[block, :, :, cols] = part.reshape(n_sp, capp, cols.size)

        for j in range(CHUNKS):
            tiled(outs[j].size, wide, functools.partial(part_a, j))
        tiled(nb, wide, part_b)

    def ya_to(block, j, d):
        e = partner_of(sp, d, n_sp)
        at = j * nz + block
        return send(
            sums_a[j].at[block, e], back_a[j].at[block, sp], ya_s.at[at, d], ya_r.at[at, d], (e, tp)
        )

    def ya_from(block, j, d):
        e = source_of(sp, d, n_sp)
        at = j * nz + block
        return send(
            sums_a[j].at[block, e], back_a[j].at[block, e], ya_s.at[at, d], ya_r.at[at, d], (e, tp)
        )

    def yb_to(d):
        e = partner_of(sp, d, n_sp)
        return send(sums_b.at[z, e], back_b.at[sp], yb_s.at[d], yb_r.at[d], (e, tp))

    def yb_from(d):
        e = source_of(sp, d, n_sp)
        return send(sums_b.at[z, e], back_b.at[e], yb_s.at[d], yb_r.at[d], (e, tp))

    def a_above(block, j):
        at = j * nz + block
        return send(a_out[j].at[block], a_up[j].at[block], au_s.at[at], au_r.at[at], above)

    def a_below(block, j):
        at = j * nz + block
        return send(a_out[j].at[block], a_dn[j].at[block], ad_s.at[at], ad_r.at[at], below)

    def c_above(block):
        return send(sums_b.at[block], b_up.at[block], cu_s.at[block], cu_r.at[block], above)

    def c_below(block):
        return send(sums_b.at[block], b_dn.at[block], cd_s.at[block], cd_r.at[block], below)

    def push(block, j):
        for d in range(1, n_sp):
            ya_to(block, j, d).start()
        back_a[j][block, sp] = sums_a[j][block, sp]

    def add_b(block, arrived):
        total = sums_b[block].astype(jnp.float32) + arrived[block].astype(jnp.float32)
        sums_b[block] = total.astype(jnp.bfloat16)

    def relay_b(block, behind):
        @pl.when(behind == 0)
        def _():
            @pl.when(z > 0)
            def _():
                c_above(block).wait_recv()
                add_b(block, b_up)

            c_above(block).start()

        @pl.when(behind == 1)
        def _():
            @pl.when(z < nz - 1)
            def _():
                c_below(block).wait_recv()
                add_b(block, b_dn)

            c_below(block).start()

    def settle_b():
        @pl.when(z > 0)
        def _():
            c_above(z).wait_recv()
            add_b(z, b_up)

        @pl.when(z < nz - 1)
        def _():
            c_below(z).wait_recv()
            add_b(z, b_dn)

        for d in range(1, n_sp):
            yb_to(d).start()
        back_b[sp] = sums_b[z, sp]

    def combined(block, j, cols):
        return dot(share[block], back_a[j][block, :, :, cols].reshape(slots, cols.size))

    def relay_a(block, behind, j):
        for d in range(1, n_sp):
            ya_from(block, j, d).wait_recv()

        @pl.when(behind == 0)
        def _():
            @pl.when(z > 0)
            def _():
                a_above(block, j).wait_recv()

            def one(cols):
                total = combined(block, j, cols)
                total = jnp.where(z > 0, total + a_up[j][block, :, cols].astype(jnp.float32), total)
                a_out[j][block, :, cols] = total.astype(jnp.bfloat16)

            tiled(outs[j].size, wide, one)
            a_above(block, j).start()

        @pl.when(behind == 1)
        def _():
            @pl.when(z < nz - 1)
            def _():
                a_below(block, j).wait_recv()

            def one(cols):
                total = combined(block, j, cols)
                total = jnp.where(
                    z < nz - 1, total + a_dn[j][block, :, cols].astype(jnp.float32), total
                )
                a_out[j][block, :, cols] = total.astype(jnp.bfloat16)

            tiled(outs[j].size, wide, one)
            a_below(block, j).start()

    swap.wait()
    table, words = order_words(nz)

    def word_of(w):
        word = jnp.int32(0)
        for level in range(nz):
            for at in range(words):
                word = jnp.where((z == level) & (w == at), jnp.int32(table[level][at]), word)
        return word

    def task(i, word):
        kind = lax.rem(word, KINDS)
        block = lax.rem(word // KINDS, BLOCKS)
        behind = jnp.where(block < z, 1, 0)
        elsewhere = block != z

        @pl.when(kind <= LAST_IN)
        def _():
            for j in range(CHUNKS):
                @pl.when(kind == RAW[j])
                def _():
                    gather_raw(block, behind, j)

            @pl.when((kind == NEAR) & elsewhere)
            def _():
                gather_b(block, behind)

            @pl.when((kind == NEAR) & (block == z))
            def _():
                spread_own()

            @pl.when(kind == SERVE)
            def _():
                serve(block)

        @pl.when(kind > LAST_IN)
        def _():
            for j in range(CHUNKS):
                @pl.when(kind == PUSH[j])
                def _():
                    push(block, j)

                @pl.when(kind == RELAY[j])
                def _():
                    relay_a(block, behind, j)

            @pl.when((kind == CHAIN) & elsewhere)
            def _():
                relay_b(block, behind)

            @pl.when((kind == CHAIN) & (block == z))
            def _():
                settle_b()

        return word // (KINDS * BLOCKS)

    def tasks(w, carry):
        lax.fori_loop(0, PER_WORD, task, word_of(w))
        return carry

    lax.fori_loop(0, words, tasks, 0)

    for d in range(1, n_sp):
        yb_from(d).wait_recv()

    def final_b(cols):
        at = shifted(cols, na)
        total = dot(share[z], back_b[:, :, cols].reshape(slots, cols.size))
        out[:, at] = (stream[:, at].astype(jnp.float32) + total).astype(jnp.bfloat16)

    tiled(nb, wide, final_b)
    for j in range(CHUNKS):
        for d in range(1, n_sp):
            ya_from(z, j, d).wait_recv()

        @pl.when(z > 0)
        def _():
            a_above(z, j).wait_recv()

        @pl.when(z < nz - 1)
        def _():
            a_below(z, j).wait_recv()

        def final_a(cols):
            at = shifted(cols, outs[j].start)
            total = combined(z, j, cols)
            total = jnp.where(z > 0, total + a_up[j][z, :, cols].astype(jnp.float32), total)
            total = jnp.where(z < nz - 1, total + a_dn[j][z, :, cols].astype(jnp.float32), total)
            out[:, at] = (stream[:, at].astype(jnp.float32) + total).astype(jnp.bfloat16)

        tiled(outs[j].size, wide, final_a)

    for d in range(1, n_sp):
        xb_to(d).wait_send()
        yb_to(d).wait_send()

    def drain_exchange(block):
        for j in range(CHUNKS):
            for d in range(1, n_sp):
                xa_to(block, j, d).wait_send()
                ya_to(block, j, d).wait_send()

    drain_exchange(z)

    @pl.when(z < nz - 1)
    def _():
        b_above(z).wait_send()
        for j in range(CHUNKS):
            raw_above(z, j, own_raw(j)).wait_send()

    @pl.when(z > 0)
    def _():
        b_below(z).wait_send()
        for j in range(CHUNKS):
            raw_below(z, j, own_raw(j)).wait_send()

    def drain(block, behind):
        drain_exchange(block)

        @pl.when(behind == 0)
        def _():
            c_above(block).wait_send()
            for j in range(CHUNKS):
                a_above(block, j).wait_send()

        @pl.when(behind == 1)
        def _():
            c_below(block).wait_send()
            for j in range(CHUNKS):
                a_below(block, j).wait_send()

        @pl.when((behind == 1) & (z < nz - 1))
        def _():
            b_above(block).wait_send()
            for j in range(CHUNKS):
                raw_above(block, j, toks[j].at[block]).wait_send()

        @pl.when((behind == 0) & (z > 0))
        def _():
            b_below(block).wait_send()
            for j in range(CHUNKS):
                raw_below(block, j, toks[j].at[block]).wait_send()

    def drain_all(i, carry):
        both_sides(z, nz, i, drain)
        return carry

    lax.fori_loop(1, nz, drain_all, 0)


def held_bytes(scratch):
    total = 0
    for ref in scratch:
        if getattr(ref, "memory_space", None) == pltpu.VMEM:
            item = jnp.dtype(ref.dtype).itemsize
            lead = math.prod(ref.shape[:-2])
            rows = round_up(ref.shape[-2], 32 // item)
            total += lead * rows * round_up(ref.shape[-1], LANES) * item
    return total


def spans(widths):
    return [pl.ds(sum(widths[:j]), width) for j, width in enumerate(widths)]


def halves(width):
    first = round_up(width // 2, LANES)
    return (first, width - first)


def split_columns(width, share):
    return max(2 * LANES, min(width - LANES, int(width * share) // LANES * LANES))


class Swap:
    def __init__(self, place_at, weights, held, sems):
        sp, z, c = place_at
        peer_core = (sp, z * CORES + 1 - c)
        units = weights[0].shape[1]
        mine = pl.ds(pl.multiple_of(c * units, units), units)
        gate_v, up_v, down_v = held
        into = (gate_v.at[:, mine], up_v.at[:, mine], down_v.at[mine, :])
        w_l, w_s, w_r = sems
        self.copies = [
            pltpu.make_async_copy(src, dst, w_l.at[i]) for i, (src, dst) in enumerate(zip(weights, into))
        ] + [
            send(src, dst, w_s.at[i], w_r.at[i], peer_core)
            for i, (src, dst) in enumerate(zip(weights, into))
        ]

    def start(self):
        for copy in self.copies:
            copy.start()

    def wait(self):
        for copy in self.copies:
            copy.wait()


def tables(n_sp, nz, tok, capp, c, routes, rw_all, onehot, share):
    choose = routes.shape[0]
    epad = round_up(n_sp, 16)
    earlier = lax.broadcasted_iota(jnp.int32, (tok, tok), 0) < lax.broadcasted_iota(
        jnp.int32, (tok, tok), 1
    )
    earlier = jnp.where(earlier, 1.0, 0.0).astype(jnp.bfloat16)
    same = lax.broadcasted_iota(jnp.int32, (tok, tok), 0) == lax.broadcasted_iota(
        jnp.int32, (tok, tok), 1
    )
    same = jnp.where(same, 1.0, 0.0).astype(jnp.bfloat16)
    which = lax.broadcasted_iota(jnp.int32, (epad, tok), 0)
    place_in = lax.broadcasted_iota(jnp.int32, (capp, tok), 0).astype(jnp.float32)
    for b in range(nz):
        first = routes[:, (CORES * b) * tok : (CORES * b + 1) * tok]
        second = routes[:, (CORES * b + 1) * tok : (CORES * b + 2) * tok]
        ids = jnp.where(c == 0, first, second)
        weight = jnp.zeros((epad, tok), jnp.float32)
        member = jnp.zeros((epad, tok), jnp.float32)
        for m in range(choose):
            named = ids[m : m + 1, :] == which
            member = jnp.where(named, 1.0, member)
            weight = jnp.where(named, rw_all[b, m : m + 1, :tok], weight)
        rank = dot(member.astype(jnp.bfloat16), earlier)
        rank = jnp.where(member > 0.0, rank, -1.0)
        shares = []
        for e in range(n_sp):
            hit = place_in == rank[e : e + 1, :]
            onehot[b, e * capp : (e + 1) * capp, :] = jnp.where(hit, 1.0, 0.0).astype(jnp.bfloat16)
            shares.append(jnp.where(hit, weight[e : e + 1, :], 0.0).astype(jnp.bfloat16))
        turned = lax.dot_general(
            same,
            jnp.concatenate(shares, axis=0),
            (((1,), (1,)), ((), ())),
            preferred_element_type=jnp.float32,
        )
        share[b] = turned.astype(jnp.bfloat16)


def layer_kernel(
    n_sp, n_tp, tok, capp, q, k, v, sink_in, residual, weight, gain_in, routes_in, rweight,
    gate, up, down, out, normed, stream, onehot, share, gate_v, up_v, down_v,
    q_all, k_all, v_all, k_tail, v_tail, att, got, w_all, res, acc, rw_src, rw_all,
    sink, gain, routes, rw_in,
    in_s, o_s, t_s, t_r, a_s, a_r, g_s, g_r, w_l, w_s, w_r, *rest,
):
    sp, z, c = place()
    tp = z * CORES + c
    nz = n_tp // CORES
    span, kv_cols = k.shape
    cols = q.shape[1]
    width = weight.shape[1]
    kv_local = kv_cols // HEAD
    group = cols // kv_cols
    blocks = span // WINDOW
    pieces = WINDOW // tok
    scale = HEAD ** (-0.5)
    body = pl.ds(WINDOW, span)
    copies = [
        pltpu.make_async_copy(k, k_all.at[body], in_s.at[0]),
        pltpu.make_async_copy(v, v_all.at[body], in_s.at[1]),
        pltpu.make_async_copy(q, q_all, in_s.at[2]),
        pltpu.make_async_copy(rweight, rw_in, in_s.at[3]),
        pltpu.make_async_copy(sink_in, sink, in_s.at[4]),
        pltpu.make_async_copy(routes_in, routes, in_s.at[5]),
        pltpu.make_async_copy(residual, res, in_s.at[6]),
        pltpu.make_async_copy(gain_in, gain, in_s.at[7]),
    ]
    for copy in copies:
        copy.start()

    def out_rows(p):
        rows = pl.ds(pl.multiple_of(p * cols, cols), cols)
        return pltpu.make_async_copy(weight.at[rows], w_all.at[rows], o_s.at[p])

    barrier = pltpu.get_barrier_semaphore()
    for d in range(1, n_tp):
        pl.semaphore_signal(
            barrier, inc=1, device_id=(sp, lax.rem(tp + d, n_tp)), device_id_type=MESH
        )

    for d in range(1, n_sp):
        pl.semaphore_signal(
            barrier, inc=1, device_id=(lax.rem(sp + d, n_sp), tp), device_id_type=MESH
        )
    swap = Swap((sp, z, c), (gate, up, down), (gate_v, up_v, down_v), (w_l, w_s, w_r))
    rw_src[...] = jnp.zeros_like(rw_src)
    copies[3].wait()
    rw_src[: rweight.shape[0], :tok] = rw_in[...]
    rw_all[z] = rw_src[...]
    pl.semaphore_wait(barrier, n_tp - 1 + n_sp - 1)
    ahead = (lax.rem(sp + 1, n_sp), tp)
    last = pl.ds(span, WINDOW)
    tails = (
        send(k_all.at[last], k_tail, t_s.at[0], t_r.at[0], ahead),
        send(v_all.at[last], v_tail, t_s.at[1], t_r.at[1], ahead),
    )
    copies[0].wait()
    copies[1].wait()

    @pl.when(sp < n_sp - 1)
    def _():
        for copy in tails:
            copy.start()

    def tell(d):
        there = lax.rem(z + d, nz)
        return send(rw_src, rw_all.at[z], g_s.at[d], g_r.at[z], (sp, there * CORES + c))

    def told(d):
        there = lax.rem(z + d, nz)
        return send(rw_src, rw_all.at[there], g_s.at[d], g_r.at[there], (sp, there * CORES + c))

    for d in range(1, nz):
        tell(d).start()
    copies[2].wait()
    copies[4].wait()
    for p in range(n_tp):
        out_rows(p).start()

    row = lax.broadcasted_iota(jnp.int32, (WINDOW, 2 * WINDOW), 0)
    col = lax.broadcasted_iota(jnp.int32, (WINDOW, 2 * WINDOW), 1)
    distance = row + WINDOW - col
    banded = (distance >= 0) & (distance < WINDOW)
    low = z < nz // 2
    half = max(1, blocks // 2)

    own_cols = pl.ds(pl.multiple_of(tp * cols, cols), cols)

    def to_owner(dest):
        at = pl.multiple_of(dest * tok, tok)
        return send(
            att.at[pl.ds(at, tok)], got.at[:, own_cols], a_s.at[dest], a_r.at[tp], (sp, dest)
        )

    def attend(i, carry):
        turned = jnp.where(i < half, lax.rem(i + 1, half), i)
        block = jnp.where(low, blocks - 1 - i, turned)

        @pl.when(block == 0)
        def _():
            @pl.when(sp > 0)
            def _():
                for copy in tails:
                    copy.wait_recv()
                k_all[pl.ds(0, WINDOW), :] = k_tail[...]
                v_all[pl.ds(0, WINDOW), :] = v_tail[...]

            @pl.when(sp == 0)
            def _():
                k_all[pl.ds(0, WINDOW), :] = jnp.zeros((WINDOW, kv_cols), jnp.bfloat16)
                v_all[pl.ds(0, WINDOW), :] = jnp.zeros((WINDOW, kv_cols), jnp.bfloat16)

        at = pl.multiple_of(block * WINDOW, WINDOW)
        start = jnp.where((sp == 0) & (block == 0), WINDOW, 0)
        allowed = banded & (col >= start)
        band = pl.ds(at, 2 * WINDOW)
        for g in range(kv_local):
            keys = k_all[band, g * HEAD : (g + 1) * HEAD]
            values = v_all[band, g * HEAD : (g + 1) * HEAD]
            heads = []
            for m in range(group):
                h = g * group + m
                query = q_all[pl.ds(at, WINDOW), h * HEAD : (h + 1) * HEAD] * jnp.bfloat16(scale)
                scores = lax.dot_general(
                    query, keys, (((1,), (1,)), ((), ())), preferred_element_type=jnp.float32
                )
                logits = jnp.where(allowed, scores, -jnp.inf)
                top = jnp.maximum(jnp.max(logits, axis=-1, keepdims=True), sink[h])
                raised = jnp.exp(logits - top)
                total = jnp.sum(raised, axis=-1, keepdims=True) + jnp.exp(sink[h] - top)
                probs = (raised * (1.0 / total)).astype(jnp.bfloat16)
                heads.append(dot(probs, values))
            att[pl.ds(at, WINDOW), g * group * HEAD : (g + 1) * group * HEAD] = jnp.concatenate(
                heads, axis=1
            ).astype(jnp.bfloat16)
        for piece in range(pieces):
            dest = block * pieces + piece

            @pl.when(dest != tp)
            def _():
                to_owner(dest).start()

        return carry

    lax.fori_loop(0, blocks, attend, 0)
    for d in range(1, nz):
        told(d).wait_recv()
    copies[5].wait()
    tables(n_sp, nz, tok, capp, c, routes, rw_all, onehot, share)
    swap.start()
    got[:, own_cols] = att[pl.ds(pl.multiple_of(tp * tok, tok), tok), :]
    copies[6].wait()
    copies[7].wait()
    wide = math.gcd(width, 512)

    def begin(at):
        acc[:, at] = res[:, at].astype(jnp.float32)

    tiled(width, wide, begin)
    for p in range(n_tp):
        out_rows(p).wait()

    part = n_tp // 2

    def arrived(i, carry):
        p = jnp.where(low, n_tp - 1 - i, i)

        @pl.when(tp != p)
        def _():
            into = got.at[:, pl.ds(pl.multiple_of(p * cols, cols), cols)]
            send(att.at[pl.ds(0, tok)], into, a_s.at[p], a_r.at[p], (sp, p)).wait_recv()

        return carry

    for far in range(2):
        lax.fori_loop(far * part, (far + 1) * part, arrived, 0)
        first = jnp.where(low, (1 - far) * part, far * part) * cols
        rows = pl.ds(pl.multiple_of(first, part * cols), part * cols)

        def one(at):
            acc[:, at] = acc[:, at] + dot(got[:, rows], w_all[rows, at])

        tiled(width, wide, one)

    squares = jnp.zeros((tok, 1), jnp.float32)
    for t in range(width // wide):
        at = slice(t * wide, (t + 1) * wide)
        held = acc[:, at].astype(jnp.bfloat16)
        stream[:, at] = held
        held32 = held.astype(jnp.float32)
        squares = squares + jnp.sum(held32 * held32, axis=-1, keepdims=True)
    root = lax.rsqrt(squares * (1.0 / width) + eps)
    for t in range(width // wide):
        at = slice(t * wide, (t + 1) * wide)
        normed[:, at] = (stream[:, at].astype(jnp.float32) * root * gain[:, at]).astype(
            jnp.bfloat16
        )
    expert_kernel(
        n_sp, nz, swap, normed, stream, onehot, share, out, gate_v, up_v, down_v, *rest
    )
    for p in range(n_tp):
        @pl.when(tp != p)
        def _():
            to_owner(p).wait_send()

    for d in range(1, nz):
        tell(d).wait_send()

    @pl.when(sp < n_sp - 1)
    def _():
        for copy in tails:
            copy.wait_send()


def local(
    query_heads,
    key_heads,
    value_heads,
    sink_logit,
    residual,
    out_weight,
    norm_gain,
    routes,
    route_weight,
    gate_weight,
    up_weight,
    down_weight,
):
    n_sp, n_tp = lax.axis_size("sp"), lax.axis_size("tp")
    nz = n_tp // CORES
    span, cols = query_heads.shape
    kv_cols = key_heads.shape[1]
    tok, width = residual.shape
    choose = routes.shape[1]
    capp = round_up(max(2, 5 * tok * choose // (4 * n_sp)), 16)
    slots = n_sp * capp
    hidden = CORES * gate_weight.shape[2]
    ka = split_columns(width, DISPATCH_SHARE)
    na = split_columns(width, RETURN_SHARE)
    kb, nb = width - ka, width - na
    vmem = pl.BlockSpec(memory_space=pltpu.VMEM)
    inputs = (
        query_heads, key_heads, value_heads, sink_logit, residual, out_weight,
        norm_gain.reshape(1, -1), routes.T, route_weight.T,
        gate_weight[0], up_weight[0], down_weight[0],
    )
    dma = pltpu.SemaphoreType.DMA
    bf = jnp.bfloat16
    line = [dma((nz,))] * 4
    scratch = (
        [
            pltpu.VMEM((tok, width), bf),
            pltpu.VMEM((tok, width), bf),
            pltpu.VMEM((nz, slots, tok), bf),
            pltpu.VMEM((nz, tok, slots), bf),
            pltpu.VMEM((width, hidden), bf),
            pltpu.VMEM((width, hidden), bf),
            pltpu.VMEM((hidden, width), bf),
            pltpu.VMEM((span, cols), bf),
            pltpu.VMEM((span + WINDOW, kv_cols), bf),
            pltpu.VMEM((span + WINDOW, kv_cols), bf),
            pltpu.VMEM((WINDOW, kv_cols), bf),
            pltpu.VMEM((WINDOW, kv_cols), bf),
            pltpu.VMEM((span, cols), bf),
            pltpu.VMEM((tok, n_tp * cols), bf),
            pltpu.VMEM((n_tp * cols, width), bf),
            pltpu.VMEM((tok, width), bf),
            pltpu.VMEM((tok, width), jnp.float32),
            pltpu.VMEM((8, LANES), jnp.float32),
            pltpu.VMEM((nz, 8, LANES), jnp.float32),
            pltpu.SMEM(sink_logit.shape, jnp.float32),
            pltpu.VMEM((1, width), jnp.float32),
            pltpu.VMEM(routes.shape[::-1], routes.dtype),
            pltpu.VMEM(route_weight.shape[::-1], jnp.float32),
            dma((8,)),
            dma((n_tp,)),
            dma((2,)),
            dma((2,)),
            dma((n_tp,)),
            dma((n_tp,)),
            dma((nz,)),
            dma((nz,)),
        ]
        + [dma((3,))] * 3
        + [pltpu.VMEM((nz, tok, w), bf) for w in halves(ka)]
        + [pltpu.VMEM((nz, n_sp, capp, w), bf) for w in halves(ka)]
        + [pltpu.VMEM((n_sp, capp, kb), bf)]
        + [pltpu.VMEM((nz, n_sp, capp, w), bf) for w in (*halves(ka), kb)]
        + [pltpu.VMEM((slots, hidden), bf)]
        + [pltpu.VMEM((nz, n_sp, capp, w), bf) for w in (*halves(na), nb, *halves(na))]
        + [pltpu.VMEM((n_sp, capp, nb), bf)]
        + [pltpu.VMEM((nz, tok, w), bf) for w in halves(na) * 3]
        + [pltpu.VMEM((nz, n_sp, capp, nb), bf)] * 2
        + [dma((CHUNKS * nz,))] * 4
        + [dma((CHUNKS * nz, n_sp))] * 2
        + [dma((n_sp,))] * 2
        + line
        + [dma((CHUNKS * nz, n_sp))] * 2
        + [dma((n_sp,))] * 2
        + [dma((CHUNKS * nz,))] * 4
        + line
    )
    return pl.pallas_call(
        functools.partial(layer_kernel, n_sp, n_tp, tok, capp),
        out_shape=jax.ShapeDtypeStruct((tok, width), bf),
        in_specs=[pl.BlockSpec(memory_space=pltpu.HBM)] * len(inputs),
        out_specs=vmem,
        scratch_shapes=scratch,
        compiler_params=pltpu.CompilerParams(
            collective_id=0, has_side_effects=True, vmem_limit_bytes=held_bytes(scratch) + SPARE
        ),
        name="layer",
    )(*[pltpu.with_memory_space_constraint(x, pltpu.HBM) for x in inputs])


def solution(mesh):
    placed = (
        P("sp", "tp"),
        P("sp", "tp"),
        P("sp", "tp"),
        P("tp"),
        P(("sp", "tp"), None),
        P(),
        P(),
        P("sp", None),
        P(("sp", "tp"), None),
        P("sp", None, "tp"),
        P("sp", None, "tp"),
        P("sp", "tp", None),
    )
    return jax.shard_map(
        local, mesh=mesh, in_specs=placed, out_specs=P(("sp", "tp"), None), check_vma=False
    )
```

```python
import functools
import math

import jax
import jax.numpy as jnp
from jax import lax
from jax.experimental import pallas as pl
from jax.experimental.pallas import tpu as pltpu
from jax.sharding import PartitionSpec as P

HEAD = 64
WINDOW = 128


eps = 1e-06
clamp_limit = 7.0
sigmoid_alpha = 1.702


MESH = pl.DeviceIdType.MESH
CORES = 2
LANES = 128
SPARE = 2 * 1024 * 1024


def round_up(value, unit):
    return (value + unit - 1) // unit * unit


def place():
    tp = lax.axis_index("tp")
    return lax.axis_index("sp"), tp // CORES, lax.rem(tp, CORES)


def partner_of(sp, d, n_sp):
    if n_sp & (n_sp - 1):
        return lax.rem(sp + d, n_sp)
    total, bit = 0, 1
    while bit < n_sp:
        total = total + lax.rem(sp // bit + d // bit, 2) * bit
        bit *= 2
    return total


def source_of(sp, d, n_sp):
    if n_sp & (n_sp - 1):
        return lax.rem(sp + n_sp - d, n_sp)
    return partner_of(sp, d, n_sp)


def send(src, dst, send_sem, recv_sem, device):
    return pltpu.make_async_remote_copy(
        src_ref=src,
        dst_ref=dst,
        send_sem=send_sem,
        recv_sem=recv_sem,
        device_id=device,
        device_id_type=MESH,
    )


def dot(a, b):
    return jnp.dot(a, b, preferred_element_type=jnp.float32)


def tiled(extent, tile, visit):
    for start in range(0, extent, tile):
        visit(pl.ds(start, min(tile, extent - start)))


def shifted(cols, offset):
    return pl.ds(cols.start + offset, cols.size)


CHUNKS = 2
NEAR, SERVE = 1, 2
RAW = (3, 4)
CHAIN = 5
PUSH = (6, 7)
RELAY = (8, 9)
LAST_IN = 4
KINDS = 16
BLOCKS = 64
PER_WORD = 3


def sides(nz, z, away):
    return [b for b in ((z + away, z - away) if away else (z,)) if 0 <= b < nz]


def plain_order(nz, z):
    order = []
    for i in range(1, nz):
        order += [(RAW[j], b) for b in sides(nz, z, i) for j in range(CHUNKS)]
        order += [(NEAR, b) for b in sides(nz, z, i - 1)]
        if i > 1:
            order += [(SERVE, b) for b in sides(nz, z, i - 2)]
    order += [(SERVE, b) for b in sides(nz, z, nz - 2)]
    order += [(NEAR, b) for b in sides(nz, z, nz - 1)]
    order += [(SERVE, b) for b in sides(nz, z, nz - 1)]
    for away in range(nz - 1, -1, -1):
        order += [(PUSH[j], b) for b in sides(nz, z, away) for j in range(CHUNKS)]
    order += [(CHAIN, b) for b in sides(nz, z, nz - 1)]
    for away in range(nz - 1, 0, -1):
        order += [(CHAIN, b) for b in sides(nz, z, away - 1)]
        order += [(RELAY[j], b) for b in sides(nz, z, away) for j in range(CHUNKS)]
    return order


ORDERS = {
    4: [
        [
            (RAW[0], 1), (NEAR, 0), (RAW[1], 1), (RAW[1], 2), (RAW[0], 3),
            (RAW[1], 3), (RAW[0], 2), (NEAR, 1), (SERVE, 1), (CHAIN, 1),
            (NEAR, 3), (PUSH[0], 1), (SERVE, 3), (CHAIN, 3), (PUSH[1], 3),
            (NEAR, 2), (SERVE, 2), (CHAIN, 2), (PUSH[0], 3), (PUSH[0], 2),
            (RELAY[1], 3), (SERVE, 0), (PUSH[1], 2), (PUSH[1], 1), (RELAY[0], 2),
            (RELAY[0], 3), (RELAY[1], 2), (PUSH[0], 0), (CHAIN, 0), (RELAY[0], 1),
            (RELAY[1], 1), (PUSH[1], 0),
        ],
        [
            (RAW[0], 2), (RAW[0], 0), (RAW[1], 0), (RAW[1], 2), (RAW[0], 3),
            (NEAR, 0), (RAW[1], 3), (NEAR, 1), (NEAR, 3), (SERVE, 0),
            (NEAR, 2), (SERVE, 1), (PUSH[0], 1), (SERVE, 3), (PUSH[0], 3),
            (SERVE, 2), (PUSH[1], 0), (PUSH[0], 2), (CHAIN, 3), (PUSH[1], 3),
            (CHAIN, 2), (PUSH[1], 2), (CHAIN, 0), (PUSH[0], 0), (PUSH[1], 1),
            (RELAY[1], 3), (RELAY[0], 3), (RELAY[1], 0), (RELAY[0], 2), (CHAIN, 1),
            (RELAY[1], 2), (RELAY[0], 0),
        ],
    ],
}
DISPATCH_SHARE = 0.6875
RETURN_SHARE = 0.6875


def order_of(nz, z):
    if nz not in ORDERS:
        return plain_order(nz, z)
    if z < nz // 2:
        return ORDERS[nz][z]
    return [(kind, nz - 1 - b) for kind, b in ORDERS[nz][nz - 1 - z]]


def order_words(nz):
    orders = [order_of(nz, z) for z in range(nz)]
    words = round_up(max(len(order) for order in orders), PER_WORD) // PER_WORD
    table = []
    for order in orders:
        codes = [b * KINDS + kind for kind, b in order]
        codes += [0] * (words * PER_WORD - len(codes))
        base = KINDS * BLOCKS
        table.append([
            sum(code * base**i for i, code in enumerate(codes[w * PER_WORD : (w + 1) * PER_WORD]))
            for w in range(words)
        ])
    return table, words


def both_sides(z, nz, away, visit):
    def one(behind, carry):
        block = z + away * (1 - 2 * behind)

        @pl.when((block >= 0) & (block < nz))
        def _():
            visit(block, behind)

        return carry

    lax.fori_loop(0, 2, one, 0)


def expert_kernel(
    n_sp, nz, swap, normed, stream, onehot, share, out,
    gate_v, up_v, down_v, toks_0, toks_1, comp_a0, comp_a1, comp_b, rows_a0, rows_a1, rows_b, hid,
    sums_a0, sums_a1, sums_b, back_a0, back_a1, back_b, a_out0, a_out1, a_up0, a_up1, a_dn0, a_dn1,
    b_up, b_dn, ru_s, ru_r, rd_s, rd_r, xa_s, xa_r, xb_s, xb_r,
    bu_s, bu_r, bd_s, bd_r, ya_s, ya_r, yb_s, yb_r,
    au_s, au_r, ad_s, ad_r, cu_s, cu_r, cd_s, cd_r,
):
    sp, z, c = place()
    tp = z * CORES + c
    toks, comp_a, rows_a = (toks_0, toks_1), (comp_a0, comp_a1), (rows_a0, rows_a1)
    sums_a, back_a = (sums_a0, sums_a1), (back_a0, back_a1)
    a_out, a_up, a_dn = (a_out0, a_out1), (a_up0, a_up1), (a_dn0, a_dn1)
    above = (sp, lax.rem(z + 1, nz) * CORES + c)
    below = (sp, lax.rem(z + nz - 1, nz) * CORES + c)
    capp, kb, nb = rows_b.shape[2], rows_b.shape[3], sums_b.shape[3]
    ins = spans([ref.shape[-1] for ref in rows_a])
    outs = spans([ref.shape[-1] for ref in sums_a])
    ka, na = normed.shape[1] - kb, normed.shape[1] - nb
    slots = n_sp * capp
    units = gate_v.shape[1] // CORES
    tile, wide = 512, 512

    def raw_above(block, j, src):
        at = j * nz + block
        return send(src, toks[j].at[block], ru_s.at[at], ru_r.at[at], above)

    def raw_below(block, j, src):
        at = j * nz + block
        return send(src, toks[j].at[block], rd_s.at[at], rd_r.at[at], below)

    def own_raw(j):
        return normed.at[:, pl.ds(ins[j].start, ins[j].size)]

    for j in range(CHUNKS):
        @pl.when(z < nz - 1)
        def _():
            raw_above(z, j, own_raw(j)).start()

        @pl.when(z > 0)
        def _():
            raw_below(z, j, own_raw(j)).start()

    def xa_to(block, j, d):
        e = partner_of(sp, d, n_sp)
        at = j * nz + block
        return send(
            comp_a[j].at[block, e], rows_a[j].at[block, sp], xa_s.at[at, d], xa_r.at[at, d], (e, tp)
        )

    def xa_from(block, j, d):
        e = source_of(sp, d, n_sp)
        at = j * nz + block
        return send(
            comp_a[j].at[block, e], rows_a[j].at[block, e], xa_s.at[at, d], xa_r.at[at, d], (e, tp)
        )

    def xb_to(d):
        e = partner_of(sp, d, n_sp)
        return send(comp_b.at[e], rows_b.at[z, sp], xb_s.at[d], xb_r.at[d], (e, tp))

    def xb_from(d):
        e = source_of(sp, d, n_sp)
        return send(comp_b.at[e], rows_b.at[z, e], xb_s.at[d], xb_r.at[d], (e, tp))

    def b_above(block):
        return send(rows_b.at[block], rows_b.at[block], bu_s.at[block], bu_r.at[block], above)

    def b_below(block):
        return send(rows_b.at[block], rows_b.at[block], bd_s.at[block], bd_r.at[block], below)

    def deal_b(cols):
        picked = dot(onehot[z], normed[:, shifted(cols, ka)])
        comp_b[:, :, cols] = picked.astype(jnp.bfloat16).reshape(n_sp, capp, cols.size)

    tiled(kb, tile, deal_b)
    for d in range(1, n_sp):
        xb_to(d).start()
    rows_b[z, sp] = comp_b[sp]

    def deal(block, j, src):
        def one(cols):
            picked = dot(onehot[block], src(cols))
            comp_a[j][block, :, :, cols] = picked.astype(jnp.bfloat16).reshape(
                n_sp, capp, cols.size
            )

        tiled(ins[j].size, tile, one)
        for d in range(1, n_sp):
            xa_to(block, j, d).start()
        rows_a[j][block, sp] = comp_a[j][block, sp]

    for j in range(CHUNKS):
        deal(z, j, lambda cols: normed[:, shifted(cols, ins[j].start)])

    def spread_own():
        for d in range(1, n_sp):
            xb_from(d).wait_recv()

        @pl.when(z < nz - 1)
        def _():
            b_above(z).start()

        @pl.when(z > 0)
        def _():
            b_below(z).start()

    def gather_raw(block, behind, j):
        @pl.when(behind == 1)
        def _():
            raw_above(block, j, toks[j].at[block]).wait_recv()

            @pl.when(z < nz - 1)
            def _():
                raw_above(block, j, toks[j].at[block]).start()

        @pl.when(behind == 0)
        def _():
            raw_below(block, j, toks[j].at[block]).wait_recv()

            @pl.when(z > 0)
            def _():
                raw_below(block, j, toks[j].at[block]).start()

        deal(block, j, lambda cols: toks[j][block, :, cols])

    def gather_b(block, behind):
        @pl.when(behind == 1)
        def _():
            b_above(block).wait_recv()

            @pl.when(z < nz - 1)
            def _():
                b_above(block).start()

        @pl.when(behind == 0)
        def _():
            b_below(block).wait_recv()

            @pl.when(z > 0)
            def _():
                b_below(block).start()

    unit = min(256, CORES * units)

    def serve(block):
        for j in range(CHUNKS):
            for d in range(1, n_sp):
                xa_from(block, j, d).wait_recv()

        def through(weight, cols):
            total = dot(rows_b[block].reshape(slots, kb), weight[ka:, cols])
            for j in range(CHUNKS):
                part = rows_a[j][block].reshape(slots, ins[j].size)
                total = total + dot(part, weight[ins[j].start : ins[j].start + ins[j].size, cols])
            return total

        def one(cols):
            gate_pre, upward = through(gate_v, cols), through(up_v, cols)
            capped = jnp.minimum(gate_pre, clamp_limit)
            linear = jnp.clip(upward, -clamp_limit, clamp_limit)
            gated = capped * jax.nn.sigmoid(sigmoid_alpha * capped)
            hid[:, cols] = (gated * (linear + 1.0)).astype(jnp.bfloat16)

        tiled(CORES * units, unit, one)

        def part_a(j, cols):
            part = dot(hid[...], down_v[:, shifted(cols, outs[j].start)]).astype(jnp.bfloat16)
            sums_a[j][block, :, :, cols] = part.reshape(n_sp, capp, cols.size)

        def part_b(cols):
            part = dot(hid[...], down_v[:, shifted(cols, na)]).astype(jnp.bfloat16)
            sums_b[block, :, :, cols] = part.reshape(n_sp, capp, cols.size)

        for j in range(CHUNKS):
            tiled(outs[j].size, wide, functools.partial(part_a, j))
        tiled(nb, wide, part_b)

    def ya_to(block, j, d):
        e = partner_of(sp, d, n_sp)
        at = j * nz + block
        return send(
            sums_a[j].at[block, e], back_a[j].at[block, sp], ya_s.at[at, d], ya_r.at[at, d], (e, tp)
        )

    def ya_from(block, j, d):
        e = source_of(sp, d, n_sp)
        at = j * nz + block
        return send(
            sums_a[j].at[block, e], back_a[j].at[block, e], ya_s.at[at, d], ya_r.at[at, d], (e, tp)
        )

    def yb_to(d):
        e = partner_of(sp, d, n_sp)
        return send(sums_b.at[z, e], back_b.at[sp], yb_s.at[d], yb_r.at[d], (e, tp))

    def yb_from(d):
        e = source_of(sp, d, n_sp)
        return send(sums_b.at[z, e], back_b.at[e], yb_s.at[d], yb_r.at[d], (e, tp))

    def a_above(block, j):
        at = j * nz + block
        return send(a_out[j].at[block], a_up[j].at[block], au_s.at[at], au_r.at[at], above)

    def a_below(block, j):
        at = j * nz + block
        return send(a_out[j].at[block], a_dn[j].at[block], ad_s.at[at], ad_r.at[at], below)

    def c_above(block):
        return send(sums_b.at[block], b_up.at[block], cu_s.at[block], cu_r.at[block], above)

    def c_below(block):
        return send(sums_b.at[block], b_dn.at[block], cd_s.at[block], cd_r.at[block], below)

    def push(block, j):
        for d in range(1, n_sp):
            ya_to(block, j, d).start()
        back_a[j][block, sp] = sums_a[j][block, sp]

    def add_b(block, arrived):
        total = sums_b[block].astype(jnp.float32) + arrived[block].astype(jnp.float32)
        sums_b[block] = total.astype(jnp.bfloat16)

    def relay_b(block, behind):
        @pl.when(behind == 0)
        def _():
            @pl.when(z > 0)
            def _():
                c_above(block).wait_recv()
                add_b(block, b_up)

            c_above(block).start()

        @pl.when(behind == 1)
        def _():
            @pl.when(z < nz - 1)
            def _():
                c_below(block).wait_recv()
                add_b(block, b_dn)

            c_below(block).start()

    def settle_b():
        @pl.when(z > 0)
        def _():
            c_above(z).wait_recv()
            add_b(z, b_up)

        @pl.when(z < nz - 1)
        def _():
            c_below(z).wait_recv()
            add_b(z, b_dn)

        for d in range(1, n_sp):
            yb_to(d).start()
        back_b[sp] = sums_b[z, sp]

    def combined(block, j, cols):
        return dot(share[block], back_a[j][block, :, :, cols].reshape(slots, cols.size))

    def relay_a(block, behind, j):
        for d in range(1, n_sp):
            ya_from(block, j, d).wait_recv()

        @pl.when(behind == 0)
        def _():
            @pl.when(z > 0)
            def _():
                a_above(block, j).wait_recv()

            def one(cols):
                total = combined(block, j, cols)
                total = jnp.where(z > 0, total + a_up[j][block, :, cols].astype(jnp.float32), total)
                a_out[j][block, :, cols] = total.astype(jnp.bfloat16)

            tiled(outs[j].size, wide, one)
            a_above(block, j).start()

        @pl.when(behind == 1)
        def _():
            @pl.when(z < nz - 1)
            def _():
                a_below(block, j).wait_recv()

            def one(cols):
                total = combined(block, j, cols)
                total = jnp.where(
                    z < nz - 1, total + a_dn[j][block, :, cols].astype(jnp.float32), total
                )
                a_out[j][block, :, cols] = total.astype(jnp.bfloat16)

            tiled(outs[j].size, wide, one)
            a_below(block, j).start()

    swap.wait()
    table, words = order_words(nz)

    def word_of(w):
        word = jnp.int32(0)
        for level in range(nz):
            for at in range(words):
                word = jnp.where((z == level) & (w == at), jnp.int32(table[level][at]), word)
        return word

    def task(i, word):
        kind = lax.rem(word, KINDS)
        block = lax.rem(word // KINDS, BLOCKS)
        behind = jnp.where(block < z, 1, 0)
        elsewhere = block != z

        @pl.when(kind <= LAST_IN)
        def _():
            for j in range(CHUNKS):
                @pl.when(kind == RAW[j])
                def _():
                    gather_raw(block, behind, j)

            @pl.when((kind == NEAR) & elsewhere)
            def _():
                gather_b(block, behind)

            @pl.when((kind == NEAR) & (block == z))
            def _():
                spread_own()

            @pl.when(kind == SERVE)
            def _():
                serve(block)

        @pl.when(kind > LAST_IN)
        def _():
            for j in range(CHUNKS):
                @pl.when(kind == PUSH[j])
                def _():
                    push(block, j)

                @pl.when(kind == RELAY[j])
                def _():
                    relay_a(block, behind, j)

            @pl.when((kind == CHAIN) & elsewhere)
            def _():
                relay_b(block, behind)

            @pl.when((kind == CHAIN) & (block == z))
            def _():
                settle_b()

        return word // (KINDS * BLOCKS)

    def tasks(w, carry):
        lax.fori_loop(0, PER_WORD, task, word_of(w))
        return carry

    lax.fori_loop(0, words, tasks, 0)

    for d in range(1, n_sp):
        yb_from(d).wait_recv()

    def final_b(cols):
        at = shifted(cols, na)
        total = dot(share[z], back_b[:, :, cols].reshape(slots, cols.size))
        out[:, at] = (stream[:, at].astype(jnp.float32) + total).astype(jnp.bfloat16)

    tiled(nb, wide, final_b)
    for j in range(CHUNKS):
        for d in range(1, n_sp):
            ya_from(z, j, d).wait_recv()

        @pl.when(z > 0)
        def _():
            a_above(z, j).wait_recv()

        @pl.when(z < nz - 1)
        def _():
            a_below(z, j).wait_recv()

        def final_a(cols):
            at = shifted(cols, outs[j].start)
            total = combined(z, j, cols)
            total = jnp.where(z > 0, total + a_up[j][z, :, cols].astype(jnp.float32), total)
            total = jnp.where(z < nz - 1, total + a_dn[j][z, :, cols].astype(jnp.float32), total)
            out[:, at] = (stream[:, at].astype(jnp.float32) + total).astype(jnp.bfloat16)

        tiled(outs[j].size, wide, final_a)

    for d in range(1, n_sp):
        xb_to(d).wait_send()
        yb_to(d).wait_send()

    def drain_exchange(block):
        for j in range(CHUNKS):
            for d in range(1, n_sp):
                xa_to(block, j, d).wait_send()
                ya_to(block, j, d).wait_send()

    drain_exchange(z)

    @pl.when(z < nz - 1)
    def _():
        b_above(z).wait_send()
        for j in range(CHUNKS):
            raw_above(z, j, own_raw(j)).wait_send()

    @pl.when(z > 0)
    def _():
        b_below(z).wait_send()
        for j in range(CHUNKS):
            raw_below(z, j, own_raw(j)).wait_send()

    def drain(block, behind):
        drain_exchange(block)

        @pl.when(behind == 0)
        def _():
            c_above(block).wait_send()
            for j in range(CHUNKS):
                a_above(block, j).wait_send()

        @pl.when(behind == 1)
        def _():
            c_below(block).wait_send()
            for j in range(CHUNKS):
                a_below(block, j).wait_send()

        @pl.when((behind == 1) & (z < nz - 1))
        def _():
            b_above(block).wait_send()
            for j in range(CHUNKS):
                raw_above(block, j, toks[j].at[block]).wait_send()

        @pl.when((behind == 0) & (z > 0))
        def _():
            b_below(block).wait_send()
            for j in range(CHUNKS):
                raw_below(block, j, toks[j].at[block]).wait_send()

    def drain_all(i, carry):
        both_sides(z, nz, i, drain)
        return carry

    lax.fori_loop(1, nz, drain_all, 0)


def held_bytes(scratch):
    total = 0
    for ref in scratch:
        if getattr(ref, "memory_space", None) == pltpu.VMEM:
            item = jnp.dtype(ref.dtype).itemsize
            lead = math.prod(ref.shape[:-2])
            rows = round_up(ref.shape[-2], 32 // item)
            total += lead * rows * round_up(ref.shape[-1], LANES) * item
    return total


def spans(widths):
    return [pl.ds(sum(widths[:j]), width) for j, width in enumerate(widths)]


def halves(width):
    first = round_up(width // 2, LANES)
    return (first, width - first)


def split_columns(width, share):
    return max(2 * LANES, min(width - LANES, int(width * share) // LANES * LANES))


class Swap:
    def __init__(self, place_at, weights, held, sems):
        sp, z, c = place_at
        peer_core = (sp, z * CORES + 1 - c)
        units = weights[0].shape[1]
        mine = pl.ds(pl.multiple_of(c * units, units), units)
        gate_v, up_v, down_v = held
        into = (gate_v.at[:, mine], up_v.at[:, mine], down_v.at[mine, :])
        w_l, w_s, w_r = sems
        self.copies = [
            pltpu.make_async_copy(src, dst, w_l.at[i]) for i, (src, dst) in enumerate(zip(weights, into))
        ] + [
            send(src, dst, w_s.at[i], w_r.at[i], peer_core)
            for i, (src, dst) in enumerate(zip(weights, into))
        ]

    def start(self):
        for copy in self.copies:
            copy.start()

    def wait(self):
        for copy in self.copies:
            copy.wait()


def tables(n_sp, nz, tok, capp, c, routes, rw_all, onehot, share):
    choose = routes.shape[0]
    epad = round_up(n_sp, 16)
    earlier = lax.broadcasted_iota(jnp.int32, (tok, tok), 0) < lax.broadcasted_iota(
        jnp.int32, (tok, tok), 1
    )
    earlier = jnp.where(earlier, 1.0, 0.0).astype(jnp.bfloat16)
    same = lax.broadcasted_iota(jnp.int32, (tok, tok), 0) == lax.broadcasted_iota(
        jnp.int32, (tok, tok), 1
    )
    same = jnp.where(same, 1.0, 0.0).astype(jnp.bfloat16)
    which = lax.broadcasted_iota(jnp.int32, (epad, tok), 0)
    place_in = lax.broadcasted_iota(jnp.int32, (capp, tok), 0).astype(jnp.float32)
    for b in range(nz):
        first = routes[:, (CORES * b) * tok : (CORES * b + 1) * tok]
        second = routes[:, (CORES * b + 1) * tok : (CORES * b + 2) * tok]
        ids = jnp.where(c == 0, first, second)
        weight = jnp.zeros((epad, tok), jnp.float32)
        member = jnp.zeros((epad, tok), jnp.float32)
        for m in range(choose):
            named = ids[m : m + 1, :] == which
            member = jnp.where(named, 1.0, member)
            weight = jnp.where(named, rw_all[b, m : m + 1, :tok], weight)
        rank = dot(member.astype(jnp.bfloat16), earlier)
        rank = jnp.where(member > 0.0, rank, -1.0)
        shares = []
        for e in range(n_sp):
            hit = place_in == rank[e : e + 1, :]
            onehot[b, e * capp : (e + 1) * capp, :] = jnp.where(hit, 1.0, 0.0).astype(jnp.bfloat16)
            shares.append(jnp.where(hit, weight[e : e + 1, :], 0.0).astype(jnp.bfloat16))
        turned = lax.dot_general(
            same,
            jnp.concatenate(shares, axis=0),
            (((1,), (1,)), ((), ())),
            preferred_element_type=jnp.float32,
        )
        share[b] = turned.astype(jnp.bfloat16)


def layer_kernel(
    n_sp, n_tp, tok, capp, q, k, v, sink_in, residual, weight, gain_in, routes_in, rweight,
    gate, up, down, out, normed, stream, onehot, share, gate_v, up_v, down_v,
    q_all, k_all, v_all, k_tail, v_tail, att, got, w_all, res, acc, rw_src, rw_all,
    sink, gain, routes, rw_in,
    in_s, o_s, t_s, t_r, a_s, a_r, g_s, g_r, w_l, w_s, w_r, *rest,
):
    sp, z, c = place()
    tp = z * CORES + c
    nz = n_tp // CORES
    span, kv_cols = k.shape
    cols = q.shape[1]
    width = weight.shape[1]
    kv_local = kv_cols // HEAD
    group = cols // kv_cols
    blocks = span // WINDOW
    pieces = WINDOW // tok
    scale = HEAD ** (-0.5)
    body = pl.ds(WINDOW, span)
    copies = [
        pltpu.make_async_copy(k, k_all.at[body], in_s.at[0]),
        pltpu.make_async_copy(v, v_all.at[body], in_s.at[1]),
        pltpu.make_async_copy(q, q_all, in_s.at[2]),
        pltpu.make_async_copy(rweight, rw_in, in_s.at[3]),
        pltpu.make_async_copy(sink_in, sink, in_s.at[4]),
        pltpu.make_async_copy(routes_in, routes, in_s.at[5]),
        pltpu.make_async_copy(residual, res, in_s.at[6]),
        pltpu.make_async_copy(gain_in, gain, in_s.at[7]),
    ]
    for copy in copies:
        copy.start()

    def out_rows(p):
        rows = pl.ds(pl.multiple_of(p * cols, cols), cols)
        return pltpu.make_async_copy(weight.at[rows], w_all.at[rows], o_s.at[p])

    barrier = pltpu.get_barrier_semaphore()
    for d in range(1, n_tp):
        pl.semaphore_signal(
            barrier, inc=1, device_id=(sp, lax.rem(tp + d, n_tp)), device_id_type=MESH
        )

    for d in range(1, n_sp):
        pl.semaphore_signal(
            barrier, inc=1, device_id=(lax.rem(sp + d, n_sp), tp), device_id_type=MESH
        )
    swap = Swap((sp, z, c), (gate, up, down), (gate_v, up_v, down_v), (w_l, w_s, w_r))
    rw_src[...] = jnp.zeros_like(rw_src)
    copies[3].wait()
    rw_src[: rweight.shape[0], :tok] = rw_in[...]
    rw_all[z] = rw_src[...]
    pl.semaphore_wait(barrier, n_tp - 1 + n_sp - 1)
    ahead = (lax.rem(sp + 1, n_sp), tp)
    last = pl.ds(span, WINDOW)
    tails = (
        send(k_all.at[last], k_tail, t_s.at[0], t_r.at[0], ahead),
        send(v_all.at[last], v_tail, t_s.at[1], t_r.at[1], ahead),
    )
    copies[0].wait()
    copies[1].wait()

    @pl.when(sp < n_sp - 1)
    def _():
        for copy in tails:
            copy.start()

    def tell(d):
        there = lax.rem(z + d, nz)
        return send(rw_src, rw_all.at[z], g_s.at[d], g_r.at[z], (sp, there * CORES + c))

    def told(d):
        there = lax.rem(z + d, nz)
        return send(rw_src, rw_all.at[there], g_s.at[d], g_r.at[there], (sp, there * CORES + c))

    for d in range(1, nz):
        tell(d).start()
    copies[2].wait()
    copies[4].wait()
    for p in range(n_tp):
        out_rows(p).start()

    row = lax.broadcasted_iota(jnp.int32, (WINDOW, 2 * WINDOW), 0)
    col = lax.broadcasted_iota(jnp.int32, (WINDOW, 2 * WINDOW), 1)
    distance = row + WINDOW - col
    banded = (distance >= 0) & (distance < WINDOW)
    low = z < nz // 2
    half = max(1, blocks // 2)

    own_cols = pl.ds(pl.multiple_of(tp * cols, cols), cols)

    def to_owner(dest):
        at = pl.multiple_of(dest * tok, tok)
        return send(
            att.at[pl.ds(at, tok)], got.at[:, own_cols], a_s.at[dest], a_r.at[tp], (sp, dest)
        )

    def attend(i, carry):
        turned = jnp.where(i < half, lax.rem(i + 1, half), i)
        block = jnp.where(low, blocks - 1 - i, turned)

        @pl.when(block == 0)
        def _():
            @pl.when(sp > 0)
            def _():
                for copy in tails:
                    copy.wait_recv()
                k_all[pl.ds(0, WINDOW), :] = k_tail[...]
                v_all[pl.ds(0, WINDOW), :] = v_tail[...]

            @pl.when(sp == 0)
            def _():
                k_all[pl.ds(0, WINDOW), :] = jnp.zeros((WINDOW, kv_cols), jnp.bfloat16)
                v_all[pl.ds(0, WINDOW), :] = jnp.zeros((WINDOW, kv_cols), jnp.bfloat16)

        at = pl.multiple_of(block * WINDOW, WINDOW)
        start = jnp.where((sp == 0) & (block == 0), WINDOW, 0)
        allowed = banded & (col >= start)
        band = pl.ds(at, 2 * WINDOW)
        for g in range(kv_local):
            keys = k_all[band, g * HEAD : (g + 1) * HEAD]
            values = v_all[band, g * HEAD : (g + 1) * HEAD]
            heads = []
            for m in range(group):
                h = g * group + m
                query = q_all[pl.ds(at, WINDOW), h * HEAD : (h + 1) * HEAD] * jnp.bfloat16(scale)
                scores = lax.dot_general(
                    query, keys, (((1,), (1,)), ((), ())), preferred_element_type=jnp.float32
                )
                logits = jnp.where(allowed, scores, -jnp.inf)
                top = jnp.maximum(jnp.max(logits, axis=-1, keepdims=True), sink[h])
                raised = jnp.exp(logits - top)
                total = jnp.sum(raised, axis=-1, keepdims=True) + jnp.exp(sink[h] - top)
                probs = (raised * (1.0 / total)).astype(jnp.bfloat16)
                heads.append(dot(probs, values))
            att[pl.ds(at, WINDOW), g * group * HEAD : (g + 1) * group * HEAD] = jnp.concatenate(
                heads, axis=1
            ).astype(jnp.bfloat16)
        for piece in range(pieces):
            dest = block * pieces + piece

            @pl.when(dest != tp)
            def _():
                to_owner(dest).start()

        return carry

    lax.fori_loop(0, blocks, attend, 0)
    for d in range(1, nz):
        told(d).wait_recv()
    copies[5].wait()
    tables(n_sp, nz, tok, capp, c, routes, rw_all, onehot, share)
    swap.start()
    got[:, own_cols] = att[pl.ds(pl.multiple_of(tp * tok, tok), tok), :]
    copies[6].wait()
    copies[7].wait()
    wide = math.gcd(width, 512)

    def begin(at):
        acc[:, at] = res[:, at].astype(jnp.float32)

    tiled(width, wide, begin)
    for p in range(n_tp):
        out_rows(p).wait()

    part = n_tp // 2

    def arrived(i, carry):
        p = jnp.where(low, n_tp - 1 - i, i)

        @pl.when(tp != p)
        def _():
            into = got.at[:, pl.ds(pl.multiple_of(p * cols, cols), cols)]
            send(att.at[pl.ds(0, tok)], into, a_s.at[p], a_r.at[p], (sp, p)).wait_recv()

        return carry

    for far in range(2):
        lax.fori_loop(far * part, (far + 1) * part, arrived, 0)
        first = jnp.where(low, (1 - far) * part, far * part) * cols
        rows = pl.ds(pl.multiple_of(first, part * cols), part * cols)

        def one(at):
            acc[:, at] = acc[:, at] + dot(got[:, rows], w_all[rows, at])

        tiled(width, wide, one)

    squares = jnp.zeros((tok, 1), jnp.float32)
    for t in range(width // wide):
        at = slice(t * wide, (t + 1) * wide)
        held = acc[:, at].astype(jnp.bfloat16)
        stream[:, at] = held
        held32 = held.astype(jnp.float32)
        squares = squares + jnp.sum(held32 * held32, axis=-1, keepdims=True)
    root = lax.rsqrt(squares * (1.0 / width) + eps)
    for t in range(width // wide):
        at = slice(t * wide, (t + 1) * wide)
        normed[:, at] = (stream[:, at].astype(jnp.float32) * root * gain[:, at]).astype(
            jnp.bfloat16
        )
    expert_kernel(
        n_sp, nz, swap, normed, stream, onehot, share, out, gate_v, up_v, down_v, *rest
    )
    for p in range(n_tp):
        @pl.when(tp != p)
        def _():
            to_owner(p).wait_send()

    for d in range(1, nz):
        tell(d).wait_send()

    @pl.when(sp < n_sp - 1)
    def _():
        for copy in tails:
            copy.wait_send()


def local(
    query_heads,
    key_heads,
    value_heads,
    sink_logit,
    residual,
    out_weight,
    norm_gain,
    routes,
    route_weight,
    gate_weight,
    up_weight,
    down_weight,
):
    n_sp, n_tp = lax.axis_size("sp"), lax.axis_size("tp")
    nz = n_tp // CORES
    span, cols = query_heads.shape
    kv_cols = key_heads.shape[1]
    tok, width = residual.shape
    choose = routes.shape[1]
    capp = round_up(max(2, 5 * tok * choose // (4 * n_sp)), 16)
    slots = n_sp * capp
    hidden = CORES * gate_weight.shape[2]
    ka = split_columns(width, DISPATCH_SHARE)
    na = split_columns(width, RETURN_SHARE)
    kb, nb = width - ka, width - na
    vmem = pl.BlockSpec(memory_space=pltpu.VMEM)
    inputs = (
        query_heads, key_heads, value_heads, sink_logit, residual, out_weight,
        norm_gain.reshape(1, -1), routes.T, route_weight.T,
        gate_weight[0], up_weight[0], down_weight[0],
    )
    dma = pltpu.SemaphoreType.DMA
    bf = jnp.bfloat16
    line = [dma((nz,))] * 4
    scratch = (
        [
            pltpu.VMEM((tok, width), bf),
            pltpu.VMEM((tok, width), bf),
            pltpu.VMEM((nz, slots, tok), bf),
            pltpu.VMEM((nz, tok, slots), bf),
            pltpu.VMEM((width, hidden), bf),
            pltpu.VMEM((width, hidden), bf),
            pltpu.VMEM((hidden, width), bf),
            pltpu.VMEM((span, cols), bf),
            pltpu.VMEM((span + WINDOW, kv_cols), bf),
            pltpu.VMEM((span + WINDOW, kv_cols), bf),
            pltpu.VMEM((WINDOW, kv_cols), bf),
            pltpu.VMEM((WINDOW, kv_cols), bf),
            pltpu.VMEM((span, cols), bf),
            pltpu.VMEM((tok, n_tp * cols), bf),
            pltpu.VMEM((n_tp * cols, width), bf),
            pltpu.VMEM((tok, width), bf),
            pltpu.VMEM((tok, width), jnp.float32),
            pltpu.VMEM((8, LANES), jnp.float32),
            pltpu.VMEM((nz, 8, LANES), jnp.float32),
            pltpu.SMEM(sink_logit.shape, jnp.float32),
            pltpu.VMEM((1, width), jnp.float32),
            pltpu.VMEM(routes.shape[::-1], routes.dtype),
            pltpu.VMEM(route_weight.shape[::-1], jnp.float32),
            dma((8,)),
            dma((n_tp,)),
            dma((2,)),
            dma((2,)),
            dma((n_tp,)),
            dma((n_tp,)),
            dma((nz,)),
            dma((nz,)),
        ]
        + [dma((3,))] * 3
        + [pltpu.VMEM((nz, tok, w), bf) for w in halves(ka)]
        + [pltpu.VMEM((nz, n_sp, capp, w), bf) for w in halves(ka)]
        + [pltpu.VMEM((n_sp, capp, kb), bf)]
        + [pltpu.VMEM((nz, n_sp, capp, w), bf) for w in (*halves(ka), kb)]
        + [pltpu.VMEM((slots, hidden), bf)]
        + [pltpu.VMEM((nz, n_sp, capp, w), bf) for w in (*halves(na), nb, *halves(na))]
        + [pltpu.VMEM((n_sp, capp, nb), bf)]
        + [pltpu.VMEM((nz, tok, w), bf) for w in halves(na) * 3]
        + [pltpu.VMEM((nz, n_sp, capp, nb), bf)] * 2
        + [dma((CHUNKS * nz,))] * 4
        + [dma((CHUNKS * nz, n_sp))] * 2
        + [dma((n_sp,))] * 2
        + line
        + [dma((CHUNKS * nz, n_sp))] * 2
        + [dma((n_sp,))] * 2
        + [dma((CHUNKS * nz,))] * 4
        + line
    )
    return pl.pallas_call(
        functools.partial(layer_kernel, n_sp, n_tp, tok, capp),
        out_shape=jax.ShapeDtypeStruct((tok, width), bf),
        in_specs=[pl.BlockSpec(memory_space=pltpu.HBM)] * len(inputs),
        out_specs=vmem,
        scratch_shapes=scratch,
        compiler_params=pltpu.CompilerParams(
            collective_id=0, has_side_effects=True, vmem_limit_bytes=held_bytes(scratch) + SPARE
        ),
        name="layer",
    )(*[pltpu.with_memory_space_constraint(x, pltpu.HBM) for x in inputs])


def solution(mesh):
    placed = (
        P("sp", "tp"),
        P("sp", "tp"),
        P("sp", "tp"),
        P("tp"),
        P(("sp", "tp"), None),
        P(),
        P(),
        P("sp", None),
        P(("sp", "tp"), None),
        P("sp", None, "tp"),
        P("sp", None, "tp"),
        P("sp", "tp", None),
    )
    return jax.shard_map(
        local, mesh=mesh, in_specs=placed, out_specs=P(("sp", "tp"), None), check_vma=False
    )
```

```python
import functools
import math

import jax
import jax.numpy as jnp
from jax import lax
from jax.experimental import pallas as pl
from jax.experimental.pallas import tpu as pltpu
from jax.sharding import PartitionSpec as P

HEAD = 64
WINDOW = 128


eps = 1e-06
clamp_limit = 7.0
sigmoid_alpha = 1.702


MESH = pl.DeviceIdType.MESH
CORES = 2
LANES = 128
SPARE = 2 * 1024 * 1024


def round_up(value, unit):
    return (value + unit - 1) // unit * unit


def place():
    tp = lax.axis_index("tp")
    return lax.axis_index("sp"), tp // CORES, lax.rem(tp, CORES)


def partner_of(sp, d, n_sp):
    if n_sp & (n_sp - 1):
        return lax.rem(sp + d, n_sp)
    total, bit = 0, 1
    while bit < n_sp:
        total = total + lax.rem(sp // bit + d // bit, 2) * bit
        bit *= 2
    return total


def source_of(sp, d, n_sp):
    if n_sp & (n_sp - 1):
        return lax.rem(sp + n_sp - d, n_sp)
    return partner_of(sp, d, n_sp)


def send(src, dst, send_sem, recv_sem, device):
    return pltpu.make_async_remote_copy(
        src_ref=src,
        dst_ref=dst,
        send_sem=send_sem,
        recv_sem=recv_sem,
        device_id=device,
        device_id_type=MESH,
    )


def dot(a, b):
    return jnp.dot(a, b, preferred_element_type=jnp.float32)


def tiled(extent, tile, visit):
    for start in range(0, extent, tile):
        visit(pl.ds(start, min(tile, extent - start)))


def shifted(cols, offset):
    return pl.ds(cols.start + offset, cols.size)


CHUNKS = 2
NEAR, SERVE = 1, 2
RAW = (3, 4)
CHAIN = 5
PUSH = (6, 7)
RELAY = (8, 9)
LAST_IN = 4
KINDS = 16
BLOCKS = 64
PER_WORD = 3


def sides(nz, z, away):
    return [b for b in ((z + away, z - away) if away else (z,)) if 0 <= b < nz]


def plain_order(nz, z):
    order = []
    for i in range(1, nz):
        order += [(RAW[j], b) for b in sides(nz, z, i) for j in range(CHUNKS)]
        order += [(NEAR, b) for b in sides(nz, z, i - 1)]
        if i > 1:
            order += [(SERVE, b) for b in sides(nz, z, i - 2)]
    order += [(SERVE, b) for b in sides(nz, z, nz - 2)]
    order += [(NEAR, b) for b in sides(nz, z, nz - 1)]
    order += [(SERVE, b) for b in sides(nz, z, nz - 1)]
    for away in range(nz - 1, -1, -1):
        order += [(PUSH[j], b) for b in sides(nz, z, away) for j in range(CHUNKS)]
    order += [(CHAIN, b) for b in sides(nz, z, nz - 1)]
    for away in range(nz - 1, 0, -1):
        order += [(CHAIN, b) for b in sides(nz, z, away - 1)]
        order += [(RELAY[j], b) for b in sides(nz, z, away) for j in range(CHUNKS)]
    return order


ORDERS = {
    4: [
        [
            (RAW[1], 1), (RAW[0], 1), (RAW[0], 2), (NEAR, 0), (SERVE, 0),
            (RAW[1], 2), (NEAR, 1), (SERVE, 1), (CHAIN, 1), (PUSH[0], 1),
            (RAW[0], 3), (RELAY[0], 1), (NEAR, 2), (RAW[1], 3), (SERVE, 2),
            (CHAIN, 2), (PUSH[1], 2), (NEAR, 3), (SERVE, 3), (PUSH[1], 3),
            (PUSH[0], 3), (PUSH[1], 1), (CHAIN, 3), (PUSH[0], 2), (PUSH[0], 0),
            (RELAY[1], 3), (RELAY[0], 3), (RELAY[1], 2), (PUSH[1], 0), (RELAY[0], 2),
            (CHAIN, 0), (RELAY[1], 1),
        ],
        [
            (RAW[0], 0), (RAW[0], 2), (RAW[1], 0), (NEAR, 1), (RAW[1], 2),
            (RAW[0], 3), (NEAR, 0), (RAW[1], 3), (NEAR, 2), (SERVE, 1),
            (SERVE, 0), (NEAR, 3), (SERVE, 2), (PUSH[0], 0), (SERVE, 3),
            (PUSH[1], 0), (PUSH[0], 3), (PUSH[1], 3), (CHAIN, 2), (PUSH[1], 1),
            (CHAIN, 3), (PUSH[1], 2), (CHAIN, 0), (RELAY[1], 3), (RELAY[0], 3),
            (PUSH[0], 2), (CHAIN, 1), (RELAY[1], 0), (RELAY[1], 2), (PUSH[0], 1),
            (RELAY[0], 0), (RELAY[0], 2),
        ],
    ],
}
DISPATCH_SHARE = 0.6875
RETURN_SHARE = 0.75


def order_of(nz, z):
    if nz not in ORDERS:
        return plain_order(nz, z)
    if z < nz // 2:
        return ORDERS[nz][z]
    return [(kind, nz - 1 - b) for kind, b in ORDERS[nz][nz - 1 - z]]


def order_words(nz):
    orders = [order_of(nz, z) for z in range(nz)]
    words = round_up(max(len(order) for order in orders), PER_WORD) // PER_WORD
    table = []
    for order in orders:
        codes = [b * KINDS + kind for kind, b in order]
        codes += [0] * (words * PER_WORD - len(codes))
        base = KINDS * BLOCKS
        table.append([
            sum(code * base**i for i, code in enumerate(codes[w * PER_WORD : (w + 1) * PER_WORD]))
            for w in range(words)
        ])
    return table, words


def both_sides(z, nz, away, visit):
    def one(behind, carry):
        block = z + away * (1 - 2 * behind)

        @pl.when((block >= 0) & (block < nz))
        def _():
            visit(block, behind)

        return carry

    lax.fori_loop(0, 2, one, 0)


def expert_kernel(
    n_sp, nz, swap, normed, stream, onehot, share, out,
    gate_v, up_v, down_v, toks_0, toks_1, comp_a0, comp_a1, comp_b, rows_a0, rows_a1, rows_b, hid,
    sums_a0, sums_a1, sums_b, back_a0, back_a1, back_b, a_out0, a_out1, a_up0, a_up1, a_dn0, a_dn1,
    b_up, b_dn, ru_s, ru_r, rd_s, rd_r, xa_s, xa_r, xb_s, xb_r,
    bu_s, bu_r, bd_s, bd_r, ya_s, ya_r, yb_s, yb_r,
    au_s, au_r, ad_s, ad_r, cu_s, cu_r, cd_s, cd_r,
):
    sp, z, c = place()
    tp = z * CORES + c
    toks, comp_a, rows_a = (toks_0, toks_1), (comp_a0, comp_a1), (rows_a0, rows_a1)
    sums_a, back_a = (sums_a0, sums_a1), (back_a0, back_a1)
    a_out, a_up, a_dn = (a_out0, a_out1), (a_up0, a_up1), (a_dn0, a_dn1)
    above = (sp, lax.rem(z + 1, nz) * CORES + c)
    below = (sp, lax.rem(z + nz - 1, nz) * CORES + c)
    capp, kb, nb = rows_b.shape[2], rows_b.shape[3], sums_b.shape[3]
    ins = spans([ref.shape[-1] for ref in rows_a])
    outs = spans([ref.shape[-1] for ref in sums_a])
    ka, na = normed.shape[1] - kb, normed.shape[1] - nb
    slots = n_sp * capp
    units = gate_v.shape[1] // CORES
    tile, wide = 512, 512

    def raw_above(block, j, src):
        at = j * nz + block
        return send(src, toks[j].at[block], ru_s.at[at], ru_r.at[at], above)

    def raw_below(block, j, src):
        at = j * nz + block
        return send(src, toks[j].at[block], rd_s.at[at], rd_r.at[at], below)

    def own_raw(j):
        return normed.at[:, pl.ds(ins[j].start, ins[j].size)]

    for j in range(CHUNKS):
        @pl.when(z < nz - 1)
        def _():
            raw_above(z, j, own_raw(j)).start()

        @pl.when(z > 0)
        def _():
            raw_below(z, j, own_raw(j)).start()

    def xa_to(block, j, d):
        e = partner_of(sp, d, n_sp)
        at = j * nz + block
        return send(
            comp_a[j].at[block, e], rows_a[j].at[block, sp], xa_s.at[at, d], xa_r.at[at, d], (e, tp)
        )

    def xa_from(block, j, d):
        e = source_of(sp, d, n_sp)
        at = j * nz + block
        return send(
            comp_a[j].at[block, e], rows_a[j].at[block, e], xa_s.at[at, d], xa_r.at[at, d], (e, tp)
        )

    def xb_to(d):
        e = partner_of(sp, d, n_sp)
        return send(comp_b.at[e], rows_b.at[z, sp], xb_s.at[d], xb_r.at[d], (e, tp))

    def xb_from(d):
        e = source_of(sp, d, n_sp)
        return send(comp_b.at[e], rows_b.at[z, e], xb_s.at[d], xb_r.at[d], (e, tp))

    def b_above(block):
        return send(rows_b.at[block], rows_b.at[block], bu_s.at[block], bu_r.at[block], above)

    def b_below(block):
        return send(rows_b.at[block], rows_b.at[block], bd_s.at[block], bd_r.at[block], below)

    def deal_b(cols):
        picked = dot(onehot[z], normed[:, shifted(cols, ka)])
        comp_b[:, :, cols] = picked.astype(jnp.bfloat16).reshape(n_sp, capp, cols.size)

    tiled(kb, tile, deal_b)
    for d in range(1, n_sp):
        xb_to(d).start()
    rows_b[z, sp] = comp_b[sp]

    def deal(block, j, src):
        def one(cols):
            picked = dot(onehot[block], src(cols))
            comp_a[j][block, :, :, cols] = picked.astype(jnp.bfloat16).reshape(
                n_sp, capp, cols.size
            )

        tiled(ins[j].size, tile, one)
        for d in range(1, n_sp):
            xa_to(block, j, d).start()
        rows_a[j][block, sp] = comp_a[j][block, sp]

    for j in range(CHUNKS):
        deal(z, j, lambda cols: normed[:, shifted(cols, ins[j].start)])

    def spread_own():
        for d in range(1, n_sp):
            xb_from(d).wait_recv()

        @pl.when(z < nz - 1)
        def _():
            b_above(z).start()

        @pl.when(z > 0)
        def _():
            b_below(z).start()

    def gather_raw(block, behind, j):
        @pl.when(behind == 1)
        def _():
            raw_above(block, j, toks[j].at[block]).wait_recv()

            @pl.when(z < nz - 1)
            def _():
                raw_above(block, j, toks[j].at[block]).start()

        @pl.when(behind == 0)
        def _():
            raw_below(block, j, toks[j].at[block]).wait_recv()

            @pl.when(z > 0)
            def _():
                raw_below(block, j, toks[j].at[block]).start()

        deal(block, j, lambda cols: toks[j][block, :, cols])

    def gather_b(block, behind):
        @pl.when(behind == 1)
        def _():
            b_above(block).wait_recv()

            @pl.when(z < nz - 1)
            def _():
                b_above(block).start()

        @pl.when(behind == 0)
        def _():
            b_below(block).wait_recv()

            @pl.when(z > 0)
            def _():
                b_below(block).start()

    unit = min(256, CORES * units)

    def serve(block):
        for j in range(CHUNKS):
            for d in range(1, n_sp):
                xa_from(block, j, d).wait_recv()

        def through(weight, cols):
            total = dot(rows_b[block].reshape(slots, kb), weight[ka:, cols])
            for j in range(CHUNKS):
                part = rows_a[j][block].reshape(slots, ins[j].size)
                total = total + dot(part, weight[ins[j].start : ins[j].start + ins[j].size, cols])
            return total

        def one(cols):
            gate_pre, upward = through(gate_v, cols), through(up_v, cols)
            capped = jnp.minimum(gate_pre, clamp_limit)
            linear = jnp.clip(upward, -clamp_limit, clamp_limit)
            gated = capped * jax.nn.sigmoid(sigmoid_alpha * capped)
            hid[:, cols] = (gated * (linear + 1.0)).astype(jnp.bfloat16)

        tiled(CORES * units, unit, one)

        def part_a(j, cols):
            part = dot(hid[...], down_v[:, shifted(cols, outs[j].start)]).astype(jnp.bfloat16)
            sums_a[j][block, :, :, cols] = part.reshape(n_sp, capp, cols.size)

        def part_b(cols):
            part = dot(hid[...], down_v[:, shifted(cols, na)]).astype(jnp.bfloat16)
            sums_b[block, :, :, cols] = part.reshape(n_sp, capp, cols.size)

        for j in range(CHUNKS):
            tiled(outs[j].size, wide, functools.partial(part_a, j))
        tiled(nb, wide, part_b)

    def ya_to(block, j, d):
        e = partner_of(sp, d, n_sp)
        at = j * nz + block
        return send(
            sums_a[j].at[block, e], back_a[j].at[block, sp], ya_s.at[at, d], ya_r.at[at, d], (e, tp)
        )

    def ya_from(block, j, d):
        e = source_of(sp, d, n_sp)
        at = j * nz + block
        return send(
            sums_a[j].at[block, e], back_a[j].at[block, e], ya_s.at[at, d], ya_r.at[at, d], (e, tp)
        )

    def yb_to(d):
        e = partner_of(sp, d, n_sp)
        return send(sums_b.at[z, e], back_b.at[sp], yb_s.at[d], yb_r.at[d], (e, tp))

    def yb_from(d):
        e = source_of(sp, d, n_sp)
        return send(sums_b.at[z, e], back_b.at[e], yb_s.at[d], yb_r.at[d], (e, tp))

    def a_above(block, j):
        at = j * nz + block
        return send(a_out[j].at[block], a_up[j].at[block], au_s.at[at], au_r.at[at], above)

    def a_below(block, j):
        at = j * nz + block
        return send(a_out[j].at[block], a_dn[j].at[block], ad_s.at[at], ad_r.at[at], below)

    def c_above(block):
        return send(sums_b.at[block], b_up.at[block], cu_s.at[block], cu_r.at[block], above)

    def c_below(block):
        return send(sums_b.at[block], b_dn.at[block], cd_s.at[block], cd_r.at[block], below)

    def push(block, j):
        for d in range(1, n_sp):
            ya_to(block, j, d).start()
        back_a[j][block, sp] = sums_a[j][block, sp]

    def add_b(block, arrived):
        total = sums_b[block].astype(jnp.float32) + arrived[block].astype(jnp.float32)
        sums_b[block] = total.astype(jnp.bfloat16)

    def relay_b(block, behind):
        @pl.when(behind == 0)
        def _():
            @pl.when(z > 0)
            def _():
                c_above(block).wait_recv()
                add_b(block, b_up)

            c_above(block).start()

        @pl.when(behind == 1)
        def _():
            @pl.when(z < nz - 1)
            def _():
                c_below(block).wait_recv()
                add_b(block, b_dn)

            c_below(block).start()

    def settle_b():
        @pl.when(z > 0)
        def _():
            c_above(z).wait_recv()
            add_b(z, b_up)

        @pl.when(z < nz - 1)
        def _():
            c_below(z).wait_recv()
            add_b(z, b_dn)

        for d in range(1, n_sp):
            yb_to(d).start()
        back_b[sp] = sums_b[z, sp]

    def combined(block, j, cols):
        return dot(share[block], back_a[j][block, :, :, cols].reshape(slots, cols.size))

    def relay_a(block, behind, j):
        for d in range(1, n_sp):
            ya_from(block, j, d).wait_recv()

        @pl.when(behind == 0)
        def _():
            @pl.when(z > 0)
            def _():
                a_above(block, j).wait_recv()

            def one(cols):
                total = combined(block, j, cols)
                total = jnp.where(z > 0, total + a_up[j][block, :, cols].astype(jnp.float32), total)
                a_out[j][block, :, cols] = total.astype(jnp.bfloat16)

            tiled(outs[j].size, wide, one)
            a_above(block, j).start()

        @pl.when(behind == 1)
        def _():
            @pl.when(z < nz - 1)
            def _():
                a_below(block, j).wait_recv()

            def one(cols):
                total = combined(block, j, cols)
                total = jnp.where(
                    z < nz - 1, total + a_dn[j][block, :, cols].astype(jnp.float32), total
                )
                a_out[j][block, :, cols] = total.astype(jnp.bfloat16)

            tiled(outs[j].size, wide, one)
            a_below(block, j).start()

    swap.wait()
    table, words = order_words(nz)

    def word_of(w):
        word = jnp.int32(0)
        for level in range(nz):
            for at in range(words):
                word = jnp.where((z == level) & (w == at), jnp.int32(table[level][at]), word)
        return word

    def task(i, word):
        kind = lax.rem(word, KINDS)
        block = lax.rem(word // KINDS, BLOCKS)
        behind = jnp.where(block < z, 1, 0)
        elsewhere = block != z

        @pl.when(kind <= LAST_IN)
        def _():
            for j in range(CHUNKS):
                @pl.when(kind == RAW[j])
                def _():
                    gather_raw(block, behind, j)

            @pl.when((kind == NEAR) & elsewhere)
            def _():
                gather_b(block, behind)

            @pl.when((kind == NEAR) & (block == z))
            def _():
                spread_own()

            @pl.when(kind == SERVE)
            def _():
                serve(block)

        @pl.when(kind > LAST_IN)
        def _():
            for j in range(CHUNKS):
                @pl.when(kind == PUSH[j])
                def _():
                    push(block, j)

                @pl.when(kind == RELAY[j])
                def _():
                    relay_a(block, behind, j)

            @pl.when((kind == CHAIN) & elsewhere)
            def _():
                relay_b(block, behind)

            @pl.when((kind == CHAIN) & (block == z))
            def _():
                settle_b()

        return word // (KINDS * BLOCKS)

    def tasks(w, carry):
        lax.fori_loop(0, PER_WORD, task, word_of(w))
        return carry

    lax.fori_loop(0, words, tasks, 0)

    for d in range(1, n_sp):
        yb_from(d).wait_recv()

    def final_b(cols):
        at = shifted(cols, na)
        total = dot(share[z], back_b[:, :, cols].reshape(slots, cols.size))
        out[:, at] = (stream[:, at].astype(jnp.float32) + total).astype(jnp.bfloat16)

    tiled(nb, wide, final_b)
    for j in range(CHUNKS):
        for d in range(1, n_sp):
            ya_from(z, j, d).wait_recv()

        @pl.when(z > 0)
        def _():
            a_above(z, j).wait_recv()

        @pl.when(z < nz - 1)
        def _():
            a_below(z, j).wait_recv()

        def final_a(cols):
            at = shifted(cols, outs[j].start)
            total = combined(z, j, cols)
            total = jnp.where(z > 0, total + a_up[j][z, :, cols].astype(jnp.float32), total)
            total = jnp.where(z < nz - 1, total + a_dn[j][z, :, cols].astype(jnp.float32), total)
            out[:, at] = (stream[:, at].astype(jnp.float32) + total).astype(jnp.bfloat16)

        tiled(outs[j].size, wide, final_a)

    for d in range(1, n_sp):
        xb_to(d).wait_send()
        yb_to(d).wait_send()

    def drain_exchange(block):
        for j in range(CHUNKS):
            for d in range(1, n_sp):
                xa_to(block, j, d).wait_send()
                ya_to(block, j, d).wait_send()

    drain_exchange(z)

    @pl.when(z < nz - 1)
    def _():
        b_above(z).wait_send()
        for j in range(CHUNKS):
            raw_above(z, j, own_raw(j)).wait_send()

    @pl.when(z > 0)
    def _():
        b_below(z).wait_send()
        for j in range(CHUNKS):
            raw_below(z, j, own_raw(j)).wait_send()

    def drain(block, behind):
        drain_exchange(block)

        @pl.when(behind == 0)
        def _():
            c_above(block).wait_send()
            for j in range(CHUNKS):
                a_above(block, j).wait_send()

        @pl.when(behind == 1)
        def _():
            c_below(block).wait_send()
            for j in range(CHUNKS):
                a_below(block, j).wait_send()

        @pl.when((behind == 1) & (z < nz - 1))
        def _():
            b_above(block).wait_send()
            for j in range(CHUNKS):
                raw_above(block, j, toks[j].at[block]).wait_send()

        @pl.when((behind == 0) & (z > 0))
        def _():
            b_below(block).wait_send()
            for j in range(CHUNKS):
                raw_below(block, j, toks[j].at[block]).wait_send()

    def drain_all(i, carry):
        both_sides(z, nz, i, drain)
        return carry

    lax.fori_loop(1, nz, drain_all, 0)


def held_bytes(scratch):
    total = 0
    for ref in scratch:
        if getattr(ref, "memory_space", None) == pltpu.VMEM:
            item = jnp.dtype(ref.dtype).itemsize
            lead = math.prod(ref.shape[:-2])
            rows = round_up(ref.shape[-2], 32 // item)
            total += lead * rows * round_up(ref.shape[-1], LANES) * item
    return total


def spans(widths):
    return [pl.ds(sum(widths[:j]), width) for j, width in enumerate(widths)]


def halves(width):
    first = round_up(width // 2, LANES)
    return (first, width - first)


def split_columns(width, share):
    return max(2 * LANES, min(width - LANES, int(width * share) // LANES * LANES))


class Swap:
    def __init__(self, place_at, weights, held, sems):
        sp, z, c = place_at
        peer_core = (sp, z * CORES + 1 - c)
        units = weights[0].shape[1]
        mine = pl.ds(pl.multiple_of(c * units, units), units)
        gate_v, up_v, down_v = held
        into = (gate_v.at[:, mine], up_v.at[:, mine], down_v.at[mine, :])
        w_l, w_s, w_r = sems
        self.copies = [
            pltpu.make_async_copy(src, dst, w_l.at[i]) for i, (src, dst) in enumerate(zip(weights, into))
        ] + [
            send(src, dst, w_s.at[i], w_r.at[i], peer_core)
            for i, (src, dst) in enumerate(zip(weights, into))
        ]

    def start(self):
        for copy in self.copies:
            copy.start()

    def wait(self):
        for copy in self.copies:
            copy.wait()


def tables(n_sp, nz, tok, capp, c, routes, rw_all, onehot, share):
    choose = routes.shape[0]
    epad = round_up(n_sp, 16)
    earlier = lax.broadcasted_iota(jnp.int32, (tok, tok), 0) < lax.broadcasted_iota(
        jnp.int32, (tok, tok), 1
    )
    earlier = jnp.where(earlier, 1.0, 0.0).astype(jnp.bfloat16)
    same = lax.broadcasted_iota(jnp.int32, (tok, tok), 0) == lax.broadcasted_iota(
        jnp.int32, (tok, tok), 1
    )
    same = jnp.where(same, 1.0, 0.0).astype(jnp.bfloat16)
    which = lax.broadcasted_iota(jnp.int32, (epad, tok), 0)
    place_in = lax.broadcasted_iota(jnp.int32, (capp, tok), 0).astype(jnp.float32)
    for b in range(nz):
        first = routes[:, (CORES * b) * tok : (CORES * b + 1) * tok]
        second = routes[:, (CORES * b + 1) * tok : (CORES * b + 2) * tok]
        ids = jnp.where(c == 0, first, second)
        weight = jnp.zeros((epad, tok), jnp.float32)
        member = jnp.zeros((epad, tok), jnp.float32)
        for m in range(choose):
            named = ids[m : m + 1, :] == which
            member = jnp.where(named, 1.0, member)
            weight = jnp.where(named, rw_all[b, m : m + 1, :tok], weight)
        rank = dot(member.astype(jnp.bfloat16), earlier)
        rank = jnp.where(member > 0.0, rank, -1.0)
        shares = []
        for e in range(n_sp):
            hit = place_in == rank[e : e + 1, :]
            onehot[b, e * capp : (e + 1) * capp, :] = jnp.where(hit, 1.0, 0.0).astype(jnp.bfloat16)
            shares.append(jnp.where(hit, weight[e : e + 1, :], 0.0).astype(jnp.bfloat16))
        turned = lax.dot_general(
            same,
            jnp.concatenate(shares, axis=0),
            (((1,), (1,)), ((), ())),
            preferred_element_type=jnp.float32,
        )
        share[b] = turned.astype(jnp.bfloat16)


def layer_kernel(
    n_sp, n_tp, tok, capp, q, k, v, sink_in, residual, weight, gain_in, routes_in, rweight,
    gate, up, down, out, normed, stream, onehot, share, gate_v, up_v, down_v,
    q_all, k_all, v_all, k_tail, v_tail, att, got, w_all, res, acc, rw_src, rw_all,
    sink, gain, routes, rw_in,
    in_s, o_s, t_s, t_r, a_s, a_r, g_s, g_r, w_l, w_s, w_r, *rest,
):
    sp, z, c = place()
    tp = z * CORES + c
    nz = n_tp // CORES
    span, kv_cols = k.shape
    cols = q.shape[1]
    width = weight.shape[1]
    kv_local = kv_cols // HEAD
    group = cols // kv_cols
    blocks = span // WINDOW
    pieces = WINDOW // tok
    scale = HEAD ** (-0.5)
    body = pl.ds(WINDOW, span)
    copies = [
        pltpu.make_async_copy(k, k_all.at[body], in_s.at[0]),
        pltpu.make_async_copy(v, v_all.at[body], in_s.at[1]),
        pltpu.make_async_copy(q, q_all, in_s.at[2]),
        pltpu.make_async_copy(rweight, rw_in, in_s.at[3]),
        pltpu.make_async_copy(sink_in, sink, in_s.at[4]),
        pltpu.make_async_copy(routes_in, routes, in_s.at[5]),
        pltpu.make_async_copy(residual, res, in_s.at[6]),
        pltpu.make_async_copy(gain_in, gain, in_s.at[7]),
    ]
    for copy in copies:
        copy.start()

    def out_rows(p):
        rows = pl.ds(pl.multiple_of(p * cols, cols), cols)
        return pltpu.make_async_copy(weight.at[rows], w_all.at[rows], o_s.at[p])

    barrier = pltpu.get_barrier_semaphore()
    for d in range(1, n_tp):
        pl.semaphore_signal(
            barrier, inc=1, device_id=(sp, lax.rem(tp + d, n_tp)), device_id_type=MESH
        )

    for d in range(1, n_sp):
        pl.semaphore_signal(
            barrier, inc=1, device_id=(lax.rem(sp + d, n_sp), tp), device_id_type=MESH
        )
    swap = Swap((sp, z, c), (gate, up, down), (gate_v, up_v, down_v), (w_l, w_s, w_r))
    rw_src[...] = jnp.zeros_like(rw_src)
    copies[3].wait()
    rw_src[: rweight.shape[0], :tok] = rw_in[...]
    rw_all[z] = rw_src[...]
    pl.semaphore_wait(barrier, n_tp - 1 + n_sp - 1)
    ahead = (lax.rem(sp + 1, n_sp), tp)
    last = pl.ds(span, WINDOW)
    tails = (
        send(k_all.at[last], k_tail, t_s.at[0], t_r.at[0], ahead),
        send(v_all.at[last], v_tail, t_s.at[1], t_r.at[1], ahead),
    )
    copies[0].wait()
    copies[1].wait()

    @pl.when(sp < n_sp - 1)
    def _():
        for copy in tails:
            copy.start()

    def tell(d):
        there = lax.rem(z + d, nz)
        return send(rw_src, rw_all.at[z], g_s.at[d], g_r.at[z], (sp, there * CORES + c))

    def told(d):
        there = lax.rem(z + d, nz)
        return send(rw_src, rw_all.at[there], g_s.at[d], g_r.at[there], (sp, there * CORES + c))

    for d in range(1, nz):
        tell(d).start()
    copies[2].wait()
    copies[4].wait()
    for p in range(n_tp):
        out_rows(p).start()

    row = lax.broadcasted_iota(jnp.int32, (WINDOW, 2 * WINDOW), 0)
    col = lax.broadcasted_iota(jnp.int32, (WINDOW, 2 * WINDOW), 1)
    distance = row + WINDOW - col
    banded = (distance >= 0) & (distance < WINDOW)
    low = z < nz // 2
    half = max(1, blocks // 2)

    own_cols = pl.ds(pl.multiple_of(tp * cols, cols), cols)

    def to_owner(dest):
        at = pl.multiple_of(dest * tok, tok)
        return send(
            att.at[pl.ds(at, tok)], got.at[:, own_cols], a_s.at[dest], a_r.at[tp], (sp, dest)
        )

    def attend(i, carry):
        turned = jnp.where(i < half, lax.rem(i + 1, half), i)
        block = jnp.where(low, blocks - 1 - i, turned)

        @pl.when(block == 0)
        def _():
            @pl.when(sp > 0)
            def _():
                for copy in tails:
                    copy.wait_recv()
                k_all[pl.ds(0, WINDOW), :] = k_tail[...]
                v_all[pl.ds(0, WINDOW), :] = v_tail[...]

            @pl.when(sp == 0)
            def _():
                k_all[pl.ds(0, WINDOW), :] = jnp.zeros((WINDOW, kv_cols), jnp.bfloat16)
                v_all[pl.ds(0, WINDOW), :] = jnp.zeros((WINDOW, kv_cols), jnp.bfloat16)

        at = pl.multiple_of(block * WINDOW, WINDOW)
        start = jnp.where((sp == 0) & (block == 0), WINDOW, 0)
        allowed = banded & (col >= start)
        band = pl.ds(at, 2 * WINDOW)
        for g in range(kv_local):
            keys = k_all[band, g * HEAD : (g + 1) * HEAD]
            values = v_all[band, g * HEAD : (g + 1) * HEAD]
            heads = []
            for m in range(group):
                h = g * group + m
                query = q_all[pl.ds(at, WINDOW), h * HEAD : (h + 1) * HEAD] * jnp.bfloat16(scale)
                scores = lax.dot_general(
                    query, keys, (((1,), (1,)), ((), ())), preferred_element_type=jnp.float32
                )
                logits = jnp.where(allowed, scores, -jnp.inf)
                top = jnp.maximum(jnp.max(logits, axis=-1, keepdims=True), sink[h])
                raised = jnp.exp(logits - top)
                total = jnp.sum(raised, axis=-1, keepdims=True) + jnp.exp(sink[h] - top)
                probs = (raised * (1.0 / total)).astype(jnp.bfloat16)
                heads.append(dot(probs, values))
            att[pl.ds(at, WINDOW), g * group * HEAD : (g + 1) * group * HEAD] = jnp.concatenate(
                heads, axis=1
            ).astype(jnp.bfloat16)
        for piece in range(pieces):
            dest = block * pieces + piece

            @pl.when(dest != tp)
            def _():
                to_owner(dest).start()

        return carry

    lax.fori_loop(0, blocks, attend, 0)
    for d in range(1, nz):
        told(d).wait_recv()
    copies[5].wait()
    tables(n_sp, nz, tok, capp, c, routes, rw_all, onehot, share)
    swap.start()
    got[:, own_cols] = att[pl.ds(pl.multiple_of(tp * tok, tok), tok), :]
    copies[6].wait()
    copies[7].wait()
    wide = math.gcd(width, 512)

    def begin(at):
        acc[:, at] = res[:, at].astype(jnp.float32)

    tiled(width, wide, begin)
    for p in range(n_tp):
        out_rows(p).wait()

    part = n_tp // 2

    def arrived(i, carry):
        p = jnp.where(low, n_tp - 1 - i, i)

        @pl.when(tp != p)
        def _():
            into = got.at[:, pl.ds(pl.multiple_of(p * cols, cols), cols)]
            send(att.at[pl.ds(0, tok)], into, a_s.at[p], a_r.at[p], (sp, p)).wait_recv()

        return carry

    for far in range(2):
        lax.fori_loop(far * part, (far + 1) * part, arrived, 0)
        first = jnp.where(low, (1 - far) * part, far * part) * cols
        rows = pl.ds(pl.multiple_of(first, part * cols), part * cols)

        def one(at):
            acc[:, at] = acc[:, at] + dot(got[:, rows], w_all[rows, at])

        tiled(width, wide, one)

    squares = jnp.zeros((tok, 1), jnp.float32)
    for t in range(width // wide):
        at = slice(t * wide, (t + 1) * wide)
        held = acc[:, at].astype(jnp.bfloat16)
        stream[:, at] = held
        held32 = held.astype(jnp.float32)
        squares = squares + jnp.sum(held32 * held32, axis=-1, keepdims=True)
    root = lax.rsqrt(squares * (1.0 / width) + eps)
    for t in range(width // wide):
        at = slice(t * wide, (t + 1) * wide)
        normed[:, at] = (stream[:, at].astype(jnp.float32) * root * gain[:, at]).astype(
            jnp.bfloat16
        )
    expert_kernel(
        n_sp, nz, swap, normed, stream, onehot, share, out, gate_v, up_v, down_v, *rest
    )
    for p in range(n_tp):
        @pl.when(tp != p)
        def _():
            to_owner(p).wait_send()

    for d in range(1, nz):
        tell(d).wait_send()

    @pl.when(sp < n_sp - 1)
    def _():
        for copy in tails:
            copy.wait_send()


def local(
    query_heads,
    key_heads,
    value_heads,
    sink_logit,
    residual,
    out_weight,
    norm_gain,
    routes,
    route_weight,
    gate_weight,
    up_weight,
    down_weight,
):
    n_sp, n_tp = lax.axis_size("sp"), lax.axis_size("tp")
    nz = n_tp // CORES
    span, cols = query_heads.shape
    kv_cols = key_heads.shape[1]
    tok, width = residual.shape
    choose = routes.shape[1]
    capp = round_up(max(2, 5 * tok * choose // (4 * n_sp)), 16)
    slots = n_sp * capp
    hidden = CORES * gate_weight.shape[2]
    ka = split_columns(width, DISPATCH_SHARE)
    na = split_columns(width, RETURN_SHARE)
    kb, nb = width - ka, width - na
    vmem = pl.BlockSpec(memory_space=pltpu.VMEM)
    inputs = (
        query_heads, key_heads, value_heads, sink_logit, residual, out_weight,
        norm_gain.reshape(1, -1), routes.T, route_weight.T,
        gate_weight[0], up_weight[0], down_weight[0],
    )
    dma = pltpu.SemaphoreType.DMA
    bf = jnp.bfloat16
    line = [dma((nz,))] * 4
    scratch = (
        [
            pltpu.VMEM((tok, width), bf),
            pltpu.VMEM((tok, width), bf),
            pltpu.VMEM((nz, slots, tok), bf),
            pltpu.VMEM((nz, tok, slots), bf),
            pltpu.VMEM((width, hidden), bf),
            pltpu.VMEM((width, hidden), bf),
            pltpu.VMEM((hidden, width), bf),
            pltpu.VMEM((span, cols), bf),
            pltpu.VMEM((span + WINDOW, kv_cols), bf),
            pltpu.VMEM((span + WINDOW, kv_cols), bf),
            pltpu.VMEM((WINDOW, kv_cols), bf),
            pltpu.VMEM((WINDOW, kv_cols), bf),
            pltpu.VMEM((span, cols), bf),
            pltpu.VMEM((tok, n_tp * cols), bf),
            pltpu.VMEM((n_tp * cols, width), bf),
            pltpu.VMEM((tok, width), bf),
            pltpu.VMEM((tok, width), jnp.float32),
            pltpu.VMEM((8, LANES), jnp.float32),
            pltpu.VMEM((nz, 8, LANES), jnp.float32),
            pltpu.SMEM(sink_logit.shape, jnp.float32),
            pltpu.VMEM((1, width), jnp.float32),
            pltpu.VMEM(routes.shape[::-1], routes.dtype),
            pltpu.VMEM(route_weight.shape[::-1], jnp.float32),
            dma((8,)),
            dma((n_tp,)),
            dma((2,)),
            dma((2,)),
            dma((n_tp,)),
            dma((n_tp,)),
            dma((nz,)),
            dma((nz,)),
        ]
        + [dma((3,))] * 3
        + [pltpu.VMEM((nz, tok, w), bf) for w in halves(ka)]
        + [pltpu.VMEM((nz, n_sp, capp, w), bf) for w in halves(ka)]
        + [pltpu.VMEM((n_sp, capp, kb), bf)]
        + [pltpu.VMEM((nz, n_sp, capp, w), bf) for w in (*halves(ka), kb)]
        + [pltpu.VMEM((slots, hidden), bf)]
        + [pltpu.VMEM((nz, n_sp, capp, w), bf) for w in (*halves(na), nb, *halves(na))]
        + [pltpu.VMEM((n_sp, capp, nb), bf)]
        + [pltpu.VMEM((nz, tok, w), bf) for w in halves(na) * 3]
        + [pltpu.VMEM((nz, n_sp, capp, nb), bf)] * 2
        + [dma((CHUNKS * nz,))] * 4
        + [dma((CHUNKS * nz, n_sp))] * 2
        + [dma((n_sp,))] * 2
        + line
        + [dma((CHUNKS * nz, n_sp))] * 2
        + [dma((n_sp,))] * 2
        + [dma((CHUNKS * nz,))] * 4
        + line
    )
    return pl.pallas_call(
        functools.partial(layer_kernel, n_sp, n_tp, tok, capp),
        out_shape=jax.ShapeDtypeStruct((tok, width), bf),
        in_specs=[pl.BlockSpec(memory_space=pltpu.HBM)] * len(inputs),
        out_specs=vmem,
        scratch_shapes=scratch,
        compiler_params=pltpu.CompilerParams(
            collective_id=0, has_side_effects=True, vmem_limit_bytes=held_bytes(scratch) + SPARE
        ),
        name="layer",
    )(*[pltpu.with_memory_space_constraint(x, pltpu.HBM) for x in inputs])


def solution(mesh):
    placed = (
        P("sp", "tp"),
        P("sp", "tp"),
        P("sp", "tp"),
        P("tp"),
        P(("sp", "tp"), None),
        P(),
        P(),
        P("sp", None),
        P(("sp", "tp"), None),
        P("sp", None, "tp"),
        P("sp", None, "tp"),
        P("sp", "tp", None),
    )
    return jax.shard_map(
        local, mesh=mesh, in_specs=placed, out_specs=P(("sp", "tp"), None), check_vma=False
    )
```
